128 devices in a mesh: tp: 16 (over z, y), dp: 8 (over x, core).
Axes of the slice: x: 4, y: 4, z: 4, core: 2. Of those that a mesh axis runs over, the one named last changes fastest.
Arguments:
- tokens: bfloat16 [256, 4096], P('dp', 'tp'), may hold values from -6 to 6
- lengths: int32 [256], P('dp'), may hold values from 1 to 96, 6144 in all
- norm_gain: float32 [2, 4096], replicated, may hold values from 0.1 to 1.9
- w_recept: bfloat16 [2, 4096, 4096], P(None, None, ('tp', 'dp')), may hold values from -0.09375 to 0.09375
- w_key: bfloat16 [2, 4096, 4096], P(None, None, ('tp', 'dp')), may hold values from -0.09375 to 0.09375
- w_value: bfloat16 [2, 4096, 4096], P(None, None, ('tp', 'dp')), may hold values from -0.09375 to 0.09375
- w_decay: bfloat16 [2, 4096, 4096], P(None, None, ('tp', 'dp')), may hold values from -0.09375 to 0.09375
- w_rate: bfloat16 [2, 4096, 4096], P(None, None, ('tp', 'dp')), may hold values from -0.09375 to 0.09375
- w_gate: bfloat16 [2, 4096, 4096], P(None, None, ('tp', 'dp')), may hold values from -0.09375 to 0.09375
- w_out: bfloat16 [2, 4096, 4096], P(None, None, ('tp', 'dp')), may hold values from -0.09375 to 0.09375
- decay_base: float32 [2, 4096], P(None, 'tp'), may hold values from -3 to 1
- rate_base: float32 [2, 4096], P(None, 'tp'), may hold values from -3 to 3
- group_gain: float32 [2, 4096], P(None, 'tp'), may hold values from 0.1 to 1.9
- state: float32 [2, 256, 64, 64, 64], P(None, 'dp', 'tp'), may hold values from -6 to 6
Outputs:
- mixed: bfloat16 [256, 4096], P('dp', 'tp')
- new_state: float32 [2, 256, 64, 64, 64], P(None, 'dp', 'tp')
The draws below stay inside these ranges and needn't reach their ends.
Inputs may be any that keep to these rules, and one draw needn't show every extreme that they name: Each sequence's live length lies between 1 and 96, some sequences reach 96, and the lengths sum to 6144.
All inputs are finite; a program needn't handle non-finite values.
Results may differ from the reference program's by a relative error of at most 0.025.
Values may be sent and summed in bfloat16 or wider, within the bound.
A program may use at most 128 MiB of HBM per device.

```python
import math
import jax
import jax.numpy as jnp
import numpy as np
from jax import lax

D = 4096
HEAD = 64
STEP = 16
BATCH = 256


def steps_of(key, extent, cuts, least, high):
    gain, own = 1.0, jax.random.fold_in(key, 6)
    for dim, blocks in cuts:
        heights = jnp.exp(jax.random.uniform(jax.random.fold_in(own, dim), (blocks,), jnp.float32, least / len(cuts), high / len(cuts)))
        gain = gain * jnp.repeat(heights, extent[dim] // blocks).reshape([-1 if axis == dim else 1 for axis in range(len(extent))])
    return gain


def profile(amount, total, reach, slope):
    loads = [(1 << 20) // math.isqrt(grade ** slope) + 1 for grade in range(2, amount + 1)]
    surplus, given = total - reach - (amount - 1), [1] * (amount - 1)
    while surplus > 0:
        candidates = [i for i in range(amount - 1) if given[i] < reach]
        pool, left = sum([loads[i] for i in candidates]), surplus
        for i in candidates:
            addition = min(reach - given[i], max(1, left * loads[i] // pool), surplus)
            given[i] = given[i] + addition
            surplus = surplus - addition
    return np.array([reach] + given)


def uneven_parts(key, amount, total, limit, slope):
    if amount == 2:
        one = jax.random.randint(key, (), max(1, total - limit), min(limit, total - 1) + 1)
        return jnp.stack([one, total - one])
    sizes = jnp.asarray(profile(amount, total, limit, slope), jnp.int32)
    couples = (amount - 1) // 2
    donor, receiver = sizes[1:1 + 2 * couples:2], sizes[2:2 + 2 * couples:2]
    room = jnp.minimum(donor - 1, limit - receiver)
    moved = jax.random.randint(jax.random.fold_in(key, 1), (couples,), 0, 1 << 20) % (room + 1)
    sizes = sizes.at[1:1 + 2 * couples:2].set(donor - moved).at[2:2 + 2 * couples:2].set(receiver + moved)
    return sizes[jax.random.permutation(jax.random.fold_in(key, 2), amount)]


def scatter_about(rng, dims, width, reach, pieces=(), dtype=jnp.bfloat16):
    level = steps_of(rng, dims, pieces, -0.22, 0.18) if pieces else 1.0
    values = jax.random.normal(rng, dims, jnp.float32) * width * level
    return jnp.minimum(jnp.maximum(values, -reach), reach).astype(dtype)


def setup_inputs(seed: int = 0) -> dict:
    splits = jax.random.split(jax.random.key(seed), 15)
    tokens = scatter_about(splits[0], (BATCH, D), 1.0, 6.0, ((0, 8), (1, 16)))
    lengths = uneven_parts(splits[1], BATCH, 24 * BATCH, 96, 2).astype(jnp.int32)
    norm_gain = jnp.clip(1.0 + 0.18 * jax.random.normal(splits[2], (2, D), jnp.float32), 0.1, 1.9)
    w_recept = scatter_about(splits[3], (2, D, D), D ** -0.5, 0.09375, ((2, 128),))
    w_key = scatter_about(splits[4], (2, D, D), D ** -0.5, 0.09375, ((2, 128),))
    w_value = scatter_about(splits[5], (2, D, D), D ** -0.5, 0.09375, ((2, 128),))
    w_decay = scatter_about(splits[6], (2, D, D), D ** -0.5, 0.09375, ((2, 128),))
    w_rate = scatter_about(splits[7], (2, D, D), D ** -0.5, 0.09375, ((2, 128),))
    w_gate = scatter_about(splits[8], (2, D, D), D ** -0.5, 0.09375, ((2, 128),))
    w_out = scatter_about(splits[9], (2, D, D), D ** -0.5, 0.09375, ((2, 128),))
    decay_base = jnp.clip(-3.0 + 4.0 * jax.random.uniform(splits[10], (2, D), jnp.float32) ** steps_of(splits[10], (2, D), ((1, 16),), -0.2, 0.2), -3.0, 1.0)
    rate_base = scatter_about(splits[11], (2, D), 0.5, 3.0, ((1, 16),), jnp.float32)
    group_gain = jnp.clip(1.0 + 0.18 * jax.random.normal(splits[12], (2, D), jnp.float32), 0.1, 1.9)
    state = scatter_about(splits[13], (2, BATCH, D // HEAD, HEAD, HEAD), 1.0, 6.0, ((1, 8), (2, 16)), jnp.float32)
    return dict(tokens=tokens, lengths=lengths, norm_gain=norm_gain, w_recept=w_recept, w_key=w_key, w_value=w_value, w_decay=w_decay, w_rate=w_rate, w_gate=w_gate, w_out=w_out, decay_base=decay_base, rate_base=rate_base, group_gain=group_gain, state=state)


RMS_EPS = 1e-06
GROUP_EPS = 0.00064

def stored(matrix, weight):
    product = jnp.dot(matrix, weight, preferred_element_type=jnp.float32)
    return lax.optimization_barrier(product.astype(jnp.bfloat16)).astype(jnp.float32)

def recur(state_old, recept, key_vec, value_vec, decay_rate, learn_rate, active, head_size):
    split = (recept.shape[0], -1, head_size)
    recept_h = recept.reshape(split)
    key_h = key_vec.reshape(split)
    value_h = value_vec.reshape(split)
    decay_h = decay_rate.reshape(split)
    rate_h = learn_rate.reshape(split)
    key_len = jnp.sqrt(lax.optimization_barrier(jnp.sum(key_h * key_h, axis=-1, keepdims=True)))
    key_unit = key_h / jnp.maximum(key_len, 1e-12)
    state_a = jnp.einsum('bhij,bhj->bhi', state_old, -key_unit, precision=lax.Precision.HIGHEST)
    updated = state_old * decay_h[:, :, None, :] + state_a[:, :, :, None] * (key_unit * rate_h)[:, :, None, :] + value_h[:, :, :, None] * (key_h * rate_h)[:, :, None, :]
    updated = jnp.where(active[:, None, None, None], updated, state_old)
    readout = jnp.einsum('bhij,bhj->bhi', updated, recept_h, precision=lax.Precision.HIGHEST)
    centre = lax.optimization_barrier(jnp.mean(readout, axis=-1, keepdims=True))
    spread = lax.optimization_barrier(jnp.mean(jnp.square(readout - centre), axis=-1, keepdims=True))
    normal_out = ((readout - centre) * lax.rsqrt(spread + GROUP_EPS)).reshape(recept.shape[0], -1)
    return (updated, normal_out)

def reference(tokens, lengths, norm_gain, w_recept, w_key, w_value, w_decay, w_rate, w_gate, w_out, decay_base, rate_base, group_gain, state):
    active = lengths > STEP
    current = tokens
    updated_states = []
    for layer_idx in range(2):
        values = current.astype(jnp.float32)
        factor = lax.rsqrt(lax.optimization_barrier(jnp.mean(values * values, axis=1, keepdims=True)) + RMS_EPS)
        normed = (values * factor * norm_gain[layer_idx]).astype(jnp.bfloat16)
        recept = stored(normed, w_recept[layer_idx])
        key_vec = stored(normed, w_key[layer_idx])
        value_vec = stored(normed, w_value[layer_idx])
        decay_pre = stored(normed, w_decay[layer_idx])
        rate_pre = stored(normed, w_rate[layer_idx])
        gate_pre = stored(normed, w_gate[layer_idx])
        decay_rate = jnp.exp(-jnp.exp(-jax.nn.softplus(-(decay_base[layer_idx] + decay_pre)) - 0.5))
        learn_rate = jax.nn.sigmoid(rate_base[layer_idx] + rate_pre)
        gate_open = jax.nn.sigmoid(gate_pre)
        updated, normal_out = recur(state[layer_idx], recept, key_vec, value_vec, decay_rate, learn_rate, active, HEAD)
        updated_states.append(updated)
        mixed_rows = jnp.where(active[:, None], normal_out * group_gain[layer_idx] * gate_open, 0.0).astype(jnp.bfloat16)
        current = jnp.dot(mixed_rows, w_out[layer_idx], preferred_element_type=jnp.float32).astype(jnp.bfloat16)
    return (current, jnp.stack(updated_states))
```

```python
import functools

import jax
import jax.numpy as jnp
from jax import lax
from jax.experimental import pallas as pl
from jax.experimental.pallas import tpu as pltpu
from jax.sharding import PartitionSpec as P

STEP = 16
RMS_EPS = 1e-06
GROUP_EPS = 0.00064
MESH = pl.DeviceIdType.MESH
F32 = jnp.float32
BF16 = jnp.bfloat16
ORDERS = (("x", "y", "z"), ("y", "z", "x"), ("z", "x", "y"), ("y", "x", "z"))
LANES = (((1,), (1,)), ((), ()))
PLAIN = (((1,), (0,)), ((), ()))
ROWS = (((0,), (0,)), ((), ()))


def step_kernel(
    tok, lens, gain, w0, w1, w2, w3, w4, w5, w_out, dbase, rbase, ggain, state,
    mixed, sa_out, v_out, pq_out, dec_out,
    G, WP, WO, ST, SB, RB, FB, FR, V8, M2,
    g_send, g_recv, a_send, a_recv, w_local, w_send, w_recv, st_sem, tok_sem,
):
    tp, dp = lax.axis_index("tp"), lax.axis_index("dp")
    c = dp % 2
    at = {"z": tp // 4, "y": tp % 4, "x": dp // 2}
    projections = (w0, w1, w2, w3, w4, w5)

    def device(axis, hop):
        to = dict(at)
        to[axis] = (at[axis] + hop) % 4
        return (to["z"] * 4 + to["y"], to["x"] * 2 + c)

    partner = (tp, at["x"] * 2 + 1 - c)

    barrier = pltpu.get_barrier_semaphore()
    for axis in "xyz":
        for hop in (1, 2, 3):
            pl.semaphore_signal(barrier, inc=1, device_id=device(axis, hop), device_id_type=MESH)
    pl.semaphore_signal(barrier, inc=1, device_id=partner, device_id_type=MESH)

    tok_copies = []
    for q in range(4):
        rh, ch = q // 2, q % 2
        tok_copies.append(pltpu.make_async_copy(
            tok.at[pl.ds(rh * 16, 16), pl.ds(ch * 128, 128)],
            G.at[0, q, at["z"], at["y"], at["x"]],
            tok_sem.at[q],
        ))
        tok_copies[-1].start()
    mine = pl.multiple_of(c * 32, 32)
    for layer in range(2):
        for kind in range(6):
            pltpu.make_async_copy(
                projections[kind].at[layer],
                WP.at[layer, pl.ds(kind * 64 + mine, 32)],
                w_local.at[layer, 0],
            ).start()
        pltpu.make_async_copy(
            w_out.at[layer], WO.at[layer, pl.ds(mine, 32)], w_local.at[layer, 1]
        ).start()
        pltpu.make_async_copy(state.at[layer], ST.at[layer], st_sem.at[layer]).start()

    pl.semaphore_wait(barrier, 10)

    def block(a, q, free, moved=None):
        idx = [moved[ax] if moved and ax in moved else at[ax] for ax in "zyx"]
        idx = [slice(None) if ax in free else i for ax, i in zip("zyx", idx)]
        return G.at[(a, q, *idx)]

    def send(ref, axis, hop, send_sem, recv_sem):
        pltpu.make_async_remote_copy(
            src_ref=ref, dst_ref=ref, send_sem=send_sem, recv_sem=recv_sem,
            device_id=device(axis, hop), device_id_type=MESH,
        ).start()

    def landed(ref, sem):
        pltpu.make_async_copy(ref, ref, sem).wait()

    def gather_first(a):
        for q in range(4):
            if a == 0:
                tok_copies[q].wait()
            for hop in (1, 2, 3):
                send(block(a, q, ()), ORDERS[q][0], hop, g_send.at[a, q, 0], g_recv.at[a, q, 0])

    def gather_middle(a):
        for q in range(4):
            first, second, third = ORDERS[q]
            landed(G.at[a, q, 0, 0, pl.ds(0, 3)], g_recv.at[a, q, 0])
            for hop in (2, 1, 3):
                send(block(a, q, first), second, hop, g_send.at[a, q, 1], g_recv.at[a, q, hop])
            for hop in (2, 1, 3):
                send(block(a, q, first), third, hop, g_send.at[a, q, 2], g_recv.at[a, q, 4])
        for hop in (1, 3, 2):
            for q in range(4):
                first, second, third = ORDERS[q]
                landed(G.at[a, q, 0, 0], g_recv.at[a, q, hop])
                line = {second: (at[second] + 4 - hop) % 4}
                for on in (2, 1, 3):
                    send(block(a, q, first, line), third, on, g_send.at[a, q, 2], g_recv.at[a, q, 4])

    def gather_last(a):
        for q in range(4):
            landed(G.at[a, q, pl.ds(0, 3)], g_recv.at[a, q, 4])

    def gather_sent(a):
        for q in range(4):
            landed(G.at[a, q, 0, 0, pl.ds(0, 3)], g_send.at[a, q, 0])
            landed(G.at[a, q, pl.ds(0, 3), :, 0], g_send.at[a, q, 1])
            landed(G.at[a, q, pl.ds(0, 3)], g_send.at[a, q, 2])

    def rows_chunk(a, z):
        parts = []
        for y in range(4):
            for ch in range(2):
                halves = [G[a, rh * 2 + ch, z, y].reshape(64, 128) for rh in range(2)]
                parts.append(jnp.concatenate(halves, axis=0))
        return parts

    def exchange(n, src, dst):
        for hop in (2, 1, 3):
            to = (at["x"] + hop) % 4
            pltpu.make_async_remote_copy(
                src_ref=src.at[to], dst_ref=dst.at[at["x"]],
                send_sem=a_send.at[n], recv_sem=a_recv.at[n],
                device_id=device("x", hop), device_id_type=MESH,
            ).start()
        dst[at["x"]] = src[at["x"]]
        landed(dst.at[pl.ds(0, 3)], a_recv.at[n])

    def exchange_sent(n, src):
        landed(src.at[pl.ds(0, 3)], a_send.at[n])

    def weights_out():
        for layer in range(2):
            for kind in range(6):
                pltpu.make_async_remote_copy(
                    src_ref=projections[kind].at[layer],
                    dst_ref=WP.at[layer, pl.ds(kind * 64 + mine, 32)],
                    send_sem=w_send.at[layer, 0], recv_sem=w_recv.at[layer, 0],
                    device_id=partner, device_id_type=MESH,
                ).start()
            pltpu.make_async_remote_copy(
                src_ref=w_out.at[layer],
                dst_ref=WO.at[layer, pl.ds(mine, 32)],
                send_sem=w_send.at[layer, 1], recv_sem=w_recv.at[layer, 1],
                device_id=partner, device_id_type=MESH,
            ).start()

    def weights_in(layer):
        landed(WP.at[layer, pl.ds(0, 192)], w_local.at[layer, 0])
        landed(WP.at[layer, pl.ds(0, 192)], w_recv.at[layer, 0])
        landed(WO.at[layer, pl.ds(0, 32)], w_local.at[layer, 1])
        landed(WO.at[layer, pl.ds(0, 32)], w_recv.at[layer, 1])
        scale = gain[layer:layer + 1, :]

        def fold(i, carry):
            rows = pl.ds(pl.multiple_of(i * 16, 16), 16)
            WP[layer, rows, :] = (WP[layer, rows, :].astype(F32) * scale).astype(BF16)
            return carry

        lax.fori_loop(0, 24, fold, 0)

    def weights_sent():
        for layer in range(2):
            landed(WP.at[layer, pl.ds(0, 192)], w_send.at[layer, 0])
            landed(WO.at[layer, pl.ds(0, 32)], w_send.at[layer, 1])

    def put_projected(layer, projected):
        out = projected.astype(BF16)
        for to in range(4):
            SB[layer, to, 0:16, :] = out[to * 16:to * 16 + 16, :]
            SB[layer, to, 16:32, :] = out[64 + to * 16:64 + to * 16 + 16, :]

    def project_first():
        acc = jnp.zeros((128, 384), F32)
        squares = jnp.zeros((128, 128), F32)
        for z in range(4):
            parts = rows_chunk(0, z)
            for part in parts:
                wide = part.astype(F32)
                squares += wide * wide
            acc += lax.dot_general(
                jnp.concatenate(parts, axis=1), WP[0, :, z * 1024:(z + 1) * 1024], LANES,
                preferred_element_type=F32,
            )
        factor = lax.rsqrt(jnp.sum(squares, axis=1, keepdims=True) * (1.0 / 4096) + RMS_EPS)
        put_projected(0, acc * factor)

    def project_second():
        acc = jnp.zeros((384, 128), F32)
        squares = jnp.zeros((16, 128), F32)
        for z in range(4):
            parts = [G[2, q, z, y, x] for y in range(4) for x in range(4) for q in range(4)]
            for part in parts:
                wide = part.astype(F32)
                squares += wide * wide
            acc += lax.dot_general(
                WP[1, :, z * 1024:(z + 1) * 1024], jnp.concatenate(parts, axis=0), PLAIN,
                preferred_element_type=F32,
            )
        factor = lax.rsqrt(jnp.sum(squares, axis=0, keepdims=True) * (1.0 / 4096) + RMS_EPS)
        put_projected(1, (acc * factor).T)

    ident = lax.broadcasted_iota(jnp.int32, (32, 32), 0) == lax.broadcasted_iota(jnp.int32, (32, 32), 1)
    length = jnp.sum(jnp.where(ident, jnp.broadcast_to(lens[0:1, :], (32, 32)), 0), axis=1, keepdims=True)
    active = length > STEP

    def wide128(value):
        return jnp.concatenate([value, jnp.zeros_like(value)], axis=1)

    def recur(layer, a):
        values, gates, first_sums, second_sums = [], [], [], []
        for h in range(4):
            take = lambda kind: RB[layer, h, :, kind * 64:(kind + 1) * 64].astype(F32)
            recept, key, value, dpre, rpre, gpre = [take(kind) for kind in range(6)]
            cols = slice(h * 64, (h + 1) * 64)
            decay = jnp.exp(-(0.6065306597126334 * jax.nn.sigmoid(dbase[layer:layer + 1, cols] + dpre)))
            rate = jax.nn.sigmoid(rbase[layer:layer + 1, cols] + rpre)
            norm = jnp.sqrt(jnp.sum(key * key, axis=1, keepdims=True))
            unit = key / jnp.maximum(norm, 1e-12)
            up, kp = unit * rate, key * rate
            first_sums.append(jnp.broadcast_to(jnp.sum(up * recept, axis=1, keepdims=True), (32, 64)))
            second_sums.append(jnp.broadcast_to(jnp.sum(kp * recept, axis=1, keepdims=True), (32, 64)))
            values.append(value)
            gates.append(jax.nn.sigmoid(gpre))
            V8[pl.ds(h, 32, stride=8), :] = wide128(-unit)
            V8[pl.ds(4 + h, 32, stride=8), :] = wide128(decay * recept)
            pq_out[layer, pl.ds(h, 32, stride=8), :] = wide128(jnp.where(active, up, 0.0))
            pq_out[layer, pl.ds(4 + h, 32, stride=8), :] = wide128(jnp.where(active, kp, 0.0))
            dec_out[layer, pl.ds(h, 32, stride=8), :] = wide128(jnp.where(active, decay, 1.0))
            dec_out[layer, pl.ds(4 + h, 32, stride=8), :] = jnp.zeros((32, 128), F32)
        for b in range(32):
            got = lax.dot_general(
                V8[b * 8:(b + 1) * 8, 0:64].astype(BF16),
                ST[layer, b].reshape(256, 64).astype(BF16), LANES,
                preferred_element_type=F32,
            )
            for half in range(2):
                M2[half, b * 8:(b + 1) * 8, :] = got[:, half * 128:(half + 1) * 128]
        low = lax.broadcasted_iota(jnp.int32, (32, 128), 1) < 64

        def heads(base):
            return jnp.concatenate([
                jnp.where(low, M2[half, pl.ds(base + 2 * half, 32, stride=8), :],
                          M2[half, pl.ds(base + 2 * half + 1, 32, stride=8), :])
                for half in range(2)
            ], axis=1)

        sa, direct = heads(0), heads(4)
        value = jnp.concatenate(values, axis=1)
        sa_out[layer] = sa
        v_out[layer] = value
        readout = direct + sa * jnp.concatenate(first_sums, axis=1) + value * jnp.concatenate(second_sums, axis=1)
        normal = []
        for h in range(4):
            seg = readout[:, h * 64:(h + 1) * 64]
            seg = seg - jnp.sum(seg, axis=1, keepdims=True) * (1.0 / 64)
            spread = jnp.sum(seg * seg, axis=1, keepdims=True) * (1.0 / 64)
            normal.append(seg * lax.rsqrt(spread + GROUP_EPS))
        rows = jnp.concatenate(normal, axis=1) * ggain[layer:layer + 1, :] * jnp.concatenate(gates, axis=1)
        rows = jnp.where(active, rows, 0.0).astype(BF16)
        for q in range(4):
            rh, ch = q // 2, q % 2
            G[a, q, at["z"], at["y"], at["x"]] = rows[rh * 16:(rh + 1) * 16, ch * 128:(ch + 1) * 128]

    gather_first(0)
    weights_out()
    gather_middle(0)
    weights_in(0)
    gather_last(0)
    project_first()
    exchange(0, SB.at[0], RB.at[0])
    landed(ST.at[0], st_sem.at[0])
    recur(0, 1)

    gather_first(1)
    gather_middle(1)
    weights_in(1)
    gather_last(1)
    acc = jnp.zeros((64, 128), F32)
    for z in range(4):
        acc += lax.dot_general(
            WO[0, :, z * 1024:(z + 1) * 1024], jnp.concatenate(rows_chunk(1, z), axis=1), LANES,
            preferred_element_type=F32,
        )
    out = acc.astype(BF16)
    for q in range(4):
        G[2, q, at["z"], at["y"], at["x"]] = out[q * 16:(q + 1) * 16, :]

    gather_first(2)
    gather_middle(2)
    gather_last(2)
    project_second()
    exchange(1, SB.at[1], RB.at[1])
    landed(ST.at[1], st_sem.at[1])
    recur(1, 3)

    gather_first(3)
    gather_middle(3)
    gather_last(3)
    acc = jnp.zeros((128, 64), F32)
    for z in range(4):
        acc += lax.dot_general(
            jnp.concatenate(rows_chunk(3, z), axis=1), WO[1, :, z * 1024:(z + 1) * 1024], LANES,
            preferred_element_type=F32,
        )
    out = wide128(acc).astype(BF16)
    for to in range(4):
        FB[to, 0:16, :] = out[to * 16:to * 16 + 16, :]
        FB[to, 16:32, :] = out[64 + to * 16:64 + to * 16 + 16, :]
    exchange(2, FB, FR)
    mixed[...] = jnp.concatenate([FR[h, :, 0:64] for h in range(4)], axis=1)

    for a in range(4):
        gather_sent(a)
    exchange_sent(0, SB.at[0])
    exchange_sent(1, SB.at[1])
    exchange_sent(2, FB)
    weights_sent()


def update_kernel(state, sa, val, pq, dec, out):
    own = lax.broadcasted_iota(jnp.int32, (8, 256), 1) // 64
    row = lax.broadcasted_iota(jnp.int32, (8, 256), 0)
    for b in range(8):
        left = jnp.where(row < 4, jnp.broadcast_to(sa[0, b:b + 1, :], (8, 256)),
                         jnp.broadcast_to(val[0, b:b + 1, :], (8, 256)))
        left = jnp.where(row % 4 == own, left, 0.0)
        delta = lax.dot_general(
            left.astype(BF16), pq[0, b * 8:(b + 1) * 8, 0:64].astype(BF16), ROWS,
            preferred_element_type=F32,
        )
        for h in range(4):
            out[0, b, h] = state[0, b, h] * dec[0, b * 8 + h:b * 8 + h + 1, 0:64] + delta[h * 64:(h + 1) * 64, :]


def local(tokens, lengths, norm_gain, w_recept, w_key, w_value, w_decay, w_rate, w_gate, w_out,
          decay_base, rate_base, group_gain, state):
    weights = [jnp.swapaxes(w, 1, 2) for w in (w_recept, w_key, w_value, w_decay, w_rate, w_gate, w_out)]
    any_spec = pl.BlockSpec(memory_space=pl.ANY)
    vmem = pl.BlockSpec(memory_space=pltpu.VMEM)
    mixed, sa, val, pq, dec = pl.pallas_call(
        step_kernel,
        out_shape=(
            jax.ShapeDtypeStruct((32, 256), BF16),
            jax.ShapeDtypeStruct((2, 32, 256), F32),
            jax.ShapeDtypeStruct((2, 32, 256), F32),
            jax.ShapeDtypeStruct((2, 256, 128), F32),
            jax.ShapeDtypeStruct((2, 256, 128), F32),
        ),
        in_specs=[any_spec, vmem, vmem] + [any_spec] * 7 + [vmem] * 3 + [any_spec],
        out_specs=(vmem,) * 5,
        scratch_shapes=[
            pltpu.VMEM((4, 4, 4, 4, 4, 16, 128), BF16),
            pltpu.VMEM((2, 384, 4096), BF16),
            pltpu.VMEM((2, 64, 4096), BF16),
            pltpu.VMEM((2, 32, 4, 64, 64), F32),
            pltpu.VMEM((2, 4, 32, 384), BF16),
            pltpu.VMEM((2, 4, 32, 384), BF16),
            pltpu.VMEM((4, 32, 128), BF16),
            pltpu.VMEM((4, 32, 128), BF16),
            pltpu.VMEM((256, 128), F32),
            pltpu.VMEM((2, 256, 128), F32),
            pltpu.SemaphoreType.DMA((4, 4, 3)),
            pltpu.SemaphoreType.DMA((4, 4, 5)),
            pltpu.SemaphoreType.DMA((3,)),
            pltpu.SemaphoreType.DMA((3,)),
            pltpu.SemaphoreType.DMA((2, 2)),
            pltpu.SemaphoreType.DMA((2, 2)),
            pltpu.SemaphoreType.DMA((2, 2)),
            pltpu.SemaphoreType.DMA((2,)),
            pltpu.SemaphoreType.DMA((4,)),
        ],
        compiler_params=pltpu.CompilerParams(collective_id=0, has_side_effects=True),
        name="decode_step",
    )(tokens, lengths.reshape(1, 32), norm_gain, *weights, decay_base, rate_base, group_gain, state)
    new_state = pl.pallas_call(
        update_kernel,
        grid=(2, 4),
        out_shape=jax.ShapeDtypeStruct(state.shape, F32),
        in_specs=[
            pl.BlockSpec((1, 8, 4, 64, 64), lambda l, i: (l, i, 0, 0, 0)),
            pl.BlockSpec((1, 8, 256), lambda l, i: (l, i, 0)),
            pl.BlockSpec((1, 8, 256), lambda l, i: (l, i, 0)),
            pl.BlockSpec((1, 64, 128), lambda l, i: (l, i, 0)),
            pl.BlockSpec((1, 64, 128), lambda l, i: (l, i, 0)),
        ],
        out_specs=pl.BlockSpec((1, 8, 4, 64, 64), lambda l, i: (l, i, 0, 0, 0)),
        name="state_update",
    )(state, sa, val, pq, dec)
    return mixed, new_state


def solution(mesh):
    both = P(None, None, ("tp", "dp"))
    in_specs = (
        P("dp", "tp"), P("dp"), P(), both, both, both, both, both, both, both,
        P(None, "tp"), P(None, "tp"), P(None, "tp"), P(None, "dp", "tp", None, None),
    )
    out_specs = (P("dp", "tp"), P(None, "dp", "tp", None, None))
    return jax.shard_map(local, mesh=mesh, in_specs=in_specs, out_specs=out_specs, check_vma=False)
```

```python
import functools

import jax
import jax.numpy as jnp
from jax import lax
from jax.experimental import pallas as pl
from jax.experimental.pallas import tpu as pltpu
from jax.sharding import PartitionSpec as P

STEP = 16
RMS_EPS = 1e-06
GROUP_EPS = 0.00064
MESH = pl.DeviceIdType.MESH
F32 = jnp.float32
BF16 = jnp.bfloat16
ORDERS = (("x", "y", "z"), ("y", "z", "x"), ("z", "x", "y"), ("y", "x", "z"))
LANES = (((1,), (1,)), ((), ()))
PLAIN = (((1,), (0,)), ((), ()))
ROWS = (((0,), (0,)), ((), ()))


def step_kernel(
    tok, lens, gain, w0, w1, w2, w3, w4, w5, w_out, dbase, rbase, ggain, state,
    mixed, ST,
    G, WP, WO, SB, RB, FB, FR, V8, M2, SA, VA, PQ, DEC,
    g_send, g_recv, a_send, a_recv, w_local, w_send, w_recv, st_sem, tok_sem,
):
    tp, dp = lax.axis_index("tp"), lax.axis_index("dp")
    c = dp % 2
    at = {"z": tp // 4, "y": tp % 4, "x": dp // 2}
    projections = (w0, w1, w2, w3, w4, w5)

    def device(axis, hop):
        to = dict(at)
        to[axis] = (at[axis] + hop) % 4
        return (to["z"] * 4 + to["y"], to["x"] * 2 + c)

    partner = (tp, at["x"] * 2 + 1 - c)

    barrier = pltpu.get_barrier_semaphore()
    for axis in "xyz":
        for hop in (1, 2, 3):
            pl.semaphore_signal(barrier, inc=1, device_id=device(axis, hop), device_id_type=MESH)

    tok_copies = []
    for q in range(4):
        rh, ch = q // 2, q % 2
        tok_copies.append(pltpu.make_async_copy(
            tok.at[pl.ds(rh * 16, 16), pl.ds(ch * 128, 128)],
            G.at[0, q, at["z"], at["y"], at["x"]],
            tok_sem.at[q],
        ))
        tok_copies[-1].start()
    mine = pl.multiple_of(c * 32, 32)
    for layer in range(2):
        for kind in range(6):
            pltpu.make_async_copy(
                projections[kind].at[layer],
                WP.at[layer, pl.ds(kind * 64 + mine, 32)],
                w_local.at[layer, 0],
            ).start()
        pltpu.make_async_copy(
            w_out.at[layer], WO.at[layer, pl.ds(mine, 32)], w_local.at[layer, 1]
        ).start()

    pl.semaphore_wait(barrier, 9 + c)
    pl.semaphore_signal(barrier, inc=1, device_id=partner, device_id_type=MESH)

    def block(a, q, free, moved=None):
        idx = [moved[ax] if moved and ax in moved else at[ax] for ax in "zyx"]
        idx = [slice(None) if ax in free else i for ax, i in zip("zyx", idx)]
        return G.at[(a, q, *idx)]

    def send(ref, axis, hop, send_sem, recv_sem):
        pltpu.make_async_remote_copy(
            src_ref=ref, dst_ref=ref, send_sem=send_sem, recv_sem=recv_sem,
            device_id=device(axis, hop), device_id_type=MESH,
        ).start()

    def landed(ref, sem):
        pltpu.make_async_copy(ref, ref, sem).wait()

    def gather_first(a):
        for q in range(4):
            if a == 0:
                tok_copies[q].wait()
            for hop in (1, 2, 3):
                send(block(a, q, ()), ORDERS[q][0], hop, g_send.at[a, q, 0], g_recv.at[a, q, 0])

    def gather_middle(a):
        for q in range(4):
            first, second, third = ORDERS[q]
            landed(G.at[a, q, 0, 0, pl.ds(0, 3)], g_recv.at[a, q, 0])
            for hop in (2, 1, 3):
                send(block(a, q, first), second, hop, g_send.at[a, q, 1], g_recv.at[a, q, hop])
            for hop in (2, 1, 3):
                send(block(a, q, first), third, hop, g_send.at[a, q, 2], g_recv.at[a, q, 4])
        for hop in (1, 3, 2):
            for q in range(4):
                first, second, third = ORDERS[q]
                landed(G.at[a, q, 0, 0], g_recv.at[a, q, hop])
                line = {second: (at[second] + 4 - hop) % 4}
                for on in (2, 1, 3):
                    send(block(a, q, first, line), third, on, g_send.at[a, q, 2], g_recv.at[a, q, 4])

    def gather_last(a):
        for q in range(4):
            landed(G.at[a, q, pl.ds(0, 3)], g_recv.at[a, q, 4])

    def gather_sent(a):
        for q in range(4):
            landed(G.at[a, q, 0, 0, pl.ds(0, 3)], g_send.at[a, q, 0])
            landed(G.at[a, q, pl.ds(0, 3), :, 0], g_send.at[a, q, 1])
            landed(G.at[a, q, pl.ds(0, 3)], g_send.at[a, q, 2])

    def rows_chunk(a, z):
        parts = []
        for y in range(4):
            for ch in range(2):
                halves = [G[a, rh * 2 + ch, z, y].reshape(64, 128) for rh in range(2)]
                parts.append(jnp.concatenate(halves, axis=0))
        return parts

    def exchange(n, src, dst):
        for hop in (2, 1, 3):
            to = (at["x"] + hop) % 4
            pltpu.make_async_remote_copy(
                src_ref=src.at[to], dst_ref=dst.at[at["x"]],
                send_sem=a_send.at[n], recv_sem=a_recv.at[n],
                device_id=device("x", hop), device_id_type=MESH,
            ).start()
        dst[at["x"]] = src[at["x"]]
        landed(dst.at[pl.ds(0, 3)], a_recv.at[n])

    def exchange_sent(n, src):
        landed(src.at[pl.ds(0, 3)], a_send.at[n])

    def weights_out():
        for layer in range(2):
            for kind in range(6):
                pltpu.make_async_remote_copy(
                    src_ref=projections[kind].at[layer],
                    dst_ref=WP.at[layer, pl.ds(kind * 64 + mine, 32)],
                    send_sem=w_send.at[layer, 0], recv_sem=w_recv.at[layer, 0],
                    device_id=partner, device_id_type=MESH,
                ).start()
            pltpu.make_async_remote_copy(
                src_ref=w_out.at[layer],
                dst_ref=WO.at[layer, pl.ds(mine, 32)],
                send_sem=w_send.at[layer, 1], recv_sem=w_recv.at[layer, 1],
                device_id=partner, device_id_type=MESH,
            ).start()

    def weights_in(layer):
        landed(WP.at[layer, pl.ds(0, 192)], w_local.at[layer, 0])
        landed(WP.at[layer, pl.ds(0, 192)], w_recv.at[layer, 0])
        landed(WO.at[layer, pl.ds(0, 32)], w_local.at[layer, 1])
        landed(WO.at[layer, pl.ds(0, 32)], w_recv.at[layer, 1])
        scale = gain[layer:layer + 1, :]

        def fold(i, carry):
            rows = pl.ds(pl.multiple_of(i * 16, 16), 16)
            WP[layer, rows, :] = (WP[layer, rows, :].astype(F32) * scale).astype(BF16)
            return carry

        lax.fori_loop(0, 24, fold, 0)

    def weights_sent():
        for layer in range(2):
            landed(WP.at[layer, pl.ds(0, 192)], w_send.at[layer, 0])
            landed(WO.at[layer, pl.ds(0, 32)], w_send.at[layer, 1])

    def put_projected(layer, projected):
        out = projected.astype(BF16)
        for to in range(4):
            SB[layer, to, 0:16, :] = out[to * 16:to * 16 + 16, :]
            SB[layer, to, 16:32, :] = out[64 + to * 16:64 + to * 16 + 16, :]

    def project_first():
        acc = jnp.zeros((128, 384), F32)
        squares = jnp.zeros((128, 128), F32)
        for z in range(4):
            parts = rows_chunk(0, z)
            for part in parts:
                wide = part.astype(F32)
                squares += wide * wide
            acc += lax.dot_general(
                jnp.concatenate(parts, axis=1), WP[0, :, z * 1024:(z + 1) * 1024], LANES,
                preferred_element_type=F32,
            )
        factor = lax.rsqrt(jnp.sum(squares, axis=1, keepdims=True) * (1.0 / 4096) + RMS_EPS)
        put_projected(0, acc * factor)

    def project_second():
        acc = jnp.zeros((384, 128), F32)
        squares = jnp.zeros((16, 128), F32)
        for z in range(4):
            parts = [G[2, q, z, y, x] for y in range(4) for x in range(4) for q in range(4)]
            for part in parts:
                wide = part.astype(F32)
                squares += wide * wide
            acc += lax.dot_general(
                WP[1, :, z * 1024:(z + 1) * 1024], jnp.concatenate(parts, axis=0), PLAIN,
                preferred_element_type=F32,
            )
        factor = lax.rsqrt(jnp.sum(squares, axis=0, keepdims=True) * (1.0 / 4096) + RMS_EPS)
        put_projected(1, (acc * factor).T)

    ident = lax.broadcasted_iota(jnp.int32, (32, 32), 0) == lax.broadcasted_iota(jnp.int32, (32, 32), 1)
    length = jnp.sum(jnp.where(ident, jnp.broadcast_to(lens[0:1, :], (32, 32)), 0), axis=1, keepdims=True)
    active = length > STEP

    def wide128(value):
        return jnp.concatenate([value, jnp.zeros_like(value)], axis=1)

    def recur(layer, a):
        values, gates, first_sums, second_sums = [], [], [], []
        for h in range(4):
            take = lambda kind: RB[layer, h, :, kind * 64:(kind + 1) * 64].astype(F32)
            recept, key, value, dpre, rpre, gpre = [take(kind) for kind in range(6)]
            cols = slice(h * 64, (h + 1) * 64)
            decay = jnp.exp(-(0.6065306597126334 * jax.nn.sigmoid(dbase[layer:layer + 1, cols] + dpre)))
            rate = jax.nn.sigmoid(rbase[layer:layer + 1, cols] + rpre)
            norm = jnp.sqrt(jnp.sum(key * key, axis=1, keepdims=True))
            unit = key / jnp.maximum(norm, 1e-12)
            up, kp = unit * rate, key * rate
            first_sums.append(jnp.broadcast_to(jnp.sum(up * recept, axis=1, keepdims=True), (32, 64)))
            second_sums.append(jnp.broadcast_to(jnp.sum(kp * recept, axis=1, keepdims=True), (32, 64)))
            values.append(value)
            gates.append(jax.nn.sigmoid(gpre))
            V8[pl.ds(h, 32, stride=8), :] = wide128(-unit)
            V8[pl.ds(4 + h, 32, stride=8), :] = wide128(decay * recept)
            PQ[pl.ds(h, 32, stride=8), :] = wide128(jnp.where(active, up, 0.0))
            PQ[pl.ds(4 + h, 32, stride=8), :] = wide128(jnp.where(active, kp, 0.0))
            DEC[pl.ds(h, 32, stride=8), :] = wide128(jnp.where(active, decay, 1.0))
        for b in range(32):
            got = lax.dot_general(
                V8[b * 8:(b + 1) * 8, 0:64].astype(BF16),
                ST[layer, b].reshape(256, 64).astype(BF16), LANES,
                preferred_element_type=F32,
            )
            for half in range(2):
                M2[half, b * 8:(b + 1) * 8, :] = got[:, half * 128:(half + 1) * 128]
        low = lax.broadcasted_iota(jnp.int32, (32, 128), 1) < 64

        def heads(base):
            return jnp.concatenate([
                jnp.where(low, M2[half, pl.ds(base + 2 * half, 32, stride=8), :],
                          M2[half, pl.ds(base + 2 * half + 1, 32, stride=8), :])
                for half in range(2)
            ], axis=1)

        sa, direct = heads(0), heads(4)
        value = jnp.concatenate(values, axis=1)
        SA[...] = sa
        VA[...] = value
        readout = direct + sa * jnp.concatenate(first_sums, axis=1) + value * jnp.concatenate(second_sums, axis=1)
        normal = []
        for h in range(4):
            seg = readout[:, h * 64:(h + 1) * 64]
            seg = seg - jnp.sum(seg, axis=1, keepdims=True) * (1.0 / 64)
            spread = jnp.sum(seg * seg, axis=1, keepdims=True) * (1.0 / 64)
            normal.append(seg * lax.rsqrt(spread + GROUP_EPS))
        rows = jnp.concatenate(normal, axis=1) * ggain[layer:layer + 1, :] * jnp.concatenate(gates, axis=1)
        rows = jnp.where(active, rows, 0.0).astype(BF16)
        for q in range(4):
            rh, ch = q // 2, q % 2
            G[a, q, at["z"], at["y"], at["x"]] = rows[rh * 16:(rh + 1) * 16, ch * 128:(ch + 1) * 128]

    head_of = lax.broadcasted_iota(jnp.int32, (8, 256), 1) // 64
    row_of = lax.broadcasted_iota(jnp.int32, (8, 256), 0)

    def update(layer, start, count):
        for b in range(start, start + count):
            left = jnp.where(row_of < 4, jnp.broadcast_to(SA[b:b + 1, :], (8, 256)),
                             jnp.broadcast_to(VA[b:b + 1, :], (8, 256)))
            left = jnp.where(row_of % 4 == head_of, left, 0.0)
            delta = lax.dot_general(
                left.astype(BF16), PQ[b * 8:(b + 1) * 8, 0:64].astype(BF16), ROWS,
                preferred_element_type=F32,
            )
            for h in range(4):
                ST[layer, b, h] = (ST[layer, b, h] * DEC[b * 8 + h:b * 8 + h + 1, 0:64]
                                   + delta[h * 64:(h + 1) * 64, :])

    gather_first(0)
    for layer in range(2):
        pltpu.make_async_copy(state.at[layer], ST.at[layer], st_sem.at[layer]).start()

    @pl.when(c == 1)
    def _():
        weights_out()

    gather_middle(0)

    @pl.when(c == 0)
    def _():
        pl.semaphore_wait(barrier, 1)
        weights_out()

    weights_in(0)
    gather_last(0)
    project_first()
    exchange(0, SB.at[0], RB.at[0])
    landed(ST.at[0], st_sem.at[0])
    recur(0, 1)

    gather_first(1)
    update(0, 0, 10)
    gather_middle(1)
    update(0, 10, 22)
    weights_in(1)
    gather_last(1)
    acc = jnp.zeros((64, 128), F32)
    for z in range(4):
        acc += lax.dot_general(
            WO[0, :, z * 1024:(z + 1) * 1024], jnp.concatenate(rows_chunk(1, z), axis=1), LANES,
            preferred_element_type=F32,
        )
    out = acc.astype(BF16)
    for q in range(4):
        G[2, q, at["z"], at["y"], at["x"]] = out[q * 16:(q + 1) * 16, :]

    gather_first(2)
    gather_middle(2)
    gather_last(2)
    project_second()
    exchange(1, SB.at[1], RB.at[1])
    landed(ST.at[1], st_sem.at[1])
    recur(1, 3)

    gather_first(3)
    update(1, 0, 10)
    gather_middle(3)
    update(1, 10, 22)
    gather_last(3)
    acc = jnp.zeros((128, 64), F32)
    for z in range(4):
        acc += lax.dot_general(
            jnp.concatenate(rows_chunk(3, z), axis=1), WO[1, :, z * 1024:(z + 1) * 1024], LANES,
            preferred_element_type=F32,
        )
    out = wide128(acc).astype(BF16)
    for to in range(4):
        FB[to, 0:16, :] = out[to * 16:to * 16 + 16, :]
        FB[to, 16:32, :] = out[64 + to * 16:64 + to * 16 + 16, :]
    exchange(2, FB, FR)
    mixed[...] = jnp.concatenate([FR[h, :, 0:64] for h in range(4)], axis=1)

    for a in range(4):
        gather_sent(a)
    exchange_sent(0, SB.at[0])
    exchange_sent(1, SB.at[1])
    exchange_sent(2, FB)
    weights_sent()


def local(tokens, lengths, norm_gain, w_recept, w_key, w_value, w_decay, w_rate, w_gate, w_out,
          decay_base, rate_base, group_gain, state):
    weights = [jnp.swapaxes(w, 1, 2) for w in (w_recept, w_key, w_value, w_decay, w_rate, w_gate, w_out)]
    hbm = pl.BlockSpec(memory_space=pltpu.HBM)
    vmem = pl.BlockSpec(memory_space=pltpu.VMEM)
    mixed, new_state = pl.pallas_call(
        step_kernel,
        out_shape=(jax.ShapeDtypeStruct((32, 256), BF16), pltpu.VMEM(state.shape, F32)),
        in_specs=[hbm, vmem, vmem] + [hbm] * 7 + [vmem] * 3 + [hbm],
        out_specs=(vmem, vmem),
        scratch_shapes=[
            pltpu.VMEM((4, 4, 4, 4, 4, 16, 128), BF16),
            pltpu.VMEM((2, 384, 4096), BF16),
            pltpu.VMEM((2, 64, 4096), BF16),
            pltpu.VMEM((2, 4, 32, 384), BF16),
            pltpu.VMEM((2, 4, 32, 384), BF16),
            pltpu.VMEM((4, 32, 128), BF16),
            pltpu.VMEM((4, 32, 128), BF16),
            pltpu.VMEM((256, 128), F32),
            pltpu.VMEM((2, 256, 128), F32),
            pltpu.VMEM((32, 256), F32),
            pltpu.VMEM((32, 256), F32),
            pltpu.VMEM((256, 128), F32),
            pltpu.VMEM((256, 128), F32),
            pltpu.SemaphoreType.DMA((4, 4, 3)),
            pltpu.SemaphoreType.DMA((4, 4, 5)),
            pltpu.SemaphoreType.DMA((3,)),
            pltpu.SemaphoreType.DMA((3,)),
            pltpu.SemaphoreType.DMA((2, 2)),
            pltpu.SemaphoreType.DMA((2, 2)),
            pltpu.SemaphoreType.DMA((2, 2)),
            pltpu.SemaphoreType.DMA((2,)),
            pltpu.SemaphoreType.DMA((4,)),
        ],
        compiler_params=pltpu.CompilerParams(collective_id=0, has_side_effects=True, vmem_limit_bytes=52 << 20),
        name="decode_step",
    )(tokens, lengths.reshape(1, 32), norm_gain, *weights, decay_base, rate_base, group_gain, state)
    return mixed, new_state


def solution(mesh):
    both = P(None, None, ("tp", "dp"))
    in_specs = (
        P("dp", "tp"), P("dp"), P(), both, both, both, both, both, both, both,
        P(None, "tp"), P(None, "tp"), P(None, "tp"), P(None, "dp", "tp", None, None),
    )
    out_specs = (P("dp", "tp"), P(None, "dp", "tp", None, None))
    return jax.shard_map(local, mesh=mesh, in_specs=in_specs, out_specs=out_specs, check_vma=False)
```

```python
import functools

import jax
import jax.numpy as jnp
from jax import lax
from jax.experimental import pallas as pl
from jax.experimental.pallas import tpu as pltpu
from jax.sharding import PartitionSpec as P

STEP = 16
RMS_EPS = 1e-06
GROUP_EPS = 0.00064
MESH = pl.DeviceIdType.MESH
F32 = jnp.float32
BF16 = jnp.bfloat16
ORDERS = (("x", "y", "z"), ("y", "z", "x"), ("z", "x", "y"), ("y", "x", "z"))
LANES = (((1,), (1,)), ((), ()))
PLAIN = (((1,), (0,)), ((), ()))
ROWS = (((0,), (0,)), ((), ()))


def step_kernel(
    tok, lens_in, gain_in, w0, w1, w2, w3, w4, w5, w_out, dbase_in, rbase_in, ggain_in, state,
    mixed, ST,
    G, WP, WO, SB, RB, FB, FR, V8, M2, SA, VA, PQ, DEC, lens, gain, dbase, rbase, ggain,
    g_send, g_recv, a_send, a_recv, w_local, w_send, w_recv, st_sem, tok_sem, small_sem,
):
    tp, dp = lax.axis_index("tp"), lax.axis_index("dp")
    c = dp % 2
    at = {"z": tp // 4, "y": tp % 4, "x": dp // 2}
    projections = (w0, w1, w2, w3, w4, w5)

    def device(**hops):
        to = {axis: (at[axis] + hops.get(axis, 0)) % 4 for axis in "xyz"}
        return (to["z"] * 4 + to["y"], to["x"] * 2 + c)

    partner = (tp, at["x"] * 2 + 1 - c)

    barrier = pltpu.get_barrier_semaphore()
    peers = [
        dict(x=hx, y=hy, z=hz) for hx in range(4) for hy in range(4) for hz in range(4)
        if 0 in (hx, hy, hz) and (hx, hy, hz) != (0, 0, 0)
    ]
    for peer in peers:
        pl.semaphore_signal(barrier, inc=1, device_id=device(**peer), device_id_type=MESH)
    pl.semaphore_signal(barrier, inc=1, device_id=partner, device_id_type=MESH)

    tok_copies = []
    for q in range(4):
        rh, ch = q // 2, q % 2
        tok_copies.append(pltpu.make_async_copy(
            tok.at[pl.ds(rh * 16, 16), pl.ds(ch * 128, 128)],
            G.at[0, q, at["z"], at["y"], at["x"]],
            tok_sem.at[q],
        ))
        tok_copies[-1].start()
    mine = pl.multiple_of(c * 32, 32)

    def weights_local(layer):
        for kind in range(6):
            pltpu.make_async_copy(
                projections[kind].at[layer],
                WP.at[layer, pl.ds(kind * 64 + mine, 32)],
                w_local.at[layer, 0],
            ).start()
        pltpu.make_async_copy(
            w_out.at[layer], WO.at[layer, pl.ds(mine, 32)], w_local.at[layer, 1]
        ).start()

    small = [
        pltpu.make_async_copy(src, dst, small_sem.at[i])
        for i, (src, dst) in enumerate(
            ((lens_in, lens), (gain_in, gain), (dbase_in, dbase), (rbase_in, rbase), (ggain_in, ggain)))
    ]
    for copy in small:
        copy.start()
    weights_local(0)
    pl.semaphore_wait(barrier, len(peers) + 1)

    def block(a, q, free, moved=None):
        idx = [moved[ax] if moved and ax in moved else at[ax] for ax in "zyx"]
        idx = [slice(None) if ax in free else i for ax, i in zip("zyx", idx)]
        return G.at[(a, q, *idx)]

    def send(ref, send_sem, recv_sem, **hops):
        pltpu.make_async_remote_copy(
            src_ref=ref, dst_ref=ref, send_sem=send_sem, recv_sem=recv_sem,
            device_id=device(**hops), device_id_type=MESH,
        ).start()

    def landed(ref, sem):
        pltpu.make_async_copy(ref, ref, sem).wait()

    def gather_first(a):
        for q in range(4):
            first, second, third = ORDERS[q]
            if a == 0:
                tok_copies[q].wait()
            for hop in (2, 1, 3):
                send(block(a, q, ()), g_send.at[a, q, 0], g_recv.at[a, q, 0], **{first: hop})
            for over in (2, 1, 3):
                for hop in (2, 1, 3, 0):
                    send(block(a, q, ()), g_send.at[a, q, 1], g_recv.at[a, q, over],
                         **{first: hop, second: over})

    def gather_middle(a):
        for q in range(4):
            first, second, third = ORDERS[q]
            landed(G.at[a, q, 0, 0, pl.ds(0, 3)], g_recv.at[a, q, 0])
            for on in (2, 1, 3):
                send(block(a, q, first), g_send.at[a, q, 2], g_recv.at[a, q, 4], **{third: on})
        for over in (1, 3, 2):
            for q in range(4):
                first, second, third = ORDERS[q]
                landed(G.at[a, q, 0, 0], g_recv.at[a, q, over])
                line = {second: (at[second] + 4 - over) % 4}
                for on in (2, 1, 3):
                    send(block(a, q, first, line), g_send.at[a, q, 2], g_recv.at[a, q, 4], **{third: on})

    def gather_last(a):
        for q in range(4):
            landed(G.at[a, q, pl.ds(0, 3)], g_recv.at[a, q, 4])

    def gather_sent(a):
        for q in range(4):
            landed(G.at[a, q, 0, 0, pl.ds(0, 3)], g_send.at[a, q, 0])
            landed(G.at[a, q, pl.ds(0, 3), :, 0], g_send.at[a, q, 1])
            landed(G.at[a, q, pl.ds(0, 3)], g_send.at[a, q, 2])

    def rows_chunk(a, z):
        parts = []
        for y in range(4):
            for ch in range(2):
                halves = [G[a, rh * 2 + ch, z, y].reshape(64, 128) for rh in range(2)]
                parts.append(jnp.concatenate(halves, axis=0))
        return parts

    def exchange_start(n, src, dst):
        for hop in (2, 1, 3):
            to = (at["x"] + hop) % 4
            pltpu.make_async_remote_copy(
                src_ref=src.at[to], dst_ref=dst.at[at["x"]],
                send_sem=a_send.at[n], recv_sem=a_recv.at[n],
                device_id=device(x=hop), device_id_type=MESH,
            ).start()
        dst[at["x"]] = src[at["x"]]

    def exchange_done(n, dst):
        landed(dst.at[pl.ds(0, 3)], a_recv.at[n])

    def exchange_sent(n, src):
        landed(src.at[pl.ds(0, 3)], a_send.at[n])

    def projections_out(layer):
        for kind in range(6):
            pltpu.make_async_remote_copy(
                src_ref=projections[kind].at[layer],
                dst_ref=WP.at[layer, pl.ds(kind * 64 + mine, 32)],
                send_sem=w_send.at[layer, 0], recv_sem=w_recv.at[layer, 0],
                device_id=partner, device_id_type=MESH,
            ).start()

    def output_out(layer):
        pltpu.make_async_remote_copy(
            src_ref=w_out.at[layer],
            dst_ref=WO.at[layer, pl.ds(mine, 32)],
            send_sem=w_send.at[layer, 1], recv_sem=w_recv.at[layer, 1],
            device_id=partner, device_id_type=MESH,
        ).start()

    def projections_in(layer):
        landed(WP.at[layer, pl.ds(0, 192)], w_local.at[layer, 0])
        landed(WP.at[layer, pl.ds(0, 192)], w_recv.at[layer, 0])
        scale = gain[layer:layer + 1, :]

        def fold(i, carry):
            rows = pl.ds(pl.multiple_of(i * 16, 16), 16)
            WP[layer, rows, :] = (WP[layer, rows, :].astype(F32) * scale).astype(BF16)
            return carry

        lax.fori_loop(0, 24, fold, 0)

    def output_in(layer):
        landed(WO.at[layer, pl.ds(0, 32)], w_local.at[layer, 1])
        landed(WO.at[layer, pl.ds(0, 32)], w_recv.at[layer, 1])

    def weights_sent():
        for layer in range(2):
            landed(WP.at[layer, pl.ds(0, 192)], w_send.at[layer, 0])
            landed(WO.at[layer, pl.ds(0, 32)], w_send.at[layer, 1])

    def put_projected(layer, projected):
        out = projected.astype(BF16)
        for to in range(4):
            SB[layer, to, 0:16, :] = out[to * 16:to * 16 + 16, :]
            SB[layer, to, 16:32, :] = out[64 + to * 16:64 + to * 16 + 16, :]

    def project_first():
        acc = jnp.zeros((128, 384), F32)
        squares = jnp.zeros((128, 128), F32)
        for z in range(4):
            parts = rows_chunk(0, z)
            for part in parts:
                wide = part.astype(F32)
                squares += wide * wide
            acc += lax.dot_general(
                jnp.concatenate(parts, axis=1), WP[0, :, z * 1024:(z + 1) * 1024], LANES,
                preferred_element_type=F32,
            )
        factor = lax.rsqrt(jnp.sum(squares, axis=1, keepdims=True) * (1.0 / 4096) + RMS_EPS)
        put_projected(0, acc * factor)

    def project_second():
        acc = jnp.zeros((384, 128), F32)
        squares = jnp.zeros((16, 128), F32)
        for z in range(4):
            parts = [G[2, q, z, y, x] for y in range(4) for x in range(4) for q in range(4)]
            for part in parts:
                wide = part.astype(F32)
                squares += wide * wide
            acc += lax.dot_general(
                WP[1, :, z * 1024:(z + 1) * 1024], jnp.concatenate(parts, axis=0), PLAIN,
                preferred_element_type=F32,
            )
        factor = lax.rsqrt(jnp.sum(squares, axis=0, keepdims=True) * (1.0 / 4096) + RMS_EPS)
        put_projected(1, (acc * factor).T)

    def active_rows():
        row = lax.broadcasted_iota(jnp.int32, (32, 32), 0)
        col = lax.broadcasted_iota(jnp.int32, (32, 32), 1)
        spread = jnp.broadcast_to(lens[0:1, :], (32, 32))
        return jnp.sum(jnp.where(row == col, spread, 0), axis=1, keepdims=True) > STEP

    def wide128(value):
        return jnp.concatenate([value, jnp.zeros_like(value)], axis=1)

    def recur(layer, a):
        active = active_rows()
        values, gates, first_sums, second_sums = [], [], [], []
        for h in range(4):
            take = lambda kind: RB[layer, h, :, kind * 64:(kind + 1) * 64].astype(F32)
            recept, key, value, dpre, rpre, gpre = [take(kind) for kind in range(6)]
            cols = slice(h * 64, (h + 1) * 64)
            decay = jnp.exp(-(0.6065306597126334 * jax.nn.sigmoid(dbase[layer:layer + 1, cols] + dpre)))
            rate = jax.nn.sigmoid(rbase[layer:layer + 1, cols] + rpre)
            norm = jnp.sqrt(jnp.sum(key * key, axis=1, keepdims=True))
            unit = key / jnp.maximum(norm, 1e-12)
            up, kp = unit * rate, key * rate
            first_sums.append(jnp.broadcast_to(jnp.sum(up * recept, axis=1, keepdims=True), (32, 64)))
            second_sums.append(jnp.broadcast_to(jnp.sum(kp * recept, axis=1, keepdims=True), (32, 64)))
            values.append(value)
            gates.append(jax.nn.sigmoid(gpre))
            V8[pl.ds(h, 32, stride=8), :] = wide128(-unit)
            V8[pl.ds(4 + h, 32, stride=8), :] = wide128(decay * recept)
            PQ[pl.ds(h, 32, stride=8), :] = wide128(jnp.where(active, up, 0.0))
            PQ[pl.ds(4 + h, 32, stride=8), :] = wide128(jnp.where(active, kp, 0.0))
            DEC[pl.ds(h, 32, stride=8), :] = wide128(jnp.where(active, decay, 1.0))
        for b in range(32):
            got = lax.dot_general(
                V8[b * 8:(b + 1) * 8, 0:64].astype(BF16),
                ST[layer, b].reshape(256, 64).astype(BF16), LANES,
                preferred_element_type=F32,
            )
            for half in range(2):
                M2[half, b * 8:(b + 1) * 8, :] = got[:, half * 128:(half + 1) * 128]
        low = lax.broadcasted_iota(jnp.int32, (32, 128), 1) < 64

        def heads(base):
            return jnp.concatenate([
                jnp.where(low, M2[half, pl.ds(base + 2 * half, 32, stride=8), :],
                          M2[half, pl.ds(base + 2 * half + 1, 32, stride=8), :])
                for half in range(2)
            ], axis=1)

        sa, direct = heads(0), heads(4)
        value = jnp.concatenate(values, axis=1)
        SA[...] = sa
        VA[...] = value
        readout = direct + sa * jnp.concatenate(first_sums, axis=1) + value * jnp.concatenate(second_sums, axis=1)
        normal = []
        for h in range(4):
            seg = readout[:, h * 64:(h + 1) * 64]
            seg = seg - jnp.sum(seg, axis=1, keepdims=True) * (1.0 / 64)
            spread = jnp.sum(seg * seg, axis=1, keepdims=True) * (1.0 / 64)
            normal.append(seg * lax.rsqrt(spread + GROUP_EPS))
        rows = jnp.concatenate(normal, axis=1) * ggain[layer:layer + 1, :] * jnp.concatenate(gates, axis=1)
        rows = jnp.where(active, rows, 0.0).astype(BF16)
        for q in range(4):
            rh, ch = q // 2, q % 2
            G[a, q, at["z"], at["y"], at["x"]] = rows[rh * 16:(rh + 1) * 16, ch * 128:(ch + 1) * 128]

    head_of = lax.broadcasted_iota(jnp.int32, (8, 256), 1) // 64
    row_of = lax.broadcasted_iota(jnp.int32, (8, 256), 0)

    def update(layer, start, count):
        for b in range(start, start + count):
            left = jnp.where(row_of < 4, jnp.broadcast_to(SA[b:b + 1, :], (8, 256)),
                             jnp.broadcast_to(VA[b:b + 1, :], (8, 256)))
            left = jnp.where(row_of % 4 == head_of, left, 0.0)
            delta = lax.dot_general(
                left.astype(BF16), PQ[b * 8:(b + 1) * 8, 0:64].astype(BF16), ROWS,
                preferred_element_type=F32,
            )
            for h in range(4):
                ST[layer, b, h] = (ST[layer, b, h] * DEC[b * 8 + h:b * 8 + h + 1, 0:64]
                                   + delta[h * 64:(h + 1) * 64, :])

    def output_first():
        acc = jnp.zeros((64, 128), F32)
        for z in range(4):
            acc += lax.dot_general(
                WO[0, :, z * 1024:(z + 1) * 1024], jnp.concatenate(rows_chunk(1, z), axis=1), LANES,
                preferred_element_type=F32,
            )
        out = acc.astype(BF16)
        for q in range(4):
            G[2, q, at["z"], at["y"], at["x"]] = out[q * 16:(q + 1) * 16, :]

    def output_second():
        acc = jnp.zeros((128, 64), F32)
        for z in range(4):
            acc += lax.dot_general(
                jnp.concatenate(rows_chunk(3, z), axis=1), WO[1, :, z * 1024:(z + 1) * 1024], LANES,
                preferred_element_type=F32,
            )
        out = wide128(acc).astype(BF16)
        for to in range(4):
            FB[to, 0:16, :] = out[to * 16:to * 16 + 16, :]
            FB[to, 16:32, :] = out[64 + to * 16:64 + to * 16 + 16, :]

    gather_first(0)
    projections_out(0)
    pltpu.make_async_copy(state.at[0], ST.at[0], st_sem.at[0]).start()
    weights_local(1)
    pltpu.make_async_copy(state.at[1], ST.at[1], st_sem.at[1]).start()
    gather_middle(0)
    for copy in small:
        copy.wait()
    projections_in(0)
    gather_last(0)
    project_first()
    exchange_start(0, SB.at[0], RB.at[0])
    output_out(0)
    projections_out(1)
    output_out(1)
    exchange_done(0, RB.at[0])
    landed(ST.at[0], st_sem.at[0])
    recur(0, 1)
    gather_first(1)
    update(0, 0, 32)
    gather_middle(1)
    projections_in(1)
    output_in(0)
    output_in(1)
    gather_last(1)
    output_first()
    gather_first(2)
    gather_middle(2)
    gather_last(2)
    project_second()
    exchange_start(1, SB.at[1], RB.at[1])
    exchange_done(1, RB.at[1])
    landed(ST.at[1], st_sem.at[1])
    recur(1, 3)
    gather_first(3)
    update(1, 0, 32)
    gather_middle(3)
    gather_last(3)
    output_second()
    exchange_start(2, FB, FR)
    exchange_done(2, FR)
    mixed[...] = jnp.concatenate([FR[h, :, 0:64] for h in range(4)], axis=1)
    for a in range(4):
        gather_sent(a)
    exchange_sent(0, SB.at[0])
    exchange_sent(1, SB.at[1])
    exchange_sent(2, FB)
    weights_sent()


def local(tokens, lengths, norm_gain, w_recept, w_key, w_value, w_decay, w_rate, w_gate, w_out,
          decay_base, rate_base, group_gain, state):
    weights = [jnp.swapaxes(w, 1, 2) for w in (w_recept, w_key, w_value, w_decay, w_rate, w_gate, w_out)]
    hbm = pl.BlockSpec(memory_space=pltpu.HBM)
    vmem = pl.BlockSpec(memory_space=pltpu.VMEM)
    mixed, new_state = pl.pallas_call(
        step_kernel,
        out_shape=(jax.ShapeDtypeStruct((32, 256), BF16), pltpu.VMEM(state.shape, F32)),
        in_specs=[hbm] * 14,
        out_specs=(vmem, vmem),
        scratch_shapes=[
            pltpu.VMEM((4, 4, 4, 4, 4, 16, 128), BF16),
            pltpu.VMEM((2, 384, 4096), BF16),
            pltpu.VMEM((2, 64, 4096), BF16),
            pltpu.VMEM((2, 4, 32, 384), BF16),
            pltpu.VMEM((2, 4, 32, 384), BF16),
            pltpu.VMEM((4, 32, 128), BF16),
            pltpu.VMEM((4, 32, 128), BF16),
            pltpu.VMEM((256, 128), F32),
            pltpu.VMEM((2, 256, 128), F32),
            pltpu.VMEM((32, 256), F32),
            pltpu.VMEM((32, 256), F32),
            pltpu.VMEM((256, 128), F32),
            pltpu.VMEM((256, 128), F32),
            pltpu.VMEM((1, 32), jnp.int32),
            pltpu.VMEM((2, 4096), F32),
            pltpu.VMEM((2, 256), F32),
            pltpu.VMEM((2, 256), F32),
            pltpu.VMEM((2, 256), F32),
            pltpu.SemaphoreType.DMA((4, 4, 3)),
            pltpu.SemaphoreType.DMA((4, 4, 5)),
            pltpu.SemaphoreType.DMA((3,)),
            pltpu.SemaphoreType.DMA((3,)),
            pltpu.SemaphoreType.DMA((2, 2)),
            pltpu.SemaphoreType.DMA((2, 2)),
            pltpu.SemaphoreType.DMA((2, 2)),
            pltpu.SemaphoreType.DMA((2,)),
            pltpu.SemaphoreType.DMA((4,)),
            pltpu.SemaphoreType.DMA((5,)),
        ],
        compiler_params=pltpu.CompilerParams(collective_id=0, has_side_effects=True, vmem_limit_bytes=52 << 20),
        name="decode_step",
    )(tokens, lengths.reshape(1, 32), norm_gain, *weights, decay_base, rate_base, group_gain, state)
    return mixed, new_state


def solution(mesh):
    both = P(None, None, ("tp", "dp"))
    in_specs = (
        P("dp", "tp"), P("dp"), P(), both, both, both, both, both, both, both,
        P(None, "tp"), P(None, "tp"), P(None, "tp"), P(None, "dp", "tp", None, None),
    )
    out_specs = (P("dp", "tp"), P(None, "dp", "tp", None, None))
    return jax.shard_map(local, mesh=mesh, in_specs=in_specs, out_specs=out_specs, check_vma=False)
```

```python
import functools

import jax
import jax.numpy as jnp
from jax import lax
from jax.experimental import pallas as pl
from jax.experimental.pallas import tpu as pltpu
from jax.sharding import PartitionSpec as P

STEP = 16
RMS_EPS = 1e-06
GROUP_EPS = 0.00064
MESH = pl.DeviceIdType.MESH
F32 = jnp.float32
BF16 = jnp.bfloat16
ORDERS = (("x", "y", "z"), ("x", "z", "y"), ("x", "y", "z"), ("x", "z", "y"))
LANES = (((1,), (1,)), ((), ()))
ROWS = (((0,), (0,)), ((), ()))


def step_kernel(
    tok, lens_in, gain_in, w0, w1, w2, w3, w4, w5, w_out, dbase_in, rbase_in, ggain_in, state,
    mixed, ST,
    G, GP, WP, WO, SB, RB, V8, M2, SA, VA, PQ, DEC, lens, gain, dbase, rbase, ggain,
    g_send, g_recv, p_send, p_recv, a_send, a_recv, w_local, w_send, w_recv, o_sem, st_sem, tok_sem, small_sem,
):
    tp, dp = lax.axis_index("tp"), lax.axis_index("dp")
    c = dp % 2
    at = {"z": tp // 4, "y": tp % 4, "x": dp // 2}
    projections = (w0, w1, w2, w3, w4, w5)

    def device(**hops):
        to = {axis: (at[axis] + hops.get(axis, 0)) % 4 for axis in "xyz"}
        return (to["z"] * 4 + to["y"], to["x"] * 2 + c)

    partner = (tp, at["x"] * 2 + 1 - c)

    barrier = pltpu.get_barrier_semaphore()
    peers = [
        dict(x=hx, y=hy, z=hz) for hx in range(4) for hy in range(4) for hz in range(4)
        if 0 in (hx, hy, hz) and (hx, hy, hz) != (0, 0, 0)
    ]
    for peer in peers:
        pl.semaphore_signal(barrier, inc=1, device_id=device(**peer), device_id_type=MESH)
    pl.semaphore_signal(barrier, inc=1, device_id=partner, device_id_type=MESH)

    tok_copies = []
    for q in range(4):
        rh, ch = q // 2, q % 2
        tok_copies.append(pltpu.make_async_copy(
            tok.at[pl.ds(rh * 16, 16), pl.ds(ch * 128, 128)],
            G.at[0, q, at["z"], at["y"], at["x"]],
            tok_sem.at[q],
        ))
        tok_copies[-1].start()
    mine = pl.multiple_of(c * 32, 32)
    own_cols = pl.multiple_of(dp * 32, 32)

    def weights_local(layer):
        for kind in range(6):
            pltpu.make_async_copy(
                projections[kind].at[layer],
                WP.at[layer, pl.ds(kind * 64 + mine, 32)],
                w_local.at[layer],
            ).start()
        pltpu.make_async_copy(w_out.at[layer], WO.at[layer, pl.ds(own_cols, 32)], o_sem.at[layer, 0]).start()

    small = [
        pltpu.make_async_copy(src, dst, small_sem.at[i])
        for i, (src, dst) in enumerate(
            ((lens_in, lens), (gain_in, gain), (dbase_in, dbase), (rbase_in, rbase), (ggain_in, ggain)))
    ]
    for copy in small:
        copy.start()
    weights_local(0)
    pl.semaphore_wait(barrier, len(peers) + 1)

    def block(a, q, free, moved=None):
        idx = [moved[ax] if moved and ax in moved else at[ax] for ax in "zyx"]
        idx = [slice(None) if ax in free else i for ax, i in zip("zyx", idx)]
        return G.at[(a, q, *idx)]

    def send(ref, send_sem, recv_sem, **hops):
        pltpu.make_async_remote_copy(
            src_ref=ref, dst_ref=ref, send_sem=send_sem, recv_sem=recv_sem,
            device_id=device(**hops), device_id_type=MESH,
        ).start()

    def landed(ref, sem):
        pltpu.make_async_copy(ref, ref, sem).wait()

    def gather_first(a):
        for q in range(4):
            first, second, third = ORDERS[q]
            if a == 0:
                tok_copies[q].wait()
            for hop in (2, 1, 3):
                send(block(a, q, ()), g_send.at[a, q, 0], g_recv.at[a, q, 0], **{first: hop})
            for over in (2, 1, 3):
                for hop in (2, 1, 3, 0):
                    send(block(a, q, ()), g_send.at[a, q, 1], g_recv.at[a, q, over],
                         **{first: hop, second: over})

    def gather_middle(a):
        for q in range(4):
            first, second, third = ORDERS[q]
            landed(G.at[a, q, 0, 0, pl.ds(0, 3)], g_recv.at[a, q, 0])
            for on in (2, 1, 3):
                send(block(a, q, first), g_send.at[a, q, 2], g_recv.at[a, q, 4], **{third: on})
        for over in (1, 3, 2):
            for q in range(4):
                first, second, third = ORDERS[q]
                landed(G.at[a, q, 0, 0], g_recv.at[a, q, over])
                line = {second: (at[second] + 4 - over) % 4}
                for on in (2, 1, 3):
                    send(block(a, q, first, line), g_send.at[a, q, 2], g_recv.at[a, q, 4], **{third: on})

    def gather_last(a):
        for q in range(4):
            landed(G.at[a, q, pl.ds(0, 3)], g_recv.at[a, q, 4])

    def gather_sent(a):
        for q in range(4):
            landed(G.at[a, q, 0, 0, pl.ds(0, 3)], g_send.at[a, q, 0])
            landed(G.at[a, q, pl.ds(0, 3), :, 0], g_send.at[a, q, 1])
            landed(G.at[a, q, pl.ds(0, 3)], g_send.at[a, q, 2])

    def rows_chunk(a, z):
        parts = []
        for y in range(4):
            for ch in range(2):
                halves = [G[a, rh * 2 + ch, z, y].reshape(64, 128) for rh in range(2)]
                parts.append(jnp.concatenate(halves, axis=0))
        return parts

    def exchange_start(n, src, dst):
        for hop in (2, 1, 3):
            to = (at["x"] + hop) % 4
            pltpu.make_async_remote_copy(
                src_ref=src.at[to], dst_ref=dst.at[at["x"]],
                send_sem=a_send.at[n], recv_sem=a_recv.at[n],
                device_id=device(x=hop), device_id_type=MESH,
            ).start()
        dst[at["x"]] = src[at["x"]]

    def exchange_done(n, dst):
        landed(dst.at[pl.ds(0, 3)], a_recv.at[n])

    def exchange_sent(n, src):
        landed(src.at[pl.ds(0, 3)], a_send.at[n])

    def projections_out(layer):
        for kind in range(6):
            pltpu.make_async_remote_copy(
                src_ref=projections[kind].at[layer],
                dst_ref=WP.at[layer, pl.ds(kind * 64 + mine, 32)],
                send_sem=w_send.at[layer], recv_sem=w_recv.at[layer],
                device_id=partner, device_id_type=MESH,
            ).start()

    def output_over_x(layer):
        for part in range(4):
            for hop in (2, 1, 3):
                pltpu.make_async_remote_copy(
                    src_ref=w_out.at[layer, pl.ds(part * 8, 8)],
                    dst_ref=WO.at[layer, pl.ds(pl.multiple_of(own_cols + part * 8, 8), 8)],
                    send_sem=o_sem.at[layer, 1], recv_sem=o_sem.at[layer, 2],
                    device_id=device(x=hop), device_id_type=MESH,
                ).start()

    def output_to_partner(layer):
        pltpu.make_async_remote_copy(
            src_ref=w_out.at[layer], dst_ref=WO.at[layer, pl.ds(own_cols, 32)],
            send_sem=o_sem.at[layer, 3], recv_sem=o_sem.at[layer, 4],
            device_id=partner, device_id_type=MESH,
        ).start()

    def output_pass_on(layer):
        landed(WO.at[layer, pl.ds(0, 96)], o_sem.at[layer, 2])
        for hop in (1, 2, 3):
            cols = pl.ds(pl.multiple_of(((at["x"] + hop) % 4) * 64 + c * 32, 32), 32)
            pltpu.make_async_remote_copy(
                src_ref=WO.at[layer, cols], dst_ref=WO.at[layer, cols],
                send_sem=o_sem.at[layer, 5], recv_sem=o_sem.at[layer, 6],
                device_id=partner, device_id_type=MESH,
            ).start()

    def output_in(layer):
        landed(WO.at[layer, pl.ds(0, 32)], o_sem.at[layer, 0])
        landed(WO.at[layer, pl.ds(0, 32)], o_sem.at[layer, 4])
        landed(WO.at[layer, pl.ds(0, 96)], o_sem.at[layer, 6])

    def output_sent(layer):
        landed(WO.at[layer, pl.ds(0, 96)], o_sem.at[layer, 1])
        landed(WO.at[layer, pl.ds(0, 32)], o_sem.at[layer, 3])
        landed(WO.at[layer, pl.ds(0, 96)], o_sem.at[layer, 5])

    def projections_in(layer):
        landed(WP.at[layer, pl.ds(0, 192)], w_local.at[layer])
        landed(WP.at[layer, pl.ds(0, 192)], w_recv.at[layer])
        scale = gain[layer:layer + 1, :]

        def fold(i, carry):
            rows = pl.ds(pl.multiple_of(i * 16, 16), 16)
            WP[layer, rows, :] = (WP[layer, rows, :].astype(F32) * scale).astype(BF16)
            return carry

        lax.fori_loop(0, 24, fold, 0)

    def weights_sent():
        for layer in range(2):
            landed(WP.at[layer, pl.ds(0, 192)], w_send.at[layer])
            output_sent(layer)

    def put_projected(layer, projected):
        out = projected.astype(BF16)
        for to in range(4):
            SB[layer, to, 0:16, :] = out[to * 16:to * 16 + 16, :]
            SB[layer, to, 16:32, :] = out[64 + to * 16:64 + to * 16 + 16, :]

    def project(layer):
        acc = jnp.zeros((128, 384), F32)
        squares = jnp.zeros((128, 128), F32)
        for z in range(4):
            parts = rows_chunk(layer, z)
            for part in parts:
                wide = part.astype(F32)
                squares += wide * wide
            acc += lax.dot_general(
                jnp.concatenate(parts, axis=1), WP[layer, :, z * 1024:(z + 1) * 1024], LANES,
                preferred_element_type=F32,
            )
        factor = lax.rsqrt(jnp.sum(squares, axis=1, keepdims=True) * (1.0 / 4096) + RMS_EPS)
        put_projected(layer, acc * factor)

    def active_rows():
        row = lax.broadcasted_iota(jnp.int32, (32, 32), 0)
        col = lax.broadcasted_iota(jnp.int32, (32, 32), 1)
        spread = jnp.broadcast_to(lens[0:1, :], (32, 32))
        return jnp.sum(jnp.where(row == col, spread, 0), axis=1, keepdims=True) > STEP

    def wide128(value):
        return jnp.concatenate([value, jnp.zeros_like(value)], axis=1)

    def recur(layer):
        active = active_rows()
        values, gates, first_sums, second_sums = [], [], [], []
        for h in range(4):
            take = lambda kind: RB[layer, h, :, kind * 64:(kind + 1) * 64].astype(F32)
            recept, key, value, dpre, rpre, gpre = [take(kind) for kind in range(6)]
            cols = slice(h * 64, (h + 1) * 64)
            decay = jnp.exp(-(0.6065306597126334 * jax.nn.sigmoid(dbase[layer:layer + 1, cols] + dpre)))
            rate = jax.nn.sigmoid(rbase[layer:layer + 1, cols] + rpre)
            norm = jnp.sqrt(jnp.sum(key * key, axis=1, keepdims=True))
            unit = key / jnp.maximum(norm, 1e-12)
            up, kp = unit * rate, key * rate
            first_sums.append(jnp.broadcast_to(jnp.sum(up * recept, axis=1, keepdims=True), (32, 64)))
            second_sums.append(jnp.broadcast_to(jnp.sum(kp * recept, axis=1, keepdims=True), (32, 64)))
            values.append(value)
            gates.append(jax.nn.sigmoid(gpre))
            V8[pl.ds(h, 32, stride=8), :] = wide128(-unit)
            V8[pl.ds(4 + h, 32, stride=8), :] = wide128(decay * recept)
            PQ[pl.ds(h, 32, stride=8), :] = wide128(jnp.where(active, up, 0.0))
            PQ[pl.ds(4 + h, 32, stride=8), :] = wide128(jnp.where(active, kp, 0.0))
            DEC[pl.ds(h, 32, stride=8), :] = wide128(jnp.where(active, decay, 1.0))
        for b in range(32):
            got = lax.dot_general(
                V8[b * 8:(b + 1) * 8, 0:64].astype(BF16),
                ST[layer, b].reshape(256, 64).astype(BF16), LANES,
                preferred_element_type=F32,
            )
            for half in range(2):
                M2[half, b * 8:(b + 1) * 8, :] = got[:, half * 128:(half + 1) * 128]
        low = lax.broadcasted_iota(jnp.int32, (32, 128), 1) < 64

        def heads(base):
            return jnp.concatenate([
                jnp.where(low, M2[half, pl.ds(base + 2 * half, 32, stride=8), :],
                          M2[half, pl.ds(base + 2 * half + 1, 32, stride=8), :])
                for half in range(2)
            ], axis=1)

        sa, direct = heads(0), heads(4)
        value = jnp.concatenate(values, axis=1)
        SA[...] = sa
        VA[...] = value
        readout = direct + sa * jnp.concatenate(first_sums, axis=1) + value * jnp.concatenate(second_sums, axis=1)
        normal = []
        for h in range(4):
            seg = readout[:, h * 64:(h + 1) * 64]
            seg = seg - jnp.sum(seg, axis=1, keepdims=True) * (1.0 / 64)
            spread = jnp.sum(seg * seg, axis=1, keepdims=True) * (1.0 / 64)
            normal.append(seg * lax.rsqrt(spread + GROUP_EPS))
        rows = jnp.concatenate(normal, axis=1) * ggain[layer:layer + 1, :] * jnp.concatenate(gates, axis=1)
        rows = jnp.where(active, rows, 0.0).astype(BF16)
        for q in range(4):
            rh, ch = q // 2, q % 2
            GP[layer, tp, q] = rows[rh * 16:(rh + 1) * 16, ch * 128:(ch + 1) * 128]

    head_of = lax.broadcasted_iota(jnp.int32, (8, 256), 1) // 64
    row_of = lax.broadcasted_iota(jnp.int32, (8, 256), 0)

    def update(layer, start, count):
        for b in range(start, start + count):
            left = jnp.where(row_of < 4, jnp.broadcast_to(SA[b:b + 1, :], (8, 256)),
                             jnp.broadcast_to(VA[b:b + 1, :], (8, 256)))
            left = jnp.where(row_of % 4 == head_of, left, 0.0)
            delta = lax.dot_general(
                left.astype(BF16), PQ[b * 8:(b + 1) * 8, 0:64].astype(BF16), ROWS,
                preferred_element_type=F32,
            )
            for h in range(4):
                ST[layer, b, h] = (ST[layer, b, h] * DEC[b * 8 + h:b * 8 + h + 1, 0:64]
                                   + delta[h * 64:(h + 1) * 64, :])

    def plane_first(layer):
        here = GP.at[layer, tp]
        for hop_z in (2, 1, 3, 0):
            for hop_y in (2, 1, 3, 0):
                if hop_z or hop_y:
                    send(here, p_send.at[layer], p_recv.at[layer], z=hop_z, y=hop_y)

    def plane_last(layer):
        landed(GP.at[layer, pl.ds(0, 15)], p_recv.at[layer])

    def output(layer):
        acc = jnp.zeros((32, 256), F32)
        for z in range(4):
            parts = [
                jnp.concatenate([GP[layer, z * 4 + y, ch], GP[layer, z * 4 + y, 2 + ch]], axis=0)
                for y in range(4) for ch in range(2)
            ]
            acc += lax.dot_general(
                jnp.concatenate(parts, axis=1), WO[layer, :, z * 1024:(z + 1) * 1024], LANES,
                preferred_element_type=F32,
            )
        return acc.astype(BF16)

    gather_first(0)
    projections_out(0)
    pltpu.make_async_copy(state.at[0], ST.at[0], st_sem.at[0]).start()
    output_over_x(0)
    weights_local(1)
    pltpu.make_async_copy(state.at[1], ST.at[1], st_sem.at[1]).start()
    gather_middle(0)
    for copy in small:
        copy.wait()
    projections_in(0)
    gather_last(0)
    project(0)
    exchange_start(0, SB.at[0], RB.at[0])
    output_to_partner(0)
    projections_out(1)
    output_to_partner(1)
    exchange_done(0, RB.at[0])
    output_pass_on(0)
    landed(ST.at[0], st_sem.at[0])
    recur(0)
    plane_first(0)
    update(0, 0, 32)
    projections_in(1)
    output_in(0)
    plane_last(0)
    out = output(0)
    for q in range(4):
        rh, ch = q // 2, q % 2
        G[1, q, at["z"], at["y"], at["x"]] = out[rh * 16:(rh + 1) * 16, ch * 128:(ch + 1) * 128]
    gather_first(1)
    output_over_x(1)
    gather_middle(1)
    gather_last(1)
    project(1)
    exchange_start(1, SB.at[1], RB.at[1])
    exchange_done(1, RB.at[1])
    output_pass_on(1)
    landed(ST.at[1], st_sem.at[1])
    recur(1)
    plane_first(1)
    update(1, 0, 32)
    output_in(1)
    plane_last(1)
    mixed[...] = output(1)
    for a in range(2):
        gather_sent(a)
        exchange_sent(a, SB.at[a])
        landed(GP.at[a, pl.ds(0, 15)], p_send.at[a])
    weights_sent()


def finish_kernel(state_in, mixed_in, state_out, mixed_out, sem):
    copies = [
        pltpu.make_async_copy(state_in.at[0], state_out.at[0], sem.at[0]),
        pltpu.make_async_copy(state_in.at[1], state_out.at[1], sem.at[1]),
        pltpu.make_async_copy(mixed_in, mixed_out, sem.at[2]),
    ]
    for copy in copies:
        copy.start()
    for copy in copies:
        copy.wait()


def local(tokens, lengths, norm_gain, w_recept, w_key, w_value, w_decay, w_rate, w_gate, w_out,
          decay_base, rate_base, group_gain, state):
    weights = [jnp.swapaxes(w, 1, 2) for w in (w_recept, w_key, w_value, w_decay, w_rate, w_gate, w_out)]
    hbm = pl.BlockSpec(memory_space=pltpu.HBM)
    vmem = pl.BlockSpec(memory_space=pltpu.VMEM)
    mixed, stepped = pl.pallas_call(
        step_kernel,
        out_shape=(pltpu.VMEM((32, 256), BF16), pltpu.VMEM(state.shape, F32)),
        in_specs=[hbm] * 14,
        out_specs=(vmem, vmem),
        scratch_shapes=[
            pltpu.VMEM((2, 4, 4, 4, 4, 16, 128), BF16),
            pltpu.VMEM((2, 16, 4, 16, 128), BF16),
            pltpu.VMEM((2, 384, 4096), BF16),
            pltpu.VMEM((2, 256, 4096), BF16),
            pltpu.VMEM((2, 4, 32, 384), BF16),
            pltpu.VMEM((2, 4, 32, 384), BF16),
            pltpu.VMEM((256, 128), F32),
            pltpu.VMEM((2, 256, 128), F32),
            pltpu.VMEM((32, 256), F32),
            pltpu.VMEM((32, 256), F32),
            pltpu.VMEM((256, 128), F32),
            pltpu.VMEM((256, 128), F32),
            pltpu.VMEM((1, 32), jnp.int32),
            pltpu.VMEM((2, 4096), F32),
            pltpu.VMEM((2, 256), F32),
            pltpu.VMEM((2, 256), F32),
            pltpu.VMEM((2, 256), F32),
            pltpu.SemaphoreType.DMA((2, 4, 3)),
            pltpu.SemaphoreType.DMA((2, 4, 5)),
            pltpu.SemaphoreType.DMA((2,)),
            pltpu.SemaphoreType.DMA((2,)),
            pltpu.SemaphoreType.DMA((2,)),
            pltpu.SemaphoreType.DMA((2,)),
            pltpu.SemaphoreType.DMA((2,)),
            pltpu.SemaphoreType.DMA((2,)),
            pltpu.SemaphoreType.DMA((2,)),
            pltpu.SemaphoreType.DMA((2, 7)),
            pltpu.SemaphoreType.DMA((2,)),
            pltpu.SemaphoreType.DMA((4,)),
            pltpu.SemaphoreType.DMA((5,)),
        ],
        compiler_params=pltpu.CompilerParams(collective_id=0, has_side_effects=True, vmem_limit_bytes=52 << 20),
        name="decode_step",
    )(tokens, lengths.reshape(1, 32), norm_gain, *weights, decay_base, rate_base, group_gain, state)
    new_state, mixed = pl.pallas_call(
        finish_kernel,
        out_shape=(pltpu.HBM(state.shape, F32), pltpu.HBM((32, 256), BF16)),
        in_specs=[vmem, vmem],
        out_specs=(hbm, hbm),
        scratch_shapes=[pltpu.SemaphoreType.DMA((3,))],
        compiler_params=pltpu.CompilerParams(vmem_limit_bytes=1 << 20),
        name="finish",
    )(stepped, mixed)
    return mixed, new_state


def solution(mesh):
    both = P(None, None, ("tp", "dp"))
    in_specs = (
        P("dp", "tp"), P("dp"), P(), both, both, both, both, both, both, both,
        P(None, "tp"), P(None, "tp"), P(None, "tp"), P(None, "dp", "tp", None, None),
    )
    out_specs = (P("dp", "tp"), P(None, "dp", "tp", None, None))
    return jax.shard_map(local, mesh=mesh, in_specs=in_specs, out_specs=out_specs, check_vma=False)
```

```python
import functools

import jax
import jax.numpy as jnp
from jax import lax
from jax.experimental import pallas as pl
from jax.experimental.pallas import tpu as pltpu
from jax.sharding import PartitionSpec as P

STEP = 16
RMS_EPS = 1e-06
GROUP_EPS = 0.00064
MESH = pl.DeviceIdType.MESH
F32 = jnp.float32
BF16 = jnp.bfloat16
ORDERS = (("x", "y", "z"), ("x", "z", "y"), ("x", "y", "z"), ("x", "z", "y"))
LANES = (((1,), (1,)), ((), ()))
ROWS = (((0,), (0,)), ((), ()))


def output_product(rows, weight):
    acc = jnp.zeros((32, 256), F32)
    for z in range(4):
        parts = [
            jnp.concatenate([rows[z * 4 + y, ch], rows[z * 4 + y, 2 + ch]], axis=0)
            for y in range(4) for ch in range(2)
        ]
        acc += lax.dot_general(
            jnp.concatenate(parts, axis=1), weight[:, z * 1024:(z + 1) * 1024], LANES,
            preferred_element_type=F32,
        )
    return acc.astype(BF16)


def step_kernel(
    tok, lens_in, gain_in, w0, w1, w2, w3, w4, w5, w_out, dbase_in, rbase_in, ggain_in, state,
    ST, GP1, WO1,
    G, GP0, WP, WO0, SA4, RA4, SB2, RB2, V8, M2, SA, VA, PQ, DEC, lens, gain, dbase, rbase, ggain,
    g_send, g_recv, p_send, p_recv, a_send, a_recv, w_local, w_send, w_recv, o_sem, st_sem, tok_sem, small_sem,
):
    tp, dp = lax.axis_index("tp"), lax.axis_index("dp")
    c = dp % 2
    at = {"z": tp // 4, "y": tp % 4, "x": dp // 2}
    projections = (w0, w1, w2, w3, w4, w5)
    GP, WO = (GP0, GP1), (WO0, WO1)

    def device(**hops):
        to = {axis: (at[axis] + hops.get(axis, 0)) % 4 for axis in "xyz"}
        return (to["z"] * 4 + to["y"], to["x"] * 2 + c)

    partner = (tp, at["x"] * 2 + 1 - c)

    barrier = pltpu.get_barrier_semaphore()
    peers = [
        dict(x=hx, y=hy, z=hz) for hx in range(4) for hy in range(4) for hz in range(4)
        if 0 in (hx, hy, hz) and (hx, hy, hz) != (0, 0, 0)
    ]
    for peer in peers:
        pl.semaphore_signal(barrier, inc=1, device_id=device(**peer), device_id_type=MESH)
    pl.semaphore_signal(barrier, inc=1, device_id=partner, device_id_type=MESH)

    tok_copies = []
    for q in range(4):
        rh, ch = q // 2, q % 2
        tok_copies.append(pltpu.make_async_copy(
            tok.at[pl.ds(rh * 16, 16), pl.ds(ch * 128, 128)],
            G.at[0, q, at["z"], at["y"], at["x"]],
            tok_sem.at[q],
        ))
        tok_copies[-1].start()
    mine = pl.multiple_of(c * 32, 32)
    own_cols = pl.multiple_of(dp * 32, 32)

    def weights_local(layer):
        for kind in range(6):
            pltpu.make_async_copy(
                projections[kind].at[layer],
                WP.at[layer, pl.ds(kind * 64 + mine, 32)],
                w_local.at[layer],
            ).start()
        pltpu.make_async_copy(w_out.at[layer], WO[layer].at[pl.ds(own_cols, 32)], o_sem.at[layer, 0]).start()

    small = [
        pltpu.make_async_copy(src, dst, small_sem.at[i])
        for i, (src, dst) in enumerate(
            ((lens_in, lens), (gain_in, gain), (dbase_in, dbase), (rbase_in, rbase), (ggain_in, ggain)))
    ]
    for copy in small:
        copy.start()
    weights_local(0)
    pl.semaphore_wait(barrier, len(peers) + 1)

    def block(a, q, free, moved=None):
        idx = [moved[ax] if moved and ax in moved else at[ax] for ax in "zyx"]
        idx = [slice(None) if ax in free else i for ax, i in zip("zyx", idx)]
        return G.at[(a, q, *idx)]

    def send(ref, send_sem, recv_sem, **hops):
        pltpu.make_async_remote_copy(
            src_ref=ref, dst_ref=ref, send_sem=send_sem, recv_sem=recv_sem,
            device_id=device(**hops), device_id_type=MESH,
        ).start()

    def landed(ref, sem):
        pltpu.make_async_copy(ref, ref, sem).wait()

    def gather_first(a):
        for q in range(4):
            first, second, third = ORDERS[q]
            if a == 0:
                tok_copies[q].wait()
            for hop in (2, 1, 3):
                send(block(a, q, ()), g_send.at[a, q, 0], g_recv.at[a, q, 0], **{first: hop})
            for over in (2, 1, 3):
                for hop in (2, 1, 3, 0):
                    send(block(a, q, ()), g_send.at[a, q, 1], g_recv.at[a, q, over],
                         **{first: hop, second: over})

    def gather_middle(a):
        for q in range(4):
            first, second, third = ORDERS[q]
            landed(G.at[a, q, 0, 0, pl.ds(0, 3)], g_recv.at[a, q, 0])
            for on in (2, 1, 3):
                send(block(a, q, first), g_send.at[a, q, 2], g_recv.at[a, q, 4], **{third: on})
        for over in (1, 3, 2):
            for q in range(4):
                first, second, third = ORDERS[q]
                landed(G.at[a, q, 0, 0], g_recv.at[a, q, over])
                line = {second: (at[second] + 4 - over) % 4}
                for on in (2, 1, 3):
                    send(block(a, q, first, line), g_send.at[a, q, 2], g_recv.at[a, q, 4], **{third: on})

    def gather_last(a):
        for q in range(4):
            landed(G.at[a, q, pl.ds(0, 3)], g_recv.at[a, q, 4])

    def gather_sent(a):
        for q in range(4):
            landed(G.at[a, q, 0, 0, pl.ds(0, 3)], g_send.at[a, q, 0])
            landed(G.at[a, q, pl.ds(0, 3), :, 0], g_send.at[a, q, 1])
            landed(G.at[a, q, pl.ds(0, 3)], g_send.at[a, q, 2])

    def rows_chunk(a, z):
        parts = []
        for y in range(4):
            for ch in range(2):
                halves = [G[a, rh * 2 + ch, z, y].reshape(64, 128) for rh in range(2)]
                parts.append(jnp.concatenate(halves, axis=0))
        return parts

    def exchange_start(n, src, dst):
        for hop in (2, 1, 3):
            to = (at["x"] + hop) % 4
            pltpu.make_async_remote_copy(
                src_ref=src.at[to], dst_ref=dst.at[at["x"]],
                send_sem=a_send.at[n], recv_sem=a_recv.at[n],
                device_id=device(x=hop), device_id_type=MESH,
            ).start()
        dst[at["x"]] = src[at["x"]]

    def exchange_done(n, dst):
        landed(dst.at[pl.ds(0, 3)], a_recv.at[n])

    def exchange_sent(n, src):
        landed(src.at[pl.ds(0, 3)], a_send.at[n])

    def projections_out(layer):
        for kind in range(6):
            pltpu.make_async_remote_copy(
                src_ref=projections[kind].at[layer],
                dst_ref=WP.at[layer, pl.ds(kind * 64 + mine, 32)],
                send_sem=w_send.at[layer], recv_sem=w_recv.at[layer],
                device_id=partner, device_id_type=MESH,
            ).start()

    def output_over_x(layer):
        for part in range(4):
            for hop in (2, 1, 3):
                pltpu.make_async_remote_copy(
                    src_ref=w_out.at[layer, pl.ds(part * 8, 8)],
                    dst_ref=WO[layer].at[pl.ds(pl.multiple_of(own_cols + part * 8, 8), 8)],
                    send_sem=o_sem.at[layer, 1], recv_sem=o_sem.at[layer, 2],
                    device_id=device(x=hop), device_id_type=MESH,
                ).start()

    def output_to_partner(layer):
        pltpu.make_async_remote_copy(
            src_ref=w_out.at[layer], dst_ref=WO[layer].at[pl.ds(own_cols, 32)],
            send_sem=o_sem.at[layer, 3], recv_sem=o_sem.at[layer, 4],
            device_id=partner, device_id_type=MESH,
        ).start()

    def output_pass_on(layer):
        landed(WO[layer].at[pl.ds(0, 96)], o_sem.at[layer, 2])
        for hop in (1, 2, 3):
            cols = pl.ds(pl.multiple_of(((at["x"] + hop) % 4) * 64 + c * 32, 32), 32)
            pltpu.make_async_remote_copy(
                src_ref=WO[layer].at[cols], dst_ref=WO[layer].at[cols],
                send_sem=o_sem.at[layer, 5], recv_sem=o_sem.at[layer, 6],
                device_id=partner, device_id_type=MESH,
            ).start()

    def output_in(layer):
        landed(WO[layer].at[pl.ds(0, 32)], o_sem.at[layer, 0])
        landed(WO[layer].at[pl.ds(0, 32)], o_sem.at[layer, 4])
        landed(WO[layer].at[pl.ds(0, 96)], o_sem.at[layer, 6])

    def output_sent(layer):
        landed(WO[layer].at[pl.ds(0, 96)], o_sem.at[layer, 1])
        landed(WO[layer].at[pl.ds(0, 32)], o_sem.at[layer, 3])
        landed(WO[layer].at[pl.ds(0, 96)], o_sem.at[layer, 5])

    def projections_in(layer):
        landed(WP.at[layer, pl.ds(0, 192)], w_local.at[layer])
        landed(WP.at[layer, pl.ds(0, 192)], w_recv.at[layer])
        scale = gain[layer:layer + 1, :]

        def fold(i, carry):
            rows = pl.ds(pl.multiple_of(i * 16, 16), 16)
            WP[layer, rows, :] = (WP[layer, rows, :].astype(F32) * scale).astype(BF16)
            return carry

        lax.fori_loop(0, 24, fold, 0)

    def weights_sent():
        for layer in range(2):
            landed(WP.at[layer, pl.ds(0, 192)], w_send.at[layer])
            output_sent(layer)

    def put_projected(projected, dst):
        out = projected.astype(BF16)
        for to in range(4):
            dst[to, 0:16, :] = out[to * 16:to * 16 + 16, :]
            dst[to, 16:32, :] = out[64 + to * 16:64 + to * 16 + 16, :]

    def project(layer):
        squares = jnp.zeros((128, 128), F32)
        acc = jnp.zeros((128, 256), F32)
        for z in range(4):
            parts = rows_chunk(layer, z)
            for part in parts:
                wide = part.astype(F32)
                squares += wide * wide
            acc += lax.dot_general(
                jnp.concatenate(parts, axis=1), WP[layer, 0:256, z * 1024:(z + 1) * 1024], LANES,
                preferred_element_type=F32,
            )
        factor = lax.rsqrt(jnp.sum(squares, axis=1, keepdims=True) * (1.0 / 4096) + RMS_EPS)
        put_projected(acc * factor, SA4.at[layer])
        exchange_start(2 * layer, SA4.at[layer], RA4.at[layer])
        acc = jnp.zeros((128, 128), F32)
        for z in range(4):
            acc += lax.dot_general(
                jnp.concatenate(rows_chunk(layer, z), axis=1), WP[layer, 256:384, z * 1024:(z + 1) * 1024], LANES,
                preferred_element_type=F32,
            )
        put_projected(acc * factor, SB2.at[layer])
        exchange_start(2 * layer + 1, SB2.at[layer], RB2.at[layer])

    def active_rows():
        row = lax.broadcasted_iota(jnp.int32, (32, 32), 0)
        col = lax.broadcasted_iota(jnp.int32, (32, 32), 1)
        spread = jnp.broadcast_to(lens[0:1, :], (32, 32))
        return jnp.sum(jnp.where(row == col, spread, 0), axis=1, keepdims=True) > STEP

    low = lax.broadcasted_iota(jnp.int32, (32, 128), 1) < 64

    def swap(value):
        return pltpu.roll(value, 64, 1)

    def recur(layer):
        active = active_rows()
        first_sums, second_sums = [], []
        for h in range(4):
            cols = slice(h * 64, (h + 1) * 64)
            base = jnp.concatenate([dbase[layer:layer + 1, cols], rbase[layer:layer + 1, cols]], axis=1)
            rec_key = RA4[layer, h, :, 0:128].astype(F32)
            opened = jax.nn.sigmoid(base + RA4[layer, h, :, 128:256].astype(F32))
            dec_rate = jnp.where(low, jnp.exp(-0.6065306597126334 * opened), opened)
            both = rec_key * dec_rate
            key_rec = swap(rec_key)
            square = jnp.sum(jnp.where(low, key_rec * key_rec, 0.0), axis=1, keepdims=True)
            scale = 1.0 / jnp.maximum(jnp.sqrt(square), 1e-12)
            total = jnp.sum(jnp.where(low, 0.0, both * key_rec), axis=1, keepdims=True)
            first_sums.append(total * scale)
            second_sums.append(total)
            V8[pl.ds(h, 32, stride=8), :] = key_rec * -scale
            V8[pl.ds(4 + h, 32, stride=8), :] = both
            key_rate = jnp.where(active, swap(both), 0.0)
            PQ[pl.ds(h, 32, stride=8), :] = key_rate * scale
            PQ[pl.ds(4 + h, 32, stride=8), :] = key_rate
            DEC[pl.ds(h, 32, stride=8), :] = jnp.where(active, dec_rate, 1.0)
        for b in range(32):
            got = lax.dot_general(
                V8[b * 8:(b + 1) * 8, 0:64].astype(BF16),
                ST[layer, b].reshape(256, 64).astype(BF16), LANES,
                preferred_element_type=F32,
            )
            for half in range(2):
                M2[half, b * 8:(b + 1) * 8, :] = got[:, half * 128:(half + 1) * 128]
        exchange_done(2 * layer + 1, RB2.at[layer])

        def heads(base):
            return jnp.where(low, M2[base // 2 % 2, pl.ds(base, 32, stride=8), :],
                             M2[base // 2 % 2, pl.ds(base + 1, 32, stride=8), :])

        for half in range(2):
            even, odd = 2 * half, 2 * half + 1
            even_vg, odd_vg = RB2[layer, even].astype(F32), RB2[layer, odd].astype(F32)
            value = jnp.where(low, even_vg, swap(odd_vg))
            gate = jax.nn.sigmoid(jnp.where(low, swap(even_vg), odd_vg))
            sa, direct = heads(even), heads(4 + even)
            half_cols = slice(half * 128, (half + 1) * 128)
            SA[:, half_cols] = sa
            VA[:, half_cols] = value
            readout = (direct + sa * jnp.where(low, first_sums[even], first_sums[odd])
                       + value * jnp.where(low, second_sums[even], second_sums[odd]))

            def head_mean(data):
                return jnp.where(low, jnp.sum(jnp.where(low, data, 0.0), axis=1, keepdims=True),
                                 jnp.sum(jnp.where(low, 0.0, data), axis=1, keepdims=True)) * (1.0 / 64)

            readout = readout - head_mean(readout)
            normal = readout * lax.rsqrt(head_mean(readout * readout) + GROUP_EPS)
            rows = jnp.where(active, normal * ggain[layer:layer + 1, half_cols] * gate, 0.0).astype(BF16)
            for rh in range(2):
                GP[layer][tp, rh * 2 + half] = rows[rh * 16:(rh + 1) * 16, :]

    head_of = lax.broadcasted_iota(jnp.int32, (8, 256), 1) // 64
    row_of = lax.broadcasted_iota(jnp.int32, (8, 256), 0)

    def update(layer, start, count):
        for b in range(start, start + count):
            left = jnp.where(row_of < 4, jnp.broadcast_to(SA[b:b + 1, :], (8, 256)),
                             jnp.broadcast_to(VA[b:b + 1, :], (8, 256)))
            left = jnp.where(row_of % 4 == head_of, left, 0.0)
            delta = lax.dot_general(
                left.astype(BF16), PQ[b * 8:(b + 1) * 8, 0:64].astype(BF16), ROWS,
                preferred_element_type=F32,
            )
            for h in range(4):
                ST[layer, b, h] = (ST[layer, b, h] * DEC[b * 8 + h:b * 8 + h + 1, 0:64]
                                   + delta[h * 64:(h + 1) * 64, :])

    def plane_first(layer):
        here = GP[layer].at[tp]
        for hop_z in (2, 1, 3, 0):
            for hop_y in (2, 1, 3, 0):
                if hop_z or hop_y:
                    send(here, p_send.at[layer], p_recv.at[layer], z=hop_z, y=hop_y)

    def plane_last(layer):
        landed(GP[layer].at[pl.ds(0, 15)], p_recv.at[layer])

    gather_first(0)
    projections_out(0)
    pltpu.make_async_copy(state.at[0], ST.at[0], st_sem.at[0]).start()
    output_over_x(0)
    weights_local(1)
    pltpu.make_async_copy(state.at[1], ST.at[1], st_sem.at[1]).start()
    gather_middle(0)
    for copy in small:
        copy.wait()
    projections_in(0)
    gather_last(0)
    project(0)
    output_to_partner(0)
    projections_out(1)
    output_to_partner(1)
    exchange_done(0, RA4.at[0])
    output_pass_on(0)
    landed(ST.at[0], st_sem.at[0])
    recur(0)
    plane_first(0)
    update(0, 0, 32)
    projections_in(1)
    output_in(0)
    plane_last(0)
    out = output_product(GP0, WO0)
    for q in range(4):
        rh, ch = q // 2, q % 2
        G[1, q, at["z"], at["y"], at["x"]] = out[rh * 16:(rh + 1) * 16, ch * 128:(ch + 1) * 128]
    gather_first(1)
    output_over_x(1)
    gather_middle(1)
    gather_last(1)
    project(1)
    exchange_done(2, RA4.at[1])
    output_pass_on(1)
    landed(ST.at[1], st_sem.at[1])
    recur(1)
    plane_first(1)
    update(1, 0, 32)
    output_in(1)
    plane_last(1)
    for a in range(2):
        gather_sent(a)
        exchange_sent(2 * a, SA4.at[a])
        exchange_sent(2 * a + 1, SB2.at[a])
        landed(GP[a].at[pl.ds(0, 15)], p_send.at[a])
    weights_sent()


def finish_kernel(state_in, rows, weight, state_out, mixed_out, mixed, sem):
    copies = [pltpu.make_async_copy(state_in.at[layer], state_out.at[layer], sem.at[layer]) for layer in range(2)]
    for copy in copies:
        copy.start()
    mixed[...] = output_product(rows, weight)
    copies.append(pltpu.make_async_copy(mixed, mixed_out, sem.at[2]))
    copies[2].start()
    for copy in copies:
        copy.wait()


def local(tokens, lengths, norm_gain, w_recept, w_key, w_value, w_decay, w_rate, w_gate, w_out,
          decay_base, rate_base, group_gain, state):
    weights = [jnp.swapaxes(w, 1, 2) for w in (w_recept, w_key, w_decay, w_rate, w_value, w_gate, w_out)]
    hbm = pl.BlockSpec(memory_space=pltpu.HBM)
    vmem = pl.BlockSpec(memory_space=pltpu.VMEM)
    stepped, rows, columns = pl.pallas_call(
        step_kernel,
        out_shape=(pltpu.VMEM(state.shape, F32), pltpu.VMEM((16, 4, 16, 128), BF16), pltpu.VMEM((256, 4096), BF16)),
        in_specs=[hbm] * 14,
        out_specs=(vmem, vmem, vmem),
        scratch_shapes=[
            pltpu.VMEM((2, 4, 4, 4, 4, 16, 128), BF16),
            pltpu.VMEM((16, 4, 16, 128), BF16),
            pltpu.VMEM((2, 384, 4096), BF16),
            pltpu.VMEM((256, 4096), BF16),
            pltpu.VMEM((2, 4, 32, 256), BF16),
            pltpu.VMEM((2, 4, 32, 256), BF16),
            pltpu.VMEM((2, 4, 32, 128), BF16),
            pltpu.VMEM((2, 4, 32, 128), BF16),
            pltpu.VMEM((256, 128), F32),
            pltpu.VMEM((2, 256, 128), F32),
            pltpu.VMEM((32, 256), F32),
            pltpu.VMEM((32, 256), F32),
            pltpu.VMEM((256, 128), F32),
            pltpu.VMEM((256, 128), F32),
            pltpu.VMEM((1, 32), jnp.int32),
            pltpu.VMEM((2, 4096), F32),
            pltpu.VMEM((2, 256), F32),
            pltpu.VMEM((2, 256), F32),
            pltpu.VMEM((2, 256), F32),
            pltpu.SemaphoreType.DMA((2, 4, 3)),
            pltpu.SemaphoreType.DMA((2, 4, 5)),
            pltpu.SemaphoreType.DMA((2,)),
            pltpu.SemaphoreType.DMA((2,)),
            pltpu.SemaphoreType.DMA((4,)),
            pltpu.SemaphoreType.DMA((4,)),
            pltpu.SemaphoreType.DMA((2,)),
            pltpu.SemaphoreType.DMA((2,)),
            pltpu.SemaphoreType.DMA((2,)),
            pltpu.SemaphoreType.DMA((2, 7)),
            pltpu.SemaphoreType.DMA((2,)),
            pltpu.SemaphoreType.DMA((4,)),
            pltpu.SemaphoreType.DMA((5,)),
        ],
        compiler_params=pltpu.CompilerParams(collective_id=0, has_side_effects=True, vmem_limit_bytes=44 << 20),
        name="decode_step",
    )(tokens, lengths.reshape(1, 32), norm_gain, *weights, decay_base, rate_base, group_gain, state)
    new_state, mixed = pl.pallas_call(
        finish_kernel,
        out_shape=(pltpu.HBM(state.shape, F32), pltpu.HBM((32, 256), BF16)),
        in_specs=[vmem] * 3,
        out_specs=(hbm, hbm),
        scratch_shapes=[pltpu.VMEM((32, 256), BF16), pltpu.SemaphoreType.DMA((3,))],
        compiler_params=pltpu.CompilerParams(vmem_limit_bytes=4 << 20),
        name="finish",
    )(stepped, rows, columns)
    return mixed, new_state


def solution(mesh):
    both = P(None, None, ("tp", "dp"))
    in_specs = (
        P("dp", "tp"), P("dp"), P(), both, both, both, both, both, both, both,
        P(None, "tp"), P(None, "tp"), P(None, "tp"), P(None, "dp", "tp", None, None),
    )
    out_specs = (P("dp", "tp"), P(None, "dp", "tp", None, None))
    return jax.shard_map(local, mesh=mesh, in_specs=in_specs, out_specs=out_specs, check_vma=False)
```

```python
import functools

import jax
import jax.numpy as jnp
from jax import lax
from jax.experimental import pallas as pl
from jax.experimental.pallas import tpu as pltpu
from jax.sharding import PartitionSpec as P

STEP = 16
RMS_EPS = 1e-06
GROUP_EPS = 0.00064
MESH = pl.DeviceIdType.MESH
F32 = jnp.float32
BF16 = jnp.bfloat16
ORDERS = (("x", "y", "z"), ("x", "z", "y"), ("x", "y", "z"), ("x", "z", "y"))
LANES = (((1,), (1,)), ((), ()))
ROWS = (((0,), (0,)), ((), ()))


def output_product(rows, weight, planes):
    acc = jnp.zeros((32, 256), F32)
    for plane in planes:
        z = plane()
        parts = [
            jnp.concatenate([rows[z * 4 + y, ch], rows[z * 4 + y, 2 + ch]], axis=0)
            for y in range(4) for ch in range(2)
        ]
        acc += lax.dot_general(
            jnp.concatenate(parts, axis=1), weight[:, pl.ds(pl.multiple_of(z * 1024, 1024), 1024)], LANES,
            preferred_element_type=F32,
        )
    return acc.astype(BF16)


def step_kernel(
    tok, lens_in, gain_in, w0, w1, w2, w3, w4, w5, w_out, dbase_in, rbase_in, ggain_in, state,
    ST, GP1, WO1,
    G, GP0, WP, WO0, SA4, RA4, SB2, RB2, V8, M2, SA, VA, PQ, DEC, lens, gain, dbase, rbase, ggain,
    g_send, g_recv, p_send, p_recv, a_send, a_recv, w_local, w_send, w_recv, o_sem, st_sem, tok_sem, small_sem,
):
    tp, dp = lax.axis_index("tp"), lax.axis_index("dp")
    c = dp % 2
    at = {"z": tp // 4, "y": tp % 4, "x": dp // 2}
    projections = (w0, w1, w2, w3, w4, w5)
    GP, WO = (GP0, GP1), (WO0, WO1)

    def device(**hops):
        to = {axis: (at[axis] + hops.get(axis, 0)) % 4 for axis in "xyz"}
        return (to["z"] * 4 + to["y"], to["x"] * 2 + c)

    partner = (tp, at["x"] * 2 + 1 - c)

    barrier = pltpu.get_barrier_semaphore()
    peers = [
        dict(x=hx, y=hy, z=hz) for hx in range(4) for hy in range(4) for hz in range(4)
        if 0 in (hx, hy, hz) and (hx, hy, hz) != (0, 0, 0)
    ]
    for peer in peers:
        pl.semaphore_signal(barrier, inc=1, device_id=device(**peer), device_id_type=MESH)
    pl.semaphore_signal(barrier, inc=1, device_id=partner, device_id_type=MESH)

    tok_copies = []
    for q in range(4):
        rh, ch = q // 2, q % 2
        tok_copies.append(pltpu.make_async_copy(
            tok.at[pl.ds(rh * 16, 16), pl.ds(ch * 128, 128)],
            G.at[0, q, at["z"], at["y"], at["x"]],
            tok_sem.at[q],
        ))
        tok_copies[-1].start()
    mine = pl.multiple_of(c * 32, 32)
    own_cols = pl.multiple_of(dp * 32, 32)

    def weights_local(layer):
        for kind in range(6):
            pltpu.make_async_copy(
                projections[kind].at[layer],
                WP.at[layer, pl.ds(kind * 64 + mine, 32)],
                w_local.at[layer],
            ).start()
        pltpu.make_async_copy(w_out.at[layer], WO[layer].at[pl.ds(own_cols, 32)], o_sem.at[layer, 0]).start()

    small = [
        pltpu.make_async_copy(src, dst, small_sem.at[i])
        for i, (src, dst) in enumerate(
            ((lens_in, lens), (gain_in, gain), (dbase_in, dbase), (rbase_in, rbase), (ggain_in, ggain)))
    ]
    for copy in small:
        copy.start()
    weights_local(0)
    pl.semaphore_wait(barrier, len(peers) + 1)

    def block(a, q, free, moved=None):
        idx = [moved[ax] if moved and ax in moved else at[ax] for ax in "zyx"]
        idx = [slice(None) if ax in free else i for ax, i in zip("zyx", idx)]
        return G.at[(a, q, *idx)]

    def send(ref, send_sem, recv_sem, **hops):
        pltpu.make_async_remote_copy(
            src_ref=ref, dst_ref=ref, send_sem=send_sem, recv_sem=recv_sem,
            device_id=device(**hops), device_id_type=MESH,
        ).start()

    def landed(ref, sem):
        pltpu.make_async_copy(ref, ref, sem).wait()

    def gather_first(a):
        for q in range(4):
            first, second, third = ORDERS[q]
            if a == 0:
                tok_copies[q].wait()
            for hop in (2, 1, 3):
                send(block(a, q, ()), g_send.at[a, q, 0], g_recv.at[a, q, 0], **{first: hop})
            for over in (2, 1, 3):
                for hop in (2, 1, 3, 0):
                    send(block(a, q, ()), g_send.at[a, q, 1], g_recv.at[a, q, over],
                         **{first: hop, second: over})

    def gather_middle(a):
        for q in range(4):
            first, second, third = ORDERS[q]
            landed(G.at[a, q, 0, 0, pl.ds(0, 3)], g_recv.at[a, q, 0])
            for on in (2, 1, 3):
                send(block(a, q, first), g_send.at[a, q, 2], g_recv.at[a, q, 3 + on], **{third: on})
        for over in (1, 3, 2):
            for q in range(4):
                first, second, third = ORDERS[q]
                landed(G.at[a, q, 0, 0], g_recv.at[a, q, over])
                line = {second: (at[second] + 4 - over) % 4}
                for on in (2, 1, 3):
                    send(block(a, q, first, line), g_send.at[a, q, 2], g_recv.at[a, q, 3 + on], **{third: on})

    def gather_last(a, on):
        for q in range(4):
            landed(G.at[a, q, 0], g_recv.at[a, q, 3 + on])

    def gather_sent(a):
        for q in range(4):
            landed(G.at[a, q, 0, 0, pl.ds(0, 3)], g_send.at[a, q, 0])
            landed(G.at[a, q, pl.ds(0, 3), :, 0], g_send.at[a, q, 1])
            landed(G.at[a, q, pl.ds(0, 3)], g_send.at[a, q, 2])

    def rows_chunk(a, z):
        parts = []
        for y in range(4):
            for ch in range(2):
                halves = [G[a, rh * 2 + ch, z, y].reshape(64, 128) for rh in range(2)]
                parts.append(jnp.concatenate(halves, axis=0))
        return parts

    def exchange_start(n, src, dst):
        for hop in (2, 1, 3):
            to = (at["x"] + hop) % 4
            pltpu.make_async_remote_copy(
                src_ref=src.at[to], dst_ref=dst.at[at["x"]],
                send_sem=a_send.at[n], recv_sem=a_recv.at[n],
                device_id=device(x=hop), device_id_type=MESH,
            ).start()
        dst[at["x"]] = src[at["x"]]

    def exchange_done(n, dst):
        landed(dst.at[pl.ds(0, 3)], a_recv.at[n])

    def exchange_sent(n, src):
        landed(src.at[pl.ds(0, 3)], a_send.at[n])

    def projections_out(layer):
        for kind in range(6):
            pltpu.make_async_remote_copy(
                src_ref=projections[kind].at[layer],
                dst_ref=WP.at[layer, pl.ds(kind * 64 + mine, 32)],
                send_sem=w_send.at[layer], recv_sem=w_recv.at[layer],
                device_id=partner, device_id_type=MESH,
            ).start()

    def output_over_x(layer):
        for part in range(4):
            for hop in (2, 1, 3):
                pltpu.make_async_remote_copy(
                    src_ref=w_out.at[layer, pl.ds(part * 8, 8)],
                    dst_ref=WO[layer].at[pl.ds(pl.multiple_of(own_cols + part * 8, 8), 8)],
                    send_sem=o_sem.at[layer, 1], recv_sem=o_sem.at[layer, 2],
                    device_id=device(x=hop), device_id_type=MESH,
                ).start()

    def output_to_partner(layer):
        pltpu.make_async_remote_copy(
            src_ref=w_out.at[layer], dst_ref=WO[layer].at[pl.ds(own_cols, 32)],
            send_sem=o_sem.at[layer, 3], recv_sem=o_sem.at[layer, 4],
            device_id=partner, device_id_type=MESH,
        ).start()

    def output_pass_on(layer):
        landed(WO[layer].at[pl.ds(0, 96)], o_sem.at[layer, 2])
        for hop in (1, 2, 3):
            cols = pl.ds(pl.multiple_of(((at["x"] + hop) % 4) * 64 + c * 32, 32), 32)
            pltpu.make_async_remote_copy(
                src_ref=WO[layer].at[cols], dst_ref=WO[layer].at[cols],
                send_sem=o_sem.at[layer, 5], recv_sem=o_sem.at[layer, 6],
                device_id=partner, device_id_type=MESH,
            ).start()

    def output_in(layer):
        landed(WO[layer].at[pl.ds(0, 32)], o_sem.at[layer, 0])
        landed(WO[layer].at[pl.ds(0, 32)], o_sem.at[layer, 4])
        landed(WO[layer].at[pl.ds(0, 96)], o_sem.at[layer, 6])

    def output_sent(layer):
        landed(WO[layer].at[pl.ds(0, 96)], o_sem.at[layer, 1])
        landed(WO[layer].at[pl.ds(0, 32)], o_sem.at[layer, 3])
        landed(WO[layer].at[pl.ds(0, 96)], o_sem.at[layer, 5])

    def projections_in(layer):
        landed(WP.at[layer, pl.ds(0, 192)], w_local.at[layer])
        landed(WP.at[layer, pl.ds(0, 192)], w_recv.at[layer])
        scale = gain[layer:layer + 1, :]

        def fold(i, carry):
            rows = pl.ds(pl.multiple_of(i * 16, 16), 16)
            WP[layer, rows, :] = (WP[layer, rows, :].astype(F32) * scale).astype(BF16)
            return carry

        lax.fori_loop(0, 24, fold, 0)

    def weights_sent():
        for layer in range(2):
            landed(WP.at[layer, pl.ds(0, 192)], w_send.at[layer])
            output_sent(layer)

    def put_projected(projected, dst):
        out = projected.astype(BF16)
        for to in range(4):
            dst[to, 0:16, :] = out[to * 16:to * 16 + 16, :]
            dst[to, 16:32, :] = out[64 + to * 16:64 + to * 16 + 16, :]

    def project(layer):
        squares = jnp.zeros((128, 128), F32)
        acc = jnp.zeros((128, 256), F32)
        for on in (0, 1, 3, 2):
            if on:
                gather_last(layer, on)
            for ch in range(2):
                along = ORDERS[ch][2]
                came = (at[along] + 4 - on) % 4
                spots = [(came, other) if along == "z" else (other, came) for other in range(4)]
                parts, weights = [], []
                for z, y in spots:
                    parts.append(jnp.concatenate(
                        [G[layer, rh * 2 + ch, z, y].reshape(64, 128) for rh in range(2)], axis=0))
                    start = pl.multiple_of(z * 1024 + y * 256 + ch * 128, 128)
                    weights.append(WP[layer, 0:256, pl.ds(start, 128)])
                for part in parts:
                    wide = part.astype(F32)
                    squares += wide * wide
                acc += lax.dot_general(
                    jnp.concatenate(parts, axis=1), jnp.concatenate(weights, axis=1), LANES,
                    preferred_element_type=F32,
                )
        factor = lax.rsqrt(jnp.sum(squares, axis=1, keepdims=True) * (1.0 / 4096) + RMS_EPS)
        put_projected(acc * factor, SA4.at[layer])
        exchange_start(2 * layer, SA4.at[layer], RA4.at[layer])
        acc = jnp.zeros((128, 128), F32)
        for z in range(4):
            acc += lax.dot_general(
                jnp.concatenate(rows_chunk(layer, z), axis=1), WP[layer, 256:384, z * 1024:(z + 1) * 1024], LANES,
                preferred_element_type=F32,
            )
        put_projected(acc * factor, SB2.at[layer])
        exchange_start(2 * layer + 1, SB2.at[layer], RB2.at[layer])

    def active_rows():
        row = lax.broadcasted_iota(jnp.int32, (32, 32), 0)
        col = lax.broadcasted_iota(jnp.int32, (32, 32), 1)
        spread = jnp.broadcast_to(lens[0:1, :], (32, 32))
        return jnp.sum(jnp.where(row == col, spread, 0), axis=1, keepdims=True) > STEP

    low = lax.broadcasted_iota(jnp.int32, (32, 128), 1) < 64

    def swap(value):
        return pltpu.roll(value, 64, 1)

    def recur(layer):
        active = active_rows()
        first_sums, second_sums = [], []
        for h in range(4):
            cols = slice(h * 64, (h + 1) * 64)
            base = jnp.concatenate([dbase[layer:layer + 1, cols], rbase[layer:layer + 1, cols]], axis=1)
            rec_key = RA4[layer, h, :, 0:128].astype(F32)
            opened = jax.nn.sigmoid(base + RA4[layer, h, :, 128:256].astype(F32))
            dec_rate = jnp.where(low, jnp.exp(-0.6065306597126334 * opened), opened)
            both = rec_key * dec_rate
            key_rec = swap(rec_key)
            square = jnp.sum(jnp.where(low, key_rec * key_rec, 0.0), axis=1, keepdims=True)
            scale = 1.0 / jnp.maximum(jnp.sqrt(square), 1e-12)
            total = jnp.sum(jnp.where(low, 0.0, both * key_rec), axis=1, keepdims=True)
            first_sums.append(total * scale)
            second_sums.append(total)
            V8[pl.ds(h, 32, stride=8), :] = key_rec * -scale
            V8[pl.ds(4 + h, 32, stride=8), :] = both
            key_rate = jnp.where(active, swap(both), 0.0)
            PQ[pl.ds(h, 32, stride=8), :] = key_rate * scale
            PQ[pl.ds(4 + h, 32, stride=8), :] = key_rate
            DEC[pl.ds(h, 32, stride=8), :] = jnp.where(active, dec_rate, 1.0)
        for b in range(32):
            got = lax.dot_general(
                V8[b * 8:(b + 1) * 8, 0:64].astype(BF16),
                ST[layer, b].reshape(256, 64).astype(BF16), LANES,
                preferred_element_type=F32,
            )
            for half in range(2):
                M2[half, b * 8:(b + 1) * 8, :] = got[:, half * 128:(half + 1) * 128]
        exchange_done(2 * layer + 1, RB2.at[layer])

        def heads(base):
            return jnp.where(low, M2[base // 2 % 2, pl.ds(base, 32, stride=8), :],
                             M2[base // 2 % 2, pl.ds(base + 1, 32, stride=8), :])

        for half in range(2):
            even, odd = 2 * half, 2 * half + 1
            even_vg, odd_vg = RB2[layer, even].astype(F32), RB2[layer, odd].astype(F32)
            value = jnp.where(low, even_vg, swap(odd_vg))
            gate = jax.nn.sigmoid(jnp.where(low, swap(even_vg), odd_vg))
            sa, direct = heads(even), heads(4 + even)
            half_cols = slice(half * 128, (half + 1) * 128)
            SA[:, half_cols] = sa
            VA[:, half_cols] = value
            readout = (direct + sa * jnp.where(low, first_sums[even], first_sums[odd])
                       + value * jnp.where(low, second_sums[even], second_sums[odd]))

            def head_mean(data):
                return jnp.where(low, jnp.sum(jnp.where(low, data, 0.0), axis=1, keepdims=True),
                                 jnp.sum(jnp.where(low, 0.0, data), axis=1, keepdims=True)) * (1.0 / 64)

            readout = readout - head_mean(readout)
            normal = readout * lax.rsqrt(head_mean(readout * readout) + GROUP_EPS)
            rows = jnp.where(active, normal * ggain[layer:layer + 1, half_cols] * gate, 0.0).astype(BF16)
            for rh in range(2):
                GP[layer][tp, rh * 2 + half] = rows[rh * 16:(rh + 1) * 16, :]

    head_of = lax.broadcasted_iota(jnp.int32, (8, 256), 1) // 64
    row_of = lax.broadcasted_iota(jnp.int32, (8, 256), 0)

    def update(layer, start, count):
        for b in range(start, start + count):
            left = jnp.where(row_of < 4, jnp.broadcast_to(SA[b:b + 1, :], (8, 256)),
                             jnp.broadcast_to(VA[b:b + 1, :], (8, 256)))
            left = jnp.where(row_of % 4 == head_of, left, 0.0)
            delta = lax.dot_general(
                left.astype(BF16), PQ[b * 8:(b + 1) * 8, 0:64].astype(BF16), ROWS,
                preferred_element_type=F32,
            )
            for h in range(4):
                ST[layer, b, h] = (ST[layer, b, h] * DEC[b * 8 + h:b * 8 + h + 1, 0:64]
                                   + delta[h * 64:(h + 1) * 64, :])

    def plane_first(layer):
        here = GP[layer].at[tp]
        for hop_z in (2, 1, 3, 0):
            for hop_y in (2, 1, 3, 0):
                if hop_z or hop_y:
                    send(here, p_send.at[layer], p_recv.at[layer, hop_z], z=hop_z, y=hop_y)

    def plane_last(layer, hop_z):
        landed(GP[layer].at[pl.ds(0, 4 if hop_z else 3)], p_recv.at[layer, hop_z])

    gather_first(0)
    projections_out(0)
    pltpu.make_async_copy(state.at[0], ST.at[0], st_sem.at[0]).start()
    output_over_x(0)
    weights_local(1)
    pltpu.make_async_copy(state.at[1], ST.at[1], st_sem.at[1]).start()
    gather_middle(0)
    for copy in small:
        copy.wait()
    projections_in(0)
    project(0)
    output_to_partner(0)
    projections_out(1)
    output_to_partner(1)
    exchange_done(0, RA4.at[0])
    output_pass_on(0)
    landed(ST.at[0], st_sem.at[0])
    recur(0)
    plane_first(0)
    update(0, 0, 32)
    projections_in(1)
    output_in(0)

    def came(hop_z):
        plane_last(0, hop_z)
        return (at["z"] + 4 - hop_z) % 4

    out = output_product(GP0, WO0, [functools.partial(came, hop_z) for hop_z in (0, 1, 3, 2)])
    for q in range(4):
        rh, ch = q // 2, q % 2
        G[1, q, at["z"], at["y"], at["x"]] = out[rh * 16:(rh + 1) * 16, ch * 128:(ch + 1) * 128]
    gather_first(1)
    output_over_x(1)
    gather_middle(1)
    project(1)
    exchange_done(2, RA4.at[1])
    output_pass_on(1)
    landed(ST.at[1], st_sem.at[1])
    recur(1)
    plane_first(1)
    update(1, 0, 32)
    output_in(1)
    for hop_z in range(4):
        plane_last(1, hop_z)
    for a in range(2):
        gather_sent(a)
        exchange_sent(2 * a, SA4.at[a])
        exchange_sent(2 * a + 1, SB2.at[a])
        landed(GP[a].at[pl.ds(0, 15)], p_send.at[a])
    weights_sent()


def finish_kernel(state_in, rows, weight, state_out, mixed_out, mixed, sem):
    copies = [pltpu.make_async_copy(state_in.at[layer], state_out.at[layer], sem.at[layer]) for layer in range(2)]
    for copy in copies:
        copy.start()
    mixed[...] = output_product(rows, weight, [functools.partial(int, z) for z in range(4)])
    copies.append(pltpu.make_async_copy(mixed, mixed_out, sem.at[2]))
    copies[2].start()
    for copy in copies:
        copy.wait()


def local(tokens, lengths, norm_gain, w_recept, w_key, w_value, w_decay, w_rate, w_gate, w_out,
          decay_base, rate_base, group_gain, state):
    weights = [jnp.swapaxes(w, 1, 2) for w in (w_recept, w_key, w_decay, w_rate, w_value, w_gate, w_out)]
    hbm = pl.BlockSpec(memory_space=pltpu.HBM)
    vmem = pl.BlockSpec(memory_space=pltpu.VMEM)
    stepped, rows, columns = pl.pallas_call(
        step_kernel,
        out_shape=(pltpu.VMEM(state.shape, F32), pltpu.VMEM((16, 4, 16, 128), BF16), pltpu.VMEM((256, 4096), BF16)),
        in_specs=[hbm] * 14,
        out_specs=(vmem, vmem, vmem),
        scratch_shapes=[
            pltpu.VMEM((2, 4, 4, 4, 4, 16, 128), BF16),
            pltpu.VMEM((16, 4, 16, 128), BF16),
            pltpu.VMEM((2, 384, 4096), BF16),
            pltpu.VMEM((256, 4096), BF16),
            pltpu.VMEM((2, 4, 32, 256), BF16),
            pltpu.VMEM((2, 4, 32, 256), BF16),
            pltpu.VMEM((2, 4, 32, 128), BF16),
            pltpu.VMEM((2, 4, 32, 128), BF16),
            pltpu.VMEM((256, 128), F32),
            pltpu.VMEM((2, 256, 128), F32),
            pltpu.VMEM((32, 256), F32),
            pltpu.VMEM((32, 256), F32),
            pltpu.VMEM((256, 128), F32),
            pltpu.VMEM((256, 128), F32),
            pltpu.VMEM((1, 32), jnp.int32),
            pltpu.VMEM((2, 4096), F32),
            pltpu.VMEM((2, 256), F32),
            pltpu.VMEM((2, 256), F32),
            pltpu.VMEM((2, 256), F32),
            pltpu.SemaphoreType.DMA((2, 4, 3)),
            pltpu.SemaphoreType.DMA((2, 4, 7)),
            pltpu.SemaphoreType.DMA((2,)),
            pltpu.SemaphoreType.DMA((2, 4)),
            pltpu.SemaphoreType.DMA((4,)),
            pltpu.SemaphoreType.DMA((4,)),
            pltpu.SemaphoreType.DMA((2,)),
            pltpu.SemaphoreType.DMA((2,)),
            pltpu.SemaphoreType.DMA((2,)),
            pltpu.SemaphoreType.DMA((2, 7)),
            pltpu.SemaphoreType.DMA((2,)),
            pltpu.SemaphoreType.DMA((4,)),
            pltpu.SemaphoreType.DMA((5,)),
        ],
        compiler_params=pltpu.CompilerParams(collective_id=0, has_side_effects=True, vmem_limit_bytes=44 << 20),
        name="decode_step",
    )(tokens, lengths.reshape(1, 32), norm_gain, *weights, decay_base, rate_base, group_gain, state)
    new_state, mixed = pl.pallas_call(
        finish_kernel,
        out_shape=(pltpu.HBM(state.shape, F32), pltpu.HBM((32, 256), BF16)),
        in_specs=[vmem] * 3,
        out_specs=(hbm, hbm),
        scratch_shapes=[pltpu.VMEM((32, 256), BF16), pltpu.SemaphoreType.DMA((3,))],
        compiler_params=pltpu.CompilerParams(vmem_limit_bytes=4 << 20),
        name="finish",
    )(stepped, rows, columns)
    return mixed, new_state


def solution(mesh):
    both = P(None, None, ("tp", "dp"))
    in_specs = (
        P("dp", "tp"), P("dp"), P(), both, both, both, both, both, both, both,
        P(None, "tp"), P(None, "tp"), P(None, "tp"), P(None, "dp", "tp", None, None),
    )
    out_specs = (P("dp", "tp"), P(None, "dp", "tp", None, None))
    return jax.shard_map(local, mesh=mesh, in_specs=in_specs, out_specs=out_specs, check_vma=False)
```

```python
import functools

import jax
import jax.numpy as jnp
from jax import lax
from jax.experimental import pallas as pl
from jax.experimental.pallas import tpu as pltpu
from jax.sharding import PartitionSpec as P

STEP = 16
RMS_EPS = 1e-06
GROUP_EPS = 0.00064
MESH = pl.DeviceIdType.MESH
F32 = jnp.float32
BF16 = jnp.bfloat16
ORDERS = (("x", "y", "z"), ("x", "z", "y"), ("x", "y", "z"), ("x", "z", "y"))
LANES = (((1,), (1,)), ((), ()))
ROWS = (((0,), (0,)), ((), ()))


def output_product(rows, weight, planes):
    acc = jnp.zeros((32, 256), F32)
    for plane in planes:
        z = plane()
        parts = [
            jnp.concatenate([rows[z * 4 + y, ch], rows[z * 4 + y, 2 + ch]], axis=0)
            for y in range(4) for ch in range(2)
        ]
        acc += lax.dot_general(
            jnp.concatenate(parts, axis=1), weight[:, pl.ds(pl.multiple_of(z * 1024, 1024), 1024)], LANES,
            preferred_element_type=F32,
        )
    return acc.astype(BF16)


def step_kernel(
    tok, lens_in, gain_in, w0, w1, w2, w3, w4, w5, w_out, dbase_in, rbase_in, ggain_in, state,
    ST, GP1, WO1,
    G, GP0, WP, WO0, SA4, RA4, SB2, RB2, V8, M2, SA, VA, PQ, DEC, lens, gain, dbase, rbase, ggain,
    g_send, g_recv, p_send, p_recv, a_send, a_recv, w_local, w_send, w_recv, o_sem, st_sem, tok_sem, small_sem,
):
    tp, dp = lax.axis_index("tp"), lax.axis_index("dp")
    c = dp % 2
    at = {"z": tp // 4, "y": tp % 4, "x": dp // 2}
    projections = (w0, w1, w2, w3, w4, w5)
    GP, WO = (GP0, GP1), (WO0, WO1)

    def device(**hops):
        to = {axis: (at[axis] + hops.get(axis, 0)) % 4 for axis in "xyz"}
        return (to["z"] * 4 + to["y"], to["x"] * 2 + c)

    partner = (tp, at["x"] * 2 + 1 - c)

    barrier = pltpu.get_barrier_semaphore()
    peers = [
        dict(x=hx, y=hy, z=hz) for hx in range(4) for hy in range(4) for hz in range(4)
        if 0 in (hx, hy, hz) and (hx, hy, hz) != (0, 0, 0)
    ]
    for peer in peers:
        pl.semaphore_signal(barrier, inc=1, device_id=device(**peer), device_id_type=MESH)
    pl.semaphore_signal(barrier, inc=1, device_id=partner, device_id_type=MESH)

    tok_copies = []
    for q in range(4):
        rh, ch = q // 2, q % 2
        tok_copies.append(pltpu.make_async_copy(
            tok.at[pl.ds(rh * 16, 16), pl.ds(ch * 128, 128)],
            G.at[0, q, at["z"], at["y"], at["x"]],
            tok_sem.at[q],
        ))
        tok_copies[-1].start()
    mine = pl.multiple_of(c * 32, 32)
    own_cols = pl.multiple_of(dp * 32, 32)

    def weights_local(layer):
        for kind in range(6):
            pltpu.make_async_copy(
                projections[kind].at[layer],
                WP.at[layer, pl.ds(kind * 64 + mine, 32)],
                w_local.at[layer],
            ).start()
        pltpu.make_async_copy(w_out.at[layer], WO[layer].at[pl.ds(own_cols, 32)], o_sem.at[layer, 0]).start()

    small = [
        pltpu.make_async_copy(src, dst, small_sem.at[i])
        for i, (src, dst) in enumerate(
            ((lens_in, lens), (gain_in, gain), (dbase_in, dbase), (rbase_in, rbase), (ggain_in, ggain)))
    ]
    for copy in small:
        copy.start()
    weights_local(0)
    pl.semaphore_wait(barrier, len(peers) + 1)

    def block(a, q, free, moved=None):
        idx = [moved[ax] if moved and ax in moved else at[ax] for ax in "zyx"]
        idx = [slice(None) if ax in free else i for ax, i in zip("zyx", idx)]
        return G.at[(a, q, *idx)]

    def send(ref, send_sem, recv_sem, **hops):
        pltpu.make_async_remote_copy(
            src_ref=ref, dst_ref=ref, send_sem=send_sem, recv_sem=recv_sem,
            device_id=device(**hops), device_id_type=MESH,
        ).start()

    def landed(ref, sem):
        pltpu.make_async_copy(ref, ref, sem).wait()

    def gather_first(a):
        for q in range(4):
            first, second, third = ORDERS[q]
            if a == 0:
                tok_copies[q].wait()
            for hop in (2, 1, 3):
                send(block(a, q, ()), g_send.at[a, q, 0], g_recv.at[a, q, 0], **{first: hop})
            for over in (2, 1, 3):
                for hop in (2, 1, 3, 0):
                    send(block(a, q, ()), g_send.at[a, q, 1], g_recv.at[a, q, over],
                         **{first: hop, second: over})

    def gather_middle(a):
        for q in range(4):
            first, second, third = ORDERS[q]
            landed(G.at[a, q, 0, 0, pl.ds(0, 3)], g_recv.at[a, q, 0])
            for on in (2, 1, 3):
                send(block(a, q, first), g_send.at[a, q, 2], g_recv.at[a, q, 3 + on], **{third: on})
        if a == 0:
            output_over_x(0)
        for over in (1, 3, 2):
            for q in range(4):
                first, second, third = ORDERS[q]
                landed(G.at[a, q, 0, 0], g_recv.at[a, q, over])
                line = {second: (at[second] + 4 - over) % 4}
                for on in (2, 1, 3):
                    send(block(a, q, first, line), g_send.at[a, q, 2], g_recv.at[a, q, 3 + on], **{third: on})

    def gather_last(a, on):
        for q in range(4):
            landed(G.at[a, q, 0], g_recv.at[a, q, 3 + on])

    def gather_sent(a):
        for q in range(4):
            landed(G.at[a, q, 0, 0, pl.ds(0, 3)], g_send.at[a, q, 0])
            landed(G.at[a, q, pl.ds(0, 3), :, 0], g_send.at[a, q, 1])
            landed(G.at[a, q, pl.ds(0, 3)], g_send.at[a, q, 2])

    def rows_chunk(a, z):
        parts = []
        for y in range(4):
            for ch in range(2):
                halves = [G[a, rh * 2 + ch, z, y].reshape(64, 128) for rh in range(2)]
                parts.append(jnp.concatenate(halves, axis=0))
        return parts

    def exchange_start(n, src, dst):
        for hop in (2, 1, 3):
            to = (at["x"] + hop) % 4
            pltpu.make_async_remote_copy(
                src_ref=src.at[to], dst_ref=dst.at[at["x"]],
                send_sem=a_send.at[n], recv_sem=a_recv.at[n],
                device_id=device(x=hop), device_id_type=MESH,
            ).start()
        dst[at["x"]] = src[at["x"]]

    def exchange_done(n, dst):
        landed(dst.at[pl.ds(0, 3)], a_recv.at[n])

    def exchange_sent(n, src):
        landed(src.at[pl.ds(0, 3)], a_send.at[n])

    def projections_out(layer):
        for kind in range(6):
            pltpu.make_async_remote_copy(
                src_ref=projections[kind].at[layer],
                dst_ref=WP.at[layer, pl.ds(kind * 64 + mine, 32)],
                send_sem=w_send.at[layer], recv_sem=w_recv.at[layer],
                device_id=partner, device_id_type=MESH,
            ).start()

    def output_over_x(layer):
        for part in range(4):
            for hop in (1, 3):
                pltpu.make_async_remote_copy(
                    src_ref=w_out.at[layer, pl.ds(part * 8, 8)],
                    dst_ref=WO[layer].at[pl.ds(pl.multiple_of(own_cols + part * 8, 8), 8)],
                    send_sem=o_sem.at[layer, 1], recv_sem=o_sem.at[layer, 1 + hop],
                    device_id=device(x=hop), device_id_type=MESH,
                ).start()

    def output_far_x(layer):
        for half, hop in enumerate((1, 3)):
            landed(WO[layer].at[pl.ds(0, 32)], o_sem.at[layer, 1 + hop])
            cols = pl.ds(pl.multiple_of((at["x"] + 4 - hop) % 4 * 64 + c * 32 + half * 16, 16), 16)
            pltpu.make_async_remote_copy(
                src_ref=WO[layer].at[cols], dst_ref=WO[layer].at[cols],
                send_sem=o_sem.at[layer, 7], recv_sem=o_sem.at[layer, 8],
                device_id=device(x=hop), device_id_type=MESH,
            ).start()

    def output_to_partner(layer):
        pltpu.make_async_remote_copy(
            src_ref=w_out.at[layer], dst_ref=WO[layer].at[pl.ds(own_cols, 32)],
            send_sem=o_sem.at[layer, 3], recv_sem=o_sem.at[layer, 9],
            device_id=partner, device_id_type=MESH,
        ).start()

    def output_pass_on(layer):
        landed(WO[layer].at[pl.ds(0, 32)], o_sem.at[layer, 8])
        for hop in (1, 2, 3):
            cols = pl.ds(pl.multiple_of(((at["x"] + hop) % 4) * 64 + c * 32, 32), 32)
            pltpu.make_async_remote_copy(
                src_ref=WO[layer].at[cols], dst_ref=WO[layer].at[cols],
                send_sem=o_sem.at[layer, 5], recv_sem=o_sem.at[layer, 6],
                device_id=partner, device_id_type=MESH,
            ).start()

    def output_in(layer):
        landed(WO[layer].at[pl.ds(0, 32)], o_sem.at[layer, 0])
        landed(WO[layer].at[pl.ds(0, 32)], o_sem.at[layer, 9])
        landed(WO[layer].at[pl.ds(0, 96)], o_sem.at[layer, 6])

    def output_sent(layer):
        landed(WO[layer].at[pl.ds(0, 64)], o_sem.at[layer, 1])
        landed(WO[layer].at[pl.ds(0, 32)], o_sem.at[layer, 7])
        landed(WO[layer].at[pl.ds(0, 32)], o_sem.at[layer, 3])
        landed(WO[layer].at[pl.ds(0, 96)], o_sem.at[layer, 5])

    def projections_in(layer):
        landed(WP.at[layer, pl.ds(0, 192)], w_local.at[layer])
        landed(WP.at[layer, pl.ds(0, 192)], w_recv.at[layer])
        scale = gain[layer:layer + 1, :]

        def fold(i, carry):
            rows = pl.ds(pl.multiple_of(i * 16, 16), 16)
            WP[layer, rows, :] = (WP[layer, rows, :].astype(F32) * scale).astype(BF16)
            return carry

        lax.fori_loop(0, 24, fold, 0)

    def weights_sent():
        for layer in range(2):
            landed(WP.at[layer, pl.ds(0, 192)], w_send.at[layer])
            output_sent(layer)

    def put_projected(projected, dst):
        out = projected.astype(BF16)
        for to in range(4):
            dst[to, 0:16, :] = out[to * 16:to * 16 + 16, :]
            dst[to, 16:32, :] = out[64 + to * 16:64 + to * 16 + 16, :]

    def project(layer):
        squares = jnp.zeros((128, 128), F32)
        acc = jnp.zeros((128, 256), F32)
        for on in (0, 1, 3, 2):
            if on:
                gather_last(layer, on)
            for ch in range(2):
                along = ORDERS[ch][2]
                came = (at[along] + 4 - on) % 4
                spots = [(came, other) if along == "z" else (other, came) for other in range(4)]
                parts, weights = [], []
                for z, y in spots:
                    parts.append(jnp.concatenate(
                        [G[layer, rh * 2 + ch, z, y].reshape(64, 128) for rh in range(2)], axis=0))
                    start = pl.multiple_of(z * 1024 + y * 256 + ch * 128, 128)
                    weights.append(WP[layer, 0:256, pl.ds(start, 128)])
                for part in parts:
                    wide = part.astype(F32)
                    squares += wide * wide
                acc += lax.dot_general(
                    jnp.concatenate(parts, axis=1), jnp.concatenate(weights, axis=1), LANES,
                    preferred_element_type=F32,
                )
        factor = lax.rsqrt(jnp.sum(squares, axis=1, keepdims=True) * (1.0 / 4096) + RMS_EPS)
        put_projected(acc * factor, SA4.at[layer])
        exchange_start(2 * layer, SA4.at[layer], RA4.at[layer])
        acc = jnp.zeros((128, 128), F32)
        for z in range(4):
            acc += lax.dot_general(
                jnp.concatenate(rows_chunk(layer, z), axis=1), WP[layer, 256:384, z * 1024:(z + 1) * 1024], LANES,
                preferred_element_type=F32,
            )
        put_projected(acc * factor, SB2.at[layer])
        exchange_start(2 * layer + 1, SB2.at[layer], RB2.at[layer])

    def active_rows():
        row = lax.broadcasted_iota(jnp.int32, (32, 32), 0)
        col = lax.broadcasted_iota(jnp.int32, (32, 32), 1)
        spread = jnp.broadcast_to(lens[0:1, :], (32, 32))
        return jnp.sum(jnp.where(row == col, spread, 0), axis=1, keepdims=True) > STEP

    low = lax.broadcasted_iota(jnp.int32, (32, 128), 1) < 64

    def swap(value):
        return pltpu.roll(value, 64, 1)

    def recur(layer):
        active = active_rows()
        first_sums, second_sums = [], []
        for h in range(4):
            cols = slice(h * 64, (h + 1) * 64)
            base = jnp.concatenate([dbase[layer:layer + 1, cols], rbase[layer:layer + 1, cols]], axis=1)
            rec_key = RA4[layer, h, :, 0:128].astype(F32)
            opened = jax.nn.sigmoid(base + RA4[layer, h, :, 128:256].astype(F32))
            dec_rate = jnp.where(low, jnp.exp(-0.6065306597126334 * opened), opened)
            both = rec_key * dec_rate
            key_rec = swap(rec_key)
            square = jnp.sum(jnp.where(low, key_rec * key_rec, 0.0), axis=1, keepdims=True)
            scale = 1.0 / jnp.maximum(jnp.sqrt(square), 1e-12)
            total = jnp.sum(jnp.where(low, 0.0, both * key_rec), axis=1, keepdims=True)
            first_sums.append(total * scale)
            second_sums.append(total)
            V8[pl.ds(h, 32, stride=8), :] = key_rec * -scale
            V8[pl.ds(4 + h, 32, stride=8), :] = both
            key_rate = jnp.where(active, swap(both), 0.0)
            PQ[pl.ds(h, 32, stride=8), :] = key_rate * scale
            PQ[pl.ds(4 + h, 32, stride=8), :] = key_rate
            DEC[pl.ds(h, 32, stride=8), :] = jnp.where(active, dec_rate, 1.0)
        for b in range(32):
            got = lax.dot_general(
                V8[b * 8:(b + 1) * 8, 0:64].astype(BF16),
                ST[layer, b].reshape(256, 64).astype(BF16), LANES,
                preferred_element_type=F32,
            )
            for half in range(2):
                M2[half, b * 8:(b + 1) * 8, :] = got[:, half * 128:(half + 1) * 128]
        exchange_done(2 * layer + 1, RB2.at[layer])

        def heads(base):
            return jnp.where(low, M2[base // 2 % 2, pl.ds(base, 32, stride=8), :],
                             M2[base // 2 % 2, pl.ds(base + 1, 32, stride=8), :])

        for half in range(2):
            even, odd = 2 * half, 2 * half + 1
            even_vg, odd_vg = RB2[layer, even].astype(F32), RB2[layer, odd].astype(F32)
            value = jnp.where(low, even_vg, swap(odd_vg))
            gate = jax.nn.sigmoid(jnp.where(low, swap(even_vg), odd_vg))
            sa, direct = heads(even), heads(4 + even)
            half_cols = slice(half * 128, (half + 1) * 128)
            SA[:, half_cols] = sa
            VA[:, half_cols] = value
            readout = (direct + sa * jnp.where(low, first_sums[even], first_sums[odd])
                       + value * jnp.where(low, second_sums[even], second_sums[odd]))

            def head_mean(data):
                return jnp.where(low, jnp.sum(jnp.where(low, data, 0.0), axis=1, keepdims=True),
                                 jnp.sum(jnp.where(low, 0.0, data), axis=1, keepdims=True)) * (1.0 / 64)

            readout = readout - head_mean(readout)
            normal = readout * lax.rsqrt(head_mean(readout * readout) + GROUP_EPS)
            rows = jnp.where(active, normal * ggain[layer:layer + 1, half_cols] * gate, 0.0).astype(BF16)
            for rh in range(2):
                GP[layer][tp, rh * 2 + half] = rows[rh * 16:(rh + 1) * 16, :]

    head_of = lax.broadcasted_iota(jnp.int32, (8, 256), 1) // 64
    row_of = lax.broadcasted_iota(jnp.int32, (8, 256), 0)

    def update(layer, start, count):
        for b in range(start, start + count):
            left = jnp.where(row_of < 4, jnp.broadcast_to(SA[b:b + 1, :], (8, 256)),
                             jnp.broadcast_to(VA[b:b + 1, :], (8, 256)))
            left = jnp.where(row_of % 4 == head_of, left, 0.0)
            delta = lax.dot_general(
                left.astype(BF16), PQ[b * 8:(b + 1) * 8, 0:64].astype(BF16), ROWS,
                preferred_element_type=F32,
            )
            for h in range(4):
                ST[layer, b, h] = (ST[layer, b, h] * DEC[b * 8 + h:b * 8 + h + 1, 0:64]
                                   + delta[h * 64:(h + 1) * 64, :])

    def plane_first(layer):
        here = GP[layer].at[tp]
        for hop_z in (2, 1, 3, 0):
            for hop_y in (2, 1, 3, 0):
                if hop_z or hop_y:
                    send(here, p_send.at[layer], p_recv.at[layer, hop_z], z=hop_z, y=hop_y)

    def plane_last(layer, hop_z):
        landed(GP[layer].at[pl.ds(0, 4 if hop_z else 3)], p_recv.at[layer, hop_z])

    gather_first(0)
    projections_out(0)
    pltpu.make_async_copy(state.at[0], ST.at[0], st_sem.at[0]).start()
    weights_local(1)
    pltpu.make_async_copy(state.at[1], ST.at[1], st_sem.at[1]).start()
    gather_middle(0)
    for copy in small:
        copy.wait()
    projections_in(0)
    project(0)
    output_far_x(0)
    output_to_partner(0)
    projections_out(1)
    output_to_partner(1)
    exchange_done(0, RA4.at[0])
    landed(ST.at[0], st_sem.at[0])
    recur(0)
    plane_first(0)
    output_pass_on(0)
    update(0, 0, 32)
    projections_in(1)
    output_in(0)

    def came(hop_z):
        plane_last(0, hop_z)
        return (at["z"] + 4 - hop_z) % 4

    out = output_product(GP0, WO0, [functools.partial(came, hop_z) for hop_z in (0, 1, 3, 2)])
    for q in range(4):
        rh, ch = q // 2, q % 2
        G[1, q, at["z"], at["y"], at["x"]] = out[rh * 16:(rh + 1) * 16, ch * 128:(ch + 1) * 128]
    gather_first(1)
    gather_middle(1)
    output_over_x(1)
    project(1)
    output_far_x(1)
    exchange_done(2, RA4.at[1])
    landed(ST.at[1], st_sem.at[1])
    recur(1)
    plane_first(1)
    output_pass_on(1)
    update(1, 0, 32)
    output_in(1)
    for hop_z in range(4):
        plane_last(1, hop_z)
    for a in range(2):
        gather_sent(a)
        exchange_sent(2 * a, SA4.at[a])
        exchange_sent(2 * a + 1, SB2.at[a])
        landed(GP[a].at[pl.ds(0, 15)], p_send.at[a])
    weights_sent()


def finish_kernel(state_in, rows, weight, state_out, mixed_out, mixed, sem):
    copies = [pltpu.make_async_copy(state_in.at[layer], state_out.at[layer], sem.at[layer]) for layer in range(2)]
    for copy in copies:
        copy.start()
    mixed[...] = output_product(rows, weight, [functools.partial(int, z) for z in range(4)])
    copies.append(pltpu.make_async_copy(mixed, mixed_out, sem.at[2]))
    copies[2].start()
    for copy in copies:
        copy.wait()


def local(tokens, lengths, norm_gain, w_recept, w_key, w_value, w_decay, w_rate, w_gate, w_out,
          decay_base, rate_base, group_gain, state):
    weights = [jnp.swapaxes(w, 1, 2) for w in (w_recept, w_key, w_decay, w_rate, w_value, w_gate, w_out)]
    hbm = pl.BlockSpec(memory_space=pltpu.HBM)
    vmem = pl.BlockSpec(memory_space=pltpu.VMEM)
    stepped, rows, columns = pl.pallas_call(
        step_kernel,
        out_shape=(pltpu.VMEM(state.shape, F32), pltpu.VMEM((16, 4, 16, 128), BF16), pltpu.VMEM((256, 4096), BF16)),
        in_specs=[hbm] * 14,
        out_specs=(vmem, vmem, vmem),
        scratch_shapes=[
            pltpu.VMEM((2, 4, 4, 4, 4, 16, 128), BF16),
            pltpu.VMEM((16, 4, 16, 128), BF16),
            pltpu.VMEM((2, 384, 4096), BF16),
            pltpu.VMEM((256, 4096), BF16),
            pltpu.VMEM((2, 4, 32, 256), BF16),
            pltpu.VMEM((2, 4, 32, 256), BF16),
            pltpu.VMEM((2, 4, 32, 128), BF16),
            pltpu.VMEM((2, 4, 32, 128), BF16),
            pltpu.VMEM((256, 128), F32),
            pltpu.VMEM((2, 256, 128), F32),
            pltpu.VMEM((32, 256), F32),
            pltpu.VMEM((32, 256), F32),
            pltpu.VMEM((256, 128), F32),
            pltpu.VMEM((256, 128), F32),
            pltpu.VMEM((1, 32), jnp.int32),
            pltpu.VMEM((2, 4096), F32),
            pltpu.VMEM((2, 256), F32),
            pltpu.VMEM((2, 256), F32),
            pltpu.VMEM((2, 256), F32),
            pltpu.SemaphoreType.DMA((2, 4, 3)),
            pltpu.SemaphoreType.DMA((2, 4, 7)),
            pltpu.SemaphoreType.DMA((2,)),
            pltpu.SemaphoreType.DMA((2, 4)),
            pltpu.SemaphoreType.DMA((4,)),
            pltpu.SemaphoreType.DMA((4,)),
            pltpu.SemaphoreType.DMA((2,)),
            pltpu.SemaphoreType.DMA((2,)),
            pltpu.SemaphoreType.DMA((2,)),
            pltpu.SemaphoreType.DMA((2, 10)),
            pltpu.SemaphoreType.DMA((2,)),
            pltpu.SemaphoreType.DMA((4,)),
            pltpu.SemaphoreType.DMA((5,)),
        ],
        compiler_params=pltpu.CompilerParams(collective_id=0, has_side_effects=True, vmem_limit_bytes=44 << 20),
        name="decode_step",
    )(tokens, lengths.reshape(1, 32), norm_gain, *weights, decay_base, rate_base, group_gain, state)
    new_state, mixed = pl.pallas_call(
        finish_kernel,
        out_shape=(pltpu.HBM(state.shape, F32), pltpu.HBM((32, 256), BF16)),
        in_specs=[vmem] * 3,
        out_specs=(hbm, hbm),
        scratch_shapes=[pltpu.VMEM((32, 256), BF16), pltpu.SemaphoreType.DMA((3,))],
        compiler_params=pltpu.CompilerParams(vmem_limit_bytes=4 << 20),
        name="finish",
    )(stepped, rows, columns)
    return mixed, new_state


def solution(mesh):
    both = P(None, None, ("tp", "dp"))
    in_specs = (
        P("dp", "tp"), P("dp"), P(), both, both, both, both, both, both, both,
        P(None, "tp"), P(None, "tp"), P(None, "tp"), P(None, "dp", "tp", None, None),
    )
    out_specs = (P("dp", "tp"), P(None, "dp", "tp", None, None))
    return jax.shard_map(local, mesh=mesh, in_specs=in_specs, out_specs=out_specs, check_vma=False)
```

```python
import functools

import jax
import jax.numpy as jnp
from jax import lax
from jax.experimental import pallas as pl
from jax.experimental.pallas import tpu as pltpu
from jax.sharding import PartitionSpec as P

STEP = 16
RMS_EPS = 1e-06
GROUP_EPS = 0.00064
MESH = pl.DeviceIdType.MESH
F32 = jnp.float32
BF16 = jnp.bfloat16
ORDERS = (("y", "x", "z"), ("z", "x", "y"), ("y", "x", "z"), ("z", "x", "y"))
LANES = (((1,), (1,)), ((), ()))
ROWS = (((0,), (0,)), ((), ()))


def output_product(rows, weight, planes):
    acc = jnp.zeros((32, 256), F32)
    for plane in planes:
        z = plane()
        parts = [
            jnp.concatenate([rows[z * 4 + y, ch], rows[z * 4 + y, 2 + ch]], axis=0)
            for y in range(4) for ch in range(2)
        ]
        acc += lax.dot_general(
            jnp.concatenate(parts, axis=1), weight[:, pl.ds(pl.multiple_of(z * 1024, 1024), 1024)], LANES,
            preferred_element_type=F32,
        )
    return acc.astype(BF16)


def step_kernel(
    tok, lens_in, gain_in, w0, w1, w2, w3, w4, w5, w_out, dbase_in, rbase_in, ggain_in, state,
    ST, GP1, WO1,
    G, GP0, WP, WO0, SA4, RA4, SB2, RB2, V8, M2, S16, SA, VA, PQ, DEC, lens, gain, dbase, rbase, ggain,
    g_send, g_recv, p_send, p_recv, a_send, a_recv, w_local, w_send, w_recv, o_sem, st_sem, tok_sem, small_sem,
):
    tp, dp = lax.axis_index("tp"), lax.axis_index("dp")
    c = dp % 2
    at = {"z": tp // 4, "y": tp % 4, "x": dp // 2}
    projections = (w0, w1, w2, w3, w4, w5)
    GP, WO = (GP0, GP1), (WO0, WO1)

    def device(**hops):
        to = {axis: (at[axis] + hops.get(axis, 0)) % 4 for axis in "xyz"}
        return (to["z"] * 4 + to["y"], to["x"] * 2 + c)

    partner = (tp, at["x"] * 2 + 1 - c)

    barrier = pltpu.get_barrier_semaphore()
    peers = [
        dict(x=hx, y=hy, z=hz) for hx in range(4) for hy in range(4) for hz in range(4)
        if 0 in (hx, hy, hz) and (hx, hy, hz) != (0, 0, 0)
    ]
    peers.sort(key=lambda peer: -sum(min(hop, 4 - hop) for hop in peer.values()))
    for peer in peers:
        pl.semaphore_signal(barrier, inc=1, device_id=device(**peer), device_id_type=MESH)
    pl.semaphore_signal(barrier, inc=1, device_id=partner, device_id_type=MESH)

    tok_copies = []
    for q in range(4):
        rh, ch = q // 2, q % 2
        tok_copies.append(pltpu.make_async_copy(
            tok.at[pl.ds(rh * 16, 16), pl.ds(ch * 128, 128)],
            G.at[0, q, at["z"], at["y"], at["x"]],
            tok_sem.at[q],
        ))
        tok_copies[-1].start()
    mine = pl.multiple_of(c * 32, 32)
    own_cols = pl.multiple_of(dp * 32, 32)

    def weights_local(layer):
        for kind in range(6):
            pltpu.make_async_copy(
                projections[kind].at[layer],
                WP.at[layer, pl.ds(kind * 64 + mine, 32)],
                w_local.at[layer],
            ).start()
        pltpu.make_async_copy(w_out.at[layer], WO[layer].at[pl.ds(own_cols, 32)], o_sem.at[layer, 0]).start()

    small = [
        pltpu.make_async_copy(src, dst, small_sem.at[i])
        for i, (src, dst) in enumerate(
            ((lens_in, lens), (gain_in, gain), (dbase_in, dbase), (rbase_in, rbase), (ggain_in, ggain)))
    ]
    for copy in small:
        copy.start()
    weights_local(0)
    pl.semaphore_wait(barrier, len(peers) + 1)

    def block(a, q, free, moved=None):
        idx = [moved[ax] if moved and ax in moved else at[ax] for ax in "zyx"]
        idx = [slice(None) if ax in free else i for ax, i in zip("zyx", idx)]
        return G.at[(a, q, *idx)]

    def send(ref, send_sem, recv_sem, **hops):
        pltpu.make_async_remote_copy(
            src_ref=ref, dst_ref=ref, send_sem=send_sem, recv_sem=recv_sem,
            device_id=device(**hops), device_id_type=MESH,
        ).start()

    def landed(ref, sem):
        pltpu.make_async_copy(ref, ref, sem).wait()

    def gather_first(a):
        for q in range(4):
            first, second, third = ORDERS[q]
            if a == 0:
                tok_copies[q].wait()
            for hop in (2, 1, 3):
                send(block(a, q, ()), g_send.at[a, q, 0], g_recv.at[a, q, 0], **{first: hop})
            for over in (2, 1, 3):
                for hop in (2, 1, 3, 0):
                    send(block(a, q, ()), g_send.at[a, q, 1], g_recv.at[a, q, over],
                         **{first: hop, second: over})

    def gather_middle(a):
        for q in range(4):
            first, second, third = ORDERS[q]
            landed(G.at[a, q, 0, 0, pl.ds(0, 3)], g_recv.at[a, q, 0])
            for on in (2, 1, 3):
                send(block(a, q, first), g_send.at[a, q, 2], g_recv.at[a, q, 3 + on], **{third: on})
        if a == 0:
            output_over_x(0)
        for over in (1, 3, 2):
            for q in range(4):
                first, second, third = ORDERS[q]
                landed(G.at[a, q, 0, 0], g_recv.at[a, q, over])
                line = {second: (at[second] + 4 - over) % 4}
                for on in (2, 1, 3):
                    send(block(a, q, first, line), g_send.at[a, q, 2], g_recv.at[a, q, 3 + on], **{third: on})

    def gather_last(a, on):
        for q in range(4):
            landed(G.at[a, q, 0], g_recv.at[a, q, 3 + on])

    def gather_sent(a):
        for q in range(4):
            landed(G.at[a, q, 0, 0, pl.ds(0, 3)], g_send.at[a, q, 0])
            landed(G.at[a, q, pl.ds(0, 3), :, 0], g_send.at[a, q, 1])
            landed(G.at[a, q, pl.ds(0, 3)], g_send.at[a, q, 2])

    def rows_chunk(a, z):
        parts = []
        for y in range(4):
            for ch in range(2):
                halves = [G[a, rh * 2 + ch, z, y].reshape(64, 128) for rh in range(2)]
                parts.append(jnp.concatenate(halves, axis=0))
        return parts

    def exchange_start(n, src, dst):
        for hop in (2, 1, 3):
            to = (at["x"] + hop) % 4
            pltpu.make_async_remote_copy(
                src_ref=src.at[to], dst_ref=dst.at[at["x"]],
                send_sem=a_send.at[n], recv_sem=a_recv.at[n],
                device_id=device(x=hop), device_id_type=MESH,
            ).start()
        dst[at["x"]] = src[at["x"]]

    def exchange_done(n, dst):
        landed(dst.at[pl.ds(0, 3)], a_recv.at[n])

    def exchange_sent(n, src):
        landed(src.at[pl.ds(0, 3)], a_send.at[n])

    def projections_out(layer):
        for kind in range(6):
            pltpu.make_async_remote_copy(
                src_ref=projections[kind].at[layer],
                dst_ref=WP.at[layer, pl.ds(kind * 64 + mine, 32)],
                send_sem=w_send.at[layer], recv_sem=w_recv.at[layer],
                device_id=partner, device_id_type=MESH,
            ).start()

    def output_over_x(layer):
        for part in range(4):
            for hop in (1, 3):
                pltpu.make_async_remote_copy(
                    src_ref=w_out.at[layer, pl.ds(part * 8, 8)],
                    dst_ref=WO[layer].at[pl.ds(pl.multiple_of(own_cols + part * 8, 8), 8)],
                    send_sem=o_sem.at[layer, 1], recv_sem=o_sem.at[layer, 1 + hop],
                    device_id=device(x=hop), device_id_type=MESH,
                ).start()

    def output_far_x(layer):
        for half, hop in enumerate((1, 3)):
            landed(WO[layer].at[pl.ds(0, 32)], o_sem.at[layer, 1 + hop])
            cols = pl.ds(pl.multiple_of((at["x"] + 4 - hop) % 4 * 64 + c * 32 + half * 16, 16), 16)
            pltpu.make_async_remote_copy(
                src_ref=WO[layer].at[cols], dst_ref=WO[layer].at[cols],
                send_sem=o_sem.at[layer, 7], recv_sem=o_sem.at[layer, 8],
                device_id=device(x=hop), device_id_type=MESH,
            ).start()

    def output_to_partner(layer):
        pltpu.make_async_remote_copy(
            src_ref=w_out.at[layer], dst_ref=WO[layer].at[pl.ds(own_cols, 32)],
            send_sem=o_sem.at[layer, 3], recv_sem=o_sem.at[layer, 9],
            device_id=partner, device_id_type=MESH,
        ).start()

    def output_pass_on(layer):
        landed(WO[layer].at[pl.ds(0, 32)], o_sem.at[layer, 8])
        for hop in (1, 2, 3):
            cols = pl.ds(pl.multiple_of(((at["x"] + hop) % 4) * 64 + c * 32, 32), 32)
            pltpu.make_async_remote_copy(
                src_ref=WO[layer].at[cols], dst_ref=WO[layer].at[cols],
                send_sem=o_sem.at[layer, 5], recv_sem=o_sem.at[layer, 6],
                device_id=partner, device_id_type=MESH,
            ).start()

    def output_in(layer):
        landed(WO[layer].at[pl.ds(0, 32)], o_sem.at[layer, 0])
        landed(WO[layer].at[pl.ds(0, 32)], o_sem.at[layer, 9])
        landed(WO[layer].at[pl.ds(0, 96)], o_sem.at[layer, 6])

    def output_sent(layer):
        landed(WO[layer].at[pl.ds(0, 64)], o_sem.at[layer, 1])
        landed(WO[layer].at[pl.ds(0, 32)], o_sem.at[layer, 7])
        landed(WO[layer].at[pl.ds(0, 32)], o_sem.at[layer, 3])
        landed(WO[layer].at[pl.ds(0, 96)], o_sem.at[layer, 5])

    def projections_in(layer):
        landed(WP.at[layer, pl.ds(0, 192)], w_local.at[layer])
        landed(WP.at[layer, pl.ds(0, 192)], w_recv.at[layer])
        scale = gain[layer:layer + 1, :]

        def fold(i, carry):
            rows = pl.ds(pl.multiple_of(i * 16, 16), 16)
            WP[layer, rows, :] = (WP[layer, rows, :].astype(F32) * scale).astype(BF16)
            return carry

        lax.fori_loop(0, 24, fold, 0)

    def weights_sent():
        for layer in range(2):
            landed(WP.at[layer, pl.ds(0, 192)], w_send.at[layer])
            output_sent(layer)

    def put_projected(projected, dst):
        out = projected.astype(BF16)
        for to in range(4):
            dst[to, 0:16, :] = out[to * 16:to * 16 + 16, :]
            dst[to, 16:32, :] = out[64 + to * 16:64 + to * 16 + 16, :]

    def project(layer):
        squares = jnp.zeros((128, 128), F32)
        acc = jnp.zeros((128, 256), F32)
        for on in (0, 1, 3, 2):
            if on:
                gather_last(layer, on)
            for ch in range(2):
                along = ORDERS[ch][2]
                came = (at[along] + 4 - on) % 4
                spots = [(came, other) if along == "z" else (other, came) for other in range(4)]
                parts, weights = [], []
                for z, y in spots:
                    parts.append(jnp.concatenate(
                        [G[layer, rh * 2 + ch, z, y].reshape(64, 128) for rh in range(2)], axis=0))
                    start = pl.multiple_of(z * 1024 + y * 256 + ch * 128, 128)
                    weights.append(WP[layer, 0:256, pl.ds(start, 128)])
                for part in parts:
                    wide = part.astype(F32)
                    squares += wide * wide
                acc += lax.dot_general(
                    jnp.concatenate(parts, axis=1), jnp.concatenate(weights, axis=1), LANES,
                    preferred_element_type=F32,
                )
        factor = lax.rsqrt(jnp.sum(squares, axis=1, keepdims=True) * (1.0 / 4096) + RMS_EPS)
        put_projected(acc * factor, SA4.at[layer])
        exchange_start(2 * layer, SA4.at[layer], RA4.at[layer])
        acc = jnp.zeros((128, 128), F32)
        for z in range(4):
            acc += lax.dot_general(
                jnp.concatenate(rows_chunk(layer, z), axis=1), WP[layer, 256:384, z * 1024:(z + 1) * 1024], LANES,
                preferred_element_type=F32,
            )
        put_projected(acc * factor, SB2.at[layer])
        exchange_start(2 * layer + 1, SB2.at[layer], RB2.at[layer])

    def active_rows():
        row = lax.broadcasted_iota(jnp.int32, (32, 32), 0)
        col = lax.broadcasted_iota(jnp.int32, (32, 32), 1)
        spread = jnp.broadcast_to(lens[0:1, :], (32, 32))
        return jnp.sum(jnp.where(row == col, spread, 0), axis=1, keepdims=True) > STEP

    low = lax.broadcasted_iota(jnp.int32, (32, 128), 1) < 64

    def swap(value):
        return pltpu.roll(value, 64, 1)

    own_lanes = (lax.broadcasted_iota(jnp.int32, (32, 256), 0) // 8
                 == lax.broadcasted_iota(jnp.int32, (32, 256), 1) // 64)

    def pack(layer):
        landed(ST.at[layer], st_sem.at[layer])

        def four(group, carry):
            for half in range(2):
                even, odd = [
                    ST[layer, group * 4 + half * 2 + i].reshape(256, 64) for i in range(2)
                ]
                both = jnp.concatenate([even, odd], axis=1)
                S16[layer, group, :, half * 128:(half + 1) * 128] = both.astype(BF16)
            return carry

        lax.fori_loop(0, 8, four, 0)

    def recur(layer):
        active = active_rows()
        first_sums, second_sums = [], []
        for h in range(4):
            cols = slice(h * 64, (h + 1) * 64)
            base = jnp.concatenate([dbase[layer:layer + 1, cols], rbase[layer:layer + 1, cols]], axis=1)
            rec_key = RA4[layer, h, :, 0:128].astype(F32)
            opened = jax.nn.sigmoid(base + RA4[layer, h, :, 128:256].astype(F32))
            dec_rate = jnp.where(low, jnp.exp(-0.6065306597126334 * opened), opened)
            both = rec_key * dec_rate
            key_rec = swap(rec_key)
            square = jnp.sum(jnp.where(low, key_rec * key_rec, 0.0), axis=1, keepdims=True)
            scale = 1.0 / jnp.maximum(jnp.sqrt(square), 1e-12)
            total = jnp.sum(jnp.where(low, 0.0, both * key_rec), axis=1, keepdims=True)
            first_sums.append(total * scale)
            second_sums.append(total)
            V8[pl.ds(h, 32, stride=8), :] = key_rec * -scale
            V8[pl.ds(4 + h, 32, stride=8), :] = both
            key_rate = jnp.where(active, swap(both), 0.0)
            PQ[pl.ds(h, 32, stride=8), :] = key_rate * scale
            PQ[pl.ds(4 + h, 32, stride=8), :] = key_rate
            DEC[pl.ds(h, 32, stride=8), :] = jnp.where(active, dec_rate, 1.0)
        for group in range(8):
            vectors = V8[group * 32:(group + 1) * 32, :]
            vectors = jnp.where(low, vectors, swap(vectors))
            vectors = jnp.where(own_lanes, jnp.concatenate([vectors, vectors], axis=1), 0.0).astype(BF16)
            got = lax.dot_general(vectors, S16[layer, group], LANES, preferred_element_type=F32)
            for half in range(2):
                M2[half, group * 32:(group + 1) * 32, :] = got[:, half * 128:(half + 1) * 128]
        exchange_done(2 * layer + 1, RB2.at[layer])

        def heads(base):
            return jnp.where(low, M2[base // 2 % 2, pl.ds(base, 32, stride=8), :],
                             M2[base // 2 % 2, pl.ds(base + 1, 32, stride=8), :])

        for half in range(2):
            even, odd = 2 * half, 2 * half + 1
            even_vg, odd_vg = RB2[layer, even].astype(F32), RB2[layer, odd].astype(F32)
            value = jnp.where(low, even_vg, swap(odd_vg))
            gate = jax.nn.sigmoid(jnp.where(low, swap(even_vg), odd_vg))
            sa, direct = heads(even), heads(4 + even)
            half_cols = slice(half * 128, (half + 1) * 128)
            SA[:, half_cols] = sa
            VA[:, half_cols] = value
            readout = (direct + sa * jnp.where(low, first_sums[even], first_sums[odd])
                       + value * jnp.where(low, second_sums[even], second_sums[odd]))

            def head_mean(data):
                return jnp.where(low, jnp.sum(jnp.where(low, data, 0.0), axis=1, keepdims=True),
                                 jnp.sum(jnp.where(low, 0.0, data), axis=1, keepdims=True)) * (1.0 / 64)

            readout = readout - head_mean(readout)
            normal = readout * lax.rsqrt(head_mean(readout * readout) + GROUP_EPS)
            rows = jnp.where(active, normal * ggain[layer:layer + 1, half_cols] * gate, 0.0).astype(BF16)
            for rh in range(2):
                GP[layer][tp, rh * 2 + half] = rows[rh * 16:(rh + 1) * 16, :]

    head_of = lax.broadcasted_iota(jnp.int32, (8, 256), 1) // 64
    row_of = lax.broadcasted_iota(jnp.int32, (8, 256), 0)

    def update(layer, start, count):
        for b in range(start, start + count):
            left = jnp.where(row_of < 4, jnp.broadcast_to(SA[b:b + 1, :], (8, 256)),
                             jnp.broadcast_to(VA[b:b + 1, :], (8, 256)))
            left = jnp.where(row_of % 4 == head_of, left, 0.0)
            delta = lax.dot_general(
                left.astype(BF16), PQ[b * 8:(b + 1) * 8, 0:64].astype(BF16), ROWS,
                preferred_element_type=F32,
            )
            for h in range(4):
                ST[layer, b, h] = (ST[layer, b, h] * DEC[b * 8 + h:b * 8 + h + 1, 0:64]
                                   + delta[h * 64:(h + 1) * 64, :])

    def plane_first(layer):
        here = GP[layer].at[tp]
        for hop_z in (2, 1, 3, 0):
            for hop_y in (2, 1, 3, 0):
                if hop_z or hop_y:
                    send(here, p_send.at[layer], p_recv.at[layer, hop_z], z=hop_z, y=hop_y)

    def plane_last(layer, hop_z):
        landed(GP[layer].at[pl.ds(0, 4 if hop_z else 3)], p_recv.at[layer, hop_z])

    gather_first(0)
    projections_out(0)
    pltpu.make_async_copy(state.at[0], ST.at[0], st_sem.at[0]).start()
    weights_local(1)
    pltpu.make_async_copy(state.at[1], ST.at[1], st_sem.at[1]).start()
    gather_middle(0)
    for copy in small:
        copy.wait()
    projections_in(0)
    pack(0)
    project(0)
    output_far_x(0)
    output_to_partner(0)
    projections_out(1)
    output_to_partner(1)
    exchange_done(0, RA4.at[0])
    recur(0)
    plane_first(0)
    output_pass_on(0)
    update(0, 0, 32)
    projections_in(1)
    output_in(0)

    def came(hop_z):
        plane_last(0, hop_z)
        return (at["z"] + 4 - hop_z) % 4

    out = output_product(GP0, WO0, [functools.partial(came, hop_z) for hop_z in (0, 1, 3, 2)])
    for q in range(4):
        rh, ch = q // 2, q % 2
        G[1, q, at["z"], at["y"], at["x"]] = out[rh * 16:(rh + 1) * 16, ch * 128:(ch + 1) * 128]
    gather_first(1)
    gather_middle(1)
    output_over_x(1)
    pack(1)
    project(1)
    output_far_x(1)
    exchange_done(2, RA4.at[1])
    recur(1)
    plane_first(1)
    output_pass_on(1)
    update(1, 0, 32)
    output_in(1)
    for hop_z in range(4):
        plane_last(1, hop_z)
    for a in range(2):
        gather_sent(a)
        exchange_sent(2 * a, SA4.at[a])
        exchange_sent(2 * a + 1, SB2.at[a])
        landed(GP[a].at[pl.ds(0, 15)], p_send.at[a])
    weights_sent()


def finish_kernel(state_in, rows, weight, state_out, mixed_out, mixed, sem):
    copies = [pltpu.make_async_copy(state_in.at[layer], state_out.at[layer], sem.at[layer]) for layer in range(2)]
    for copy in copies:
        copy.start()
    mixed[...] = output_product(rows, weight, [functools.partial(int, z) for z in range(4)])
    copies.append(pltpu.make_async_copy(mixed, mixed_out, sem.at[2]))
    copies[2].start()
    for copy in copies:
        copy.wait()


def local(tokens, lengths, norm_gain, w_recept, w_key, w_value, w_decay, w_rate, w_gate, w_out,
          decay_base, rate_base, group_gain, state):
    weights = [jnp.swapaxes(w, 1, 2) for w in (w_recept, w_key, w_decay, w_rate, w_value, w_gate, w_out)]
    hbm = pl.BlockSpec(memory_space=pltpu.HBM)
    vmem = pl.BlockSpec(memory_space=pltpu.VMEM)
    stepped, rows, columns = pl.pallas_call(
        step_kernel,
        out_shape=(pltpu.VMEM(state.shape, F32), pltpu.VMEM((16, 4, 16, 128), BF16), pltpu.VMEM((256, 4096), BF16)),
        in_specs=[hbm] * 14,
        out_specs=(vmem, vmem, vmem),
        scratch_shapes=[
            pltpu.VMEM((2, 4, 4, 4, 4, 16, 128), BF16),
            pltpu.VMEM((16, 4, 16, 128), BF16),
            pltpu.VMEM((2, 384, 4096), BF16),
            pltpu.VMEM((256, 4096), BF16),
            pltpu.VMEM((2, 4, 32, 256), BF16),
            pltpu.VMEM((2, 4, 32, 256), BF16),
            pltpu.VMEM((2, 4, 32, 128), BF16),
            pltpu.VMEM((2, 4, 32, 128), BF16),
            pltpu.VMEM((256, 128), F32),
            pltpu.VMEM((2, 256, 128), F32),
            pltpu.VMEM((2, 8, 256, 256), BF16),
            pltpu.VMEM((32, 256), F32),
            pltpu.VMEM((32, 256), F32),
            pltpu.VMEM((256, 128), F32),
            pltpu.VMEM((256, 128), F32),
            pltpu.VMEM((1, 32), jnp.int32),
            pltpu.VMEM((2, 4096), F32),
            pltpu.VMEM((2, 256), F32),
            pltpu.VMEM((2, 256), F32),
            pltpu.VMEM((2, 256), F32),
            pltpu.SemaphoreType.DMA((2, 4, 3)),
            pltpu.SemaphoreType.DMA((2, 4, 7)),
            pltpu.SemaphoreType.DMA((2,)),
            pltpu.SemaphoreType.DMA((2, 4)),
            pltpu.SemaphoreType.DMA((4,)),
            pltpu.SemaphoreType.DMA((4,)),
            pltpu.SemaphoreType.DMA((2,)),
            pltpu.SemaphoreType.DMA((2,)),
            pltpu.SemaphoreType.DMA((2,)),
            pltpu.SemaphoreType.DMA((2, 10)),
            pltpu.SemaphoreType.DMA((2,)),
            pltpu.SemaphoreType.DMA((4,)),
            pltpu.SemaphoreType.DMA((5,)),
        ],
        compiler_params=pltpu.CompilerParams(collective_id=0, has_side_effects=True, vmem_limit_bytes=44 << 20),
        name="decode_step",
    )(tokens, lengths.reshape(1, 32), norm_gain, *weights, decay_base, rate_base, group_gain, state)
    new_state, mixed = pl.pallas_call(
        finish_kernel,
        out_shape=(pltpu.HBM(state.shape, F32), pltpu.HBM((32, 256), BF16)),
        in_specs=[vmem] * 3,
        out_specs=(hbm, hbm),
        scratch_shapes=[pltpu.VMEM((32, 256), BF16), pltpu.SemaphoreType.DMA((3,))],
        compiler_params=pltpu.CompilerParams(vmem_limit_bytes=4 << 20),
        name="finish",
    )(stepped, rows, columns)
    return mixed, new_state


def solution(mesh):
    both = P(None, None, ("tp", "dp"))
    in_specs = (
        P("dp", "tp"), P("dp"), P(), both, both, both, both, both, both, both,
        P(None, "tp"), P(None, "tp"), P(None, "tp"), P(None, "dp", "tp", None, None),
    )
    out_specs = (P("dp", "tp"), P(None, "dp", "tp", None, None))
    return jax.shard_map(local, mesh=mesh, in_specs=in_specs, out_specs=out_specs, check_vma=False)
```

```python
import functools

import jax
import jax.numpy as jnp
from jax import lax
from jax.experimental import pallas as pl
from jax.experimental.pallas import tpu as pltpu
from jax.sharding import PartitionSpec as P

STEP = 16
RMS_EPS = 1e-06
GROUP_EPS = 0.00064
MESH = pl.DeviceIdType.MESH
F32 = jnp.float32
BF16 = jnp.bfloat16
ORDERS = (("y", "x", "z"), ("z", "x", "y"), ("y", "x", "z"), ("z", "x", "y"))
LANES = (((1,), (1,)), ((), ()))
ROWS = (((0,), (0,)), ((), ()))


def output_product(rows, weight, planes):
    acc = jnp.zeros((32, 256), F32)
    for plane in planes:
        z = plane()
        parts = [
            jnp.concatenate([rows[z * 4 + y, ch], rows[z * 4 + y, 2 + ch]], axis=0)
            for y in range(4) for ch in range(2)
        ]
        acc += lax.dot_general(
            jnp.concatenate(parts, axis=1), weight[:, pl.ds(pl.multiple_of(z * 1024, 1024), 1024)], LANES,
            preferred_element_type=F32,
        )
    return acc.astype(BF16)


def step_kernel(
    tok, lens_in, gain_in, w0, w1, w2, w3, w4, w5, w_out, dbase_in, rbase_in, ggain_in, state,
    ST, GP1, WO1,
    G, GP0, WP, WO0, SA4, RA4, SB2, RB2, V8, M2, S16, SA, VA, PQ, DEC, lens, gain, dbase, rbase, ggain,
    g_send, g_recv, p_send, p_recv, a_send, a_recv, w_local, w_send, w_recv, o_sem, st_sem, tok_sem, small_sem,
):
    tp, dp = lax.axis_index("tp"), lax.axis_index("dp")
    c = dp % 2
    at = {"z": tp // 4, "y": tp % 4, "x": dp // 2}
    projections = (w0, w1, w2, w3, w4, w5)
    GP, WO = (GP0, GP1), (WO0, WO1)

    def device(**hops):
        to = {axis: (at[axis] + hops.get(axis, 0)) % 4 for axis in "xyz"}
        return (to["z"] * 4 + to["y"], to["x"] * 2 + c)

    partner = (tp, at["x"] * 2 + 1 - c)

    barrier = pltpu.get_barrier_semaphore()
    peers = [
        dict(x=hx, y=hy, z=hz) for hx in range(4) for hy in range(4) for hz in range(4)
        if 0 in (hx, hy, hz) and (hx, hy, hz) != (0, 0, 0)
    ]
    peers.sort(key=lambda peer: -sum(min(hop, 4 - hop) for hop in peer.values()))
    for peer in peers:
        pl.semaphore_signal(barrier, inc=1, device_id=device(**peer), device_id_type=MESH)
    pl.semaphore_signal(barrier, inc=1, device_id=partner, device_id_type=MESH)

    tok_copies = []
    for q in range(4):
        rh, ch = q // 2, q % 2
        tok_copies.append(pltpu.make_async_copy(
            tok.at[pl.ds(rh * 16, 16), pl.ds(ch * 128, 128)],
            G.at[0, q, at["z"], at["y"], at["x"]],
            tok_sem.at[q],
        ))
        tok_copies[-1].start()
    mine = pl.multiple_of(c * 32, 32)
    own_cols = pl.multiple_of(dp * 32, 32)

    def weights_local(layer):
        for kind in range(6):
            pltpu.make_async_copy(
                projections[kind].at[layer],
                WP.at[layer, pl.ds(kind * 64 + mine, 32)],
                w_local.at[layer],
            ).start()
        pltpu.make_async_copy(w_out.at[layer], WO[layer].at[pl.ds(own_cols, 32)], o_sem.at[layer, 0]).start()

    small = [
        pltpu.make_async_copy(src, dst, small_sem.at[i])
        for i, (src, dst) in enumerate(
            ((lens_in, lens), (gain_in, gain), (dbase_in, dbase), (rbase_in, rbase), (ggain_in, ggain)))
    ]
    for copy in small:
        copy.start()
    weights_local(0)
    pl.semaphore_wait(barrier, len(peers) + 1)

    def block(a, q, free, moved=None):
        idx = [moved[ax] if moved and ax in moved else at[ax] for ax in "zyx"]
        idx = [slice(None) if ax in free else i for ax, i in zip("zyx", idx)]
        return G.at[(a, q, *idx)]

    def send(ref, send_sem, recv_sem, **hops):
        pltpu.make_async_remote_copy(
            src_ref=ref, dst_ref=ref, send_sem=send_sem, recv_sem=recv_sem,
            device_id=device(**hops), device_id_type=MESH,
        ).start()

    def landed(ref, sem):
        pltpu.make_async_copy(ref, ref, sem).wait()

    def gather_first(a):
        for q in range(4):
            first, second, third = ORDERS[q]
            if a == 0:
                tok_copies[q].wait()
            for hop in (2, 1, 3):
                send(block(a, q, ()), g_send.at[a, q, 0], g_recv.at[a, q, 0], **{first: hop})
            for over in (2, 1, 3):
                for hop in (2, 1, 3, 0):
                    send(block(a, q, ()), g_send.at[a, q, 1], g_recv.at[a, q, over],
                         **{first: hop, second: over})

    def gather_middle(a):
        for q in range(4):
            first, second, third = ORDERS[q]
            landed(G.at[a, q, 0, 0, pl.ds(0, 3)], g_recv.at[a, q, 0])
            for on in (2, 1, 3):
                send(block(a, q, first), g_send.at[a, q, 2], g_recv.at[a, q, 3 + on], **{third: on})
        if a == 0:
            output_over_x(0)
        for over in (1, 3, 2):
            for q in range(4):
                first, second, third = ORDERS[q]
                landed(G.at[a, q, 0, 0], g_recv.at[a, q, over])
                line = {second: (at[second] + 4 - over) % 4}
                for on in (2, 1, 3):
                    send(block(a, q, first, line), g_send.at[a, q, 2], g_recv.at[a, q, 3 + on], **{third: on})

    def gather_last(a, on):
        for q in range(4):
            landed(G.at[a, q, 0], g_recv.at[a, q, 3 + on])

    def gather_sent(a):
        for q in range(4):
            landed(G.at[a, q, 0, 0, pl.ds(0, 3)], g_send.at[a, q, 0])
            landed(G.at[a, q, pl.ds(0, 3), :, 0], g_send.at[a, q, 1])
            landed(G.at[a, q, pl.ds(0, 3)], g_send.at[a, q, 2])

    def rows_chunk(a, z):
        parts = []
        for y in range(4):
            for ch in range(2):
                halves = [G[a, rh * 2 + ch, z, y].reshape(64, 128) for rh in range(2)]
                parts.append(jnp.concatenate(halves, axis=0))
        return parts

    def exchange_start(n, src, dst):
        for hop in (2, 1, 3):
            to = (at["x"] + hop) % 4
            pltpu.make_async_remote_copy(
                src_ref=src.at[to], dst_ref=dst.at[at["x"]],
                send_sem=a_send.at[n], recv_sem=a_recv.at[n],
                device_id=device(x=hop), device_id_type=MESH,
            ).start()
        dst[at["x"]] = src[at["x"]]

    def exchange_done(n, dst):
        landed(dst.at[pl.ds(0, 3)], a_recv.at[n])

    def exchange_sent(n, src):
        landed(src.at[pl.ds(0, 3)], a_send.at[n])

    def projections_out(layer):
        for kind in range(6):
            pltpu.make_async_remote_copy(
                src_ref=projections[kind].at[layer],
                dst_ref=WP.at[layer, pl.ds(kind * 64 + mine, 32)],
                send_sem=w_send.at[layer], recv_sem=w_recv.at[layer],
                device_id=partner, device_id_type=MESH,
            ).start()

    def output_over_x(layer):
        for part in range(4):
            for hop in (1, 3):
                pltpu.make_async_remote_copy(
                    src_ref=w_out.at[layer, pl.ds(part * 8, 8)],
                    dst_ref=WO[layer].at[pl.ds(pl.multiple_of(own_cols + part * 8, 8), 8)],
                    send_sem=o_sem.at[layer, 1], recv_sem=o_sem.at[layer, 1 + hop],
                    device_id=device(x=hop), device_id_type=MESH,
                ).start()

    def output_far_x(layer):
        for half, hop in enumerate((1, 3)):
            landed(WO[layer].at[pl.ds(0, 32)], o_sem.at[layer, 1 + hop])
            cols = pl.ds(pl.multiple_of((at["x"] + 4 - hop) % 4 * 64 + c * 32 + half * 16, 16), 16)
            pltpu.make_async_remote_copy(
                src_ref=WO[layer].at[cols], dst_ref=WO[layer].at[cols],
                send_sem=o_sem.at[layer, 7], recv_sem=o_sem.at[layer, 8],
                device_id=device(x=hop), device_id_type=MESH,
            ).start()

    def output_to_partner(layer):
        pltpu.make_async_remote_copy(
            src_ref=w_out.at[layer], dst_ref=WO[layer].at[pl.ds(own_cols, 32)],
            send_sem=o_sem.at[layer, 3], recv_sem=o_sem.at[layer, 9],
            device_id=partner, device_id_type=MESH,
        ).start()

    def output_pass_on(layer):
        landed(WO[layer].at[pl.ds(0, 32)], o_sem.at[layer, 8])
        for hop in (1, 2, 3):
            cols = pl.ds(pl.multiple_of(((at["x"] + hop) % 4) * 64 + c * 32, 32), 32)
            pltpu.make_async_remote_copy(
                src_ref=WO[layer].at[cols], dst_ref=WO[layer].at[cols],
                send_sem=o_sem.at[layer, 5], recv_sem=o_sem.at[layer, 6],
                device_id=partner, device_id_type=MESH,
            ).start()

    def output_in(layer):
        landed(WO[layer].at[pl.ds(0, 32)], o_sem.at[layer, 0])
        landed(WO[layer].at[pl.ds(0, 32)], o_sem.at[layer, 9])
        landed(WO[layer].at[pl.ds(0, 96)], o_sem.at[layer, 6])

    def output_sent(layer):
        landed(WO[layer].at[pl.ds(0, 64)], o_sem.at[layer, 1])
        landed(WO[layer].at[pl.ds(0, 32)], o_sem.at[layer, 7])
        landed(WO[layer].at[pl.ds(0, 32)], o_sem.at[layer, 3])
        landed(WO[layer].at[pl.ds(0, 96)], o_sem.at[layer, 5])

    def projections_in(layer):
        landed(WP.at[layer, pl.ds(0, 192)], w_local.at[layer])
        landed(WP.at[layer, pl.ds(0, 192)], w_recv.at[layer])
        scale = gain[layer:layer + 1, :]

        def fold(i, carry):
            rows = pl.ds(pl.multiple_of(i * 16, 16), 16)
            WP[layer, rows, :] = (WP[layer, rows, :].astype(F32) * scale).astype(BF16)
            return carry

        lax.fori_loop(0, 24, fold, 0)

    def weights_sent():
        for layer in range(2):
            landed(WP.at[layer, pl.ds(0, 192)], w_send.at[layer])
            output_sent(layer)

    def put_projected(projected, dst):
        out = projected.astype(BF16)
        for to in range(4):
            dst[to, 0:16, :] = out[to * 16:to * 16 + 16, :]
            dst[to, 16:32, :] = out[64 + to * 16:64 + to * 16 + 16, :]

    def project(layer):
        squares = jnp.zeros((128, 128), F32)
        acc = jnp.zeros((128, 256), F32)
        for on in (0, 1, 3, 2):
            if on:
                gather_last(layer, on)
            for ch in range(2):
                along = ORDERS[ch][2]
                came = (at[along] + 4 - on) % 4
                spots = [(came, other) if along == "z" else (other, came) for other in range(4)]
                parts, weights = [], []
                for z, y in spots:
                    parts.append(jnp.concatenate(
                        [G[layer, rh * 2 + ch, z, y].reshape(64, 128) for rh in range(2)], axis=0))
                    start = pl.multiple_of(z * 1024 + y * 256 + ch * 128, 128)
                    weights.append(WP[layer, 0:256, pl.ds(start, 128)])
                for part in parts:
                    wide = part.astype(F32)
                    squares += wide * wide
                acc += lax.dot_general(
                    jnp.concatenate(parts, axis=1), jnp.concatenate(weights, axis=1), LANES,
                    preferred_element_type=F32,
                )
        factor = lax.rsqrt(jnp.sum(squares, axis=1, keepdims=True) * (1.0 / 4096) + RMS_EPS)
        put_projected(acc * factor, SA4.at[layer])
        exchange_start(2 * layer, SA4.at[layer], RA4.at[layer])
        acc = jnp.zeros((128, 128), F32)
        for z in range(4):
            acc += lax.dot_general(
                jnp.concatenate(rows_chunk(layer, z), axis=1), WP[layer, 256:384, z * 1024:(z + 1) * 1024], LANES,
                preferred_element_type=F32,
            )
        put_projected(acc * factor, SB2.at[layer])
        exchange_start(2 * layer + 1, SB2.at[layer], RB2.at[layer])

    def active_rows():
        row = lax.broadcasted_iota(jnp.int32, (32, 32), 0)
        col = lax.broadcasted_iota(jnp.int32, (32, 32), 1)
        spread = jnp.broadcast_to(lens[0:1, :], (32, 32))
        return jnp.sum(jnp.where(row == col, spread, 0), axis=1, keepdims=True) > STEP

    low = lax.broadcasted_iota(jnp.int32, (32, 128), 1) < 64

    def swap(value):
        return pltpu.roll(value, 64, 1)

    own_lanes = (lax.broadcasted_iota(jnp.int32, (32, 256), 0) // 8
                 == lax.broadcasted_iota(jnp.int32, (32, 256), 1) // 64)

    def pack(layer):
        landed(ST.at[layer], st_sem.at[layer])

        def four(group, carry):
            for half in range(2):
                even, odd = [
                    ST[layer, group * 4 + half * 2 + i].reshape(256, 64) for i in range(2)
                ]
                both = jnp.concatenate([even, odd], axis=1)
                S16[layer, group, :, half * 128:(half + 1) * 128] = both.astype(BF16)
            return carry

        lax.fori_loop(0, 8, four, 0)

    def head_vectors(layer, h):
        cols = slice(h * 64, (h + 1) * 64)
        base = jnp.concatenate([dbase[layer:layer + 1, cols], rbase[layer:layer + 1, cols]], axis=1)
        rec_key = RA4[layer, h, :, 0:128].astype(F32)
        opened = jax.nn.sigmoid(base + RA4[layer, h, :, 128:256].astype(F32))
        dec_rate = jnp.where(low, jnp.exp(-0.6065306597126334 * opened), opened)
        both = rec_key * dec_rate
        key_rec = swap(rec_key)
        square = jnp.sum(jnp.where(low, key_rec * key_rec, 0.0), axis=1, keepdims=True)
        scale = 1.0 / jnp.maximum(jnp.sqrt(square), 1e-12)
        return dec_rate, both, key_rec, scale

    def update_vectors(layer):
        active = active_rows()
        for h in range(4):
            dec_rate, both, key_rec, scale = head_vectors(layer, h)
            key_rate = jnp.where(active, swap(both), 0.0)
            PQ[pl.ds(h, 32, stride=8), :] = key_rate * scale
            PQ[pl.ds(4 + h, 32, stride=8), :] = key_rate
            DEC[pl.ds(h, 32, stride=8), :] = jnp.where(active, dec_rate, 1.0)

    def recur(layer):
        active = active_rows()
        first_sums, second_sums = [], []
        for h in range(4):
            dec_rate, both, key_rec, scale = head_vectors(layer, h)
            total = jnp.sum(jnp.where(low, 0.0, both * key_rec), axis=1, keepdims=True)
            first_sums.append(total * scale)
            second_sums.append(total)
            V8[pl.ds(h, 32, stride=8), :] = key_rec * -scale
            V8[pl.ds(4 + h, 32, stride=8), :] = both
        for group in range(8):
            vectors = V8[group * 32:(group + 1) * 32, :]
            vectors = jnp.where(low, vectors, swap(vectors))
            vectors = jnp.where(own_lanes, jnp.concatenate([vectors, vectors], axis=1), 0.0).astype(BF16)
            got = lax.dot_general(vectors, S16[layer, group], LANES, preferred_element_type=F32)
            for half in range(2):
                M2[half, group * 32:(group + 1) * 32, :] = got[:, half * 128:(half + 1) * 128]
        exchange_done(2 * layer + 1, RB2.at[layer])

        def heads(base):
            return jnp.where(low, M2[base // 2 % 2, pl.ds(base, 32, stride=8), :],
                             M2[base // 2 % 2, pl.ds(base + 1, 32, stride=8), :])

        for half in range(2):
            even, odd = 2 * half, 2 * half + 1
            even_vg, odd_vg = RB2[layer, even].astype(F32), RB2[layer, odd].astype(F32)
            value = jnp.where(low, even_vg, swap(odd_vg))
            gate = jax.nn.sigmoid(jnp.where(low, swap(even_vg), odd_vg))
            sa, direct = heads(even), heads(4 + even)
            half_cols = slice(half * 128, (half + 1) * 128)
            SA[:, half_cols] = sa
            VA[:, half_cols] = value
            readout = (direct + sa * jnp.where(low, first_sums[even], first_sums[odd])
                       + value * jnp.where(low, second_sums[even], second_sums[odd]))

            def head_mean(data):
                return jnp.where(low, jnp.sum(jnp.where(low, data, 0.0), axis=1, keepdims=True),
                                 jnp.sum(jnp.where(low, 0.0, data), axis=1, keepdims=True)) * (1.0 / 64)

            readout = readout - head_mean(readout)
            normal = readout * lax.rsqrt(head_mean(readout * readout) + GROUP_EPS)
            rows = jnp.where(active, normal * ggain[layer:layer + 1, half_cols] * gate, 0.0).astype(BF16)
            for rh in range(2):
                GP[layer][tp, rh * 2 + half] = rows[rh * 16:(rh + 1) * 16, :]

    head_of = lax.broadcasted_iota(jnp.int32, (8, 256), 1) // 64
    row_of = lax.broadcasted_iota(jnp.int32, (8, 256), 0)

    def update(layer, start, count):
        for b in range(start, start + count):
            left = jnp.where(row_of < 4, jnp.broadcast_to(SA[b:b + 1, :], (8, 256)),
                             jnp.broadcast_to(VA[b:b + 1, :], (8, 256)))
            left = jnp.where(row_of % 4 == head_of, left, 0.0)
            delta = lax.dot_general(
                left.astype(BF16), PQ[b * 8:(b + 1) * 8, 0:64].astype(BF16), ROWS,
                preferred_element_type=F32,
            )
            for h in range(4):
                ST[layer, b, h] = (ST[layer, b, h] * DEC[b * 8 + h:b * 8 + h + 1, 0:64]
                                   + delta[h * 64:(h + 1) * 64, :])

    def plane_first(layer):
        here = GP[layer].at[tp]
        for hop_z in (2, 1, 3, 0):
            for hop_y in (2, 1, 3, 0):
                if hop_z or hop_y:
                    send(here, p_send.at[layer], p_recv.at[layer, hop_z], z=hop_z, y=hop_y)

    def plane_last(layer, hop_z):
        landed(GP[layer].at[pl.ds(0, 4 if hop_z else 3)], p_recv.at[layer, hop_z])

    gather_first(0)
    projections_out(0)
    pltpu.make_async_copy(state.at[0], ST.at[0], st_sem.at[0]).start()
    weights_local(1)
    pltpu.make_async_copy(state.at[1], ST.at[1], st_sem.at[1]).start()
    gather_middle(0)
    for copy in small:
        copy.wait()
    projections_in(0)
    pack(0)
    project(0)
    output_far_x(0)
    output_to_partner(0)
    projections_out(1)
    output_to_partner(1)
    exchange_done(0, RA4.at[0])
    recur(0)
    plane_first(0)
    output_pass_on(0)
    update_vectors(0)
    update(0, 0, 32)
    projections_in(1)
    output_in(0)

    def came(hop_z):
        plane_last(0, hop_z)
        return (at["z"] + 4 - hop_z) % 4

    out = output_product(GP0, WO0, [functools.partial(came, hop_z) for hop_z in (0, 1, 3, 2)])
    for q in range(4):
        rh, ch = q // 2, q % 2
        G[1, q, at["z"], at["y"], at["x"]] = out[rh * 16:(rh + 1) * 16, ch * 128:(ch + 1) * 128]
    gather_first(1)
    gather_middle(1)
    output_over_x(1)
    pack(1)
    project(1)
    output_far_x(1)
    exchange_done(2, RA4.at[1])
    recur(1)
    plane_first(1)
    output_pass_on(1)
    update_vectors(1)
    update(1, 0, 32)
    output_in(1)
    for hop_z in range(4):
        plane_last(1, hop_z)
    for a in range(2):
        gather_sent(a)
        exchange_sent(2 * a, SA4.at[a])
        exchange_sent(2 * a + 1, SB2.at[a])
        landed(GP[a].at[pl.ds(0, 15)], p_send.at[a])
    weights_sent()


def finish_kernel(state_in, rows, weight, state_out, mixed_out, mixed, sem):
    copies = [pltpu.make_async_copy(state_in.at[layer], state_out.at[layer], sem.at[layer]) for layer in range(2)]
    for copy in copies:
        copy.start()
    mixed[...] = output_product(rows, weight, [functools.partial(int, z) for z in range(4)])
    copies.append(pltpu.make_async_copy(mixed, mixed_out, sem.at[2]))
    copies[2].start()
    for copy in copies:
        copy.wait()


def local(tokens, lengths, norm_gain, w_recept, w_key, w_value, w_decay, w_rate, w_gate, w_out,
          decay_base, rate_base, group_gain, state):
    weights = [jnp.swapaxes(w, 1, 2) for w in (w_recept, w_key, w_decay, w_rate, w_value, w_gate, w_out)]
    hbm = pl.BlockSpec(memory_space=pltpu.HBM)
    vmem = pl.BlockSpec(memory_space=pltpu.VMEM)
    stepped, rows, columns = pl.pallas_call(
        step_kernel,
        out_shape=(pltpu.VMEM(state.shape, F32), pltpu.VMEM((16, 4, 16, 128), BF16), pltpu.VMEM((256, 4096), BF16)),
        in_specs=[hbm] * 14,
        out_specs=(vmem, vmem, vmem),
        scratch_shapes=[
            pltpu.VMEM((2, 4, 4, 4, 4, 16, 128), BF16),
            pltpu.VMEM((16, 4, 16, 128), BF16),
            pltpu.VMEM((2, 384, 4096), BF16),
            pltpu.VMEM((256, 4096), BF16),
            pltpu.VMEM((2, 4, 32, 256), BF16),
            pltpu.VMEM((2, 4, 32, 256), BF16),
            pltpu.VMEM((2, 4, 32, 128), BF16),
            pltpu.VMEM((2, 4, 32, 128), BF16),
            pltpu.VMEM((256, 128), F32),
            pltpu.VMEM((2, 256, 128), F32),
            pltpu.VMEM((2, 8, 256, 256), BF16),
            pltpu.VMEM((32, 256), F32),
            pltpu.VMEM((32, 256), F32),
            pltpu.VMEM((256, 128), F32),
            pltpu.VMEM((256, 128), F32),
            pltpu.VMEM((1, 32), jnp.int32),
            pltpu.VMEM((2, 4096), F32),
            pltpu.VMEM((2, 256), F32),
            pltpu.VMEM((2, 256), F32),
            pltpu.VMEM((2, 256), F32),
            pltpu.SemaphoreType.DMA((2, 4, 3)),
            pltpu.SemaphoreType.DMA((2, 4, 7)),
            pltpu.SemaphoreType.DMA((2,)),
            pltpu.SemaphoreType.DMA((2, 4)),
            pltpu.SemaphoreType.DMA((4,)),
            pltpu.SemaphoreType.DMA((4,)),
            pltpu.SemaphoreType.DMA((2,)),
            pltpu.SemaphoreType.DMA((2,)),
            pltpu.SemaphoreType.DMA((2,)),
            pltpu.SemaphoreType.DMA((2, 10)),
            pltpu.SemaphoreType.DMA((2,)),
            pltpu.SemaphoreType.DMA((4,)),
            pltpu.SemaphoreType.DMA((5,)),
        ],
        compiler_params=pltpu.CompilerParams(collective_id=0, has_side_effects=True, vmem_limit_bytes=44 << 20),
        name="decode_step",
    )(tokens, lengths.reshape(1, 32), norm_gain, *weights, decay_base, rate_base, group_gain, state)
    new_state, mixed = pl.pallas_call(
        finish_kernel,
        out_shape=(pltpu.HBM(state.shape, F32), pltpu.HBM((32, 256), BF16)),
        in_specs=[vmem] * 3,
        out_specs=(hbm, hbm),
        scratch_shapes=[pltpu.VMEM((32, 256), BF16), pltpu.SemaphoreType.DMA((3,))],
        compiler_params=pltpu.CompilerParams(vmem_limit_bytes=4 << 20),
        name="finish",
    )(stepped, rows, columns)
    return mixed, new_state


def solution(mesh):
    both = P(None, None, ("tp", "dp"))
    in_specs = (
        P("dp", "tp"), P("dp"), P(), both, both, both, both, both, both, both,
        P(None, "tp"), P(None, "tp"), P(None, "tp"), P(None, "dp", "tp", None, None),
    )
    out_specs = (P("dp", "tp"), P(None, "dp", "tp", None, None))
    return jax.shard_map(local, mesh=mesh, in_specs=in_specs, out_specs=out_specs, check_vma=False)
```

```python
import functools

import jax
import jax.numpy as jnp
from jax import lax
from jax.experimental import pallas as pl
from jax.experimental.pallas import tpu as pltpu
from jax.sharding import PartitionSpec as P

STEP = 16
RMS_EPS = 1e-06
GROUP_EPS = 0.00064
MESH = pl.DeviceIdType.MESH
F32 = jnp.float32
BF16 = jnp.bfloat16
ORDERS = (("x", "y", "z"), ("x", "z", "y"), ("y", "x", "z"), ("z", "x", "y"))
LANES = (((1,), (1,)), ((), ()))
ROWS = (((0,), (0,)), ((), ()))


def output_product(rows, weight, planes):
    acc = jnp.zeros((32, 256), F32)
    for plane in planes:
        z = plane()
        parts = [
            jnp.concatenate([rows[z * 4 + y, ch], rows[z * 4 + y, 2 + ch]], axis=0)
            for y in range(4) for ch in range(2)
        ]
        acc += lax.dot_general(
            jnp.concatenate(parts, axis=1), weight[:, pl.ds(pl.multiple_of(z * 1024, 1024), 1024)], LANES,
            preferred_element_type=F32,
        )
    return acc.astype(BF16)


def step_kernel(
    tok, lens_in, gain_in, w0, w1, w2, w3, w4, w5, w_out, dbase_in, rbase_in, ggain_in, state,
    ST, GP1, WO1,
    G, GP0, WP, WO0, SA4, RA4, SB2, RB2, V8, M2, S16, SA, VA, PQ, DEC, lens, gain, dbase, rbase, ggain,
    g_send, g_recv, p_send, p_recv, a_send, a_recv, w_local, w_send, w_recv, o_sem, st_sem, tok_sem, small_sem,
):
    tp, dp = lax.axis_index("tp"), lax.axis_index("dp")
    c = dp % 2
    at = {"z": tp // 4, "y": tp % 4, "x": dp // 2}
    projections = (w0, w1, w2, w3, w4, w5)
    GP, WO = (GP0, GP1), (WO0, WO1)

    def device(**hops):
        to = {axis: (at[axis] + hops.get(axis, 0)) % 4 for axis in "xyz"}
        return (to["z"] * 4 + to["y"], to["x"] * 2 + c)

    partner = (tp, at["x"] * 2 + 1 - c)

    barrier = pltpu.get_barrier_semaphore()
    peers = [
        dict(x=hx, y=hy, z=hz) for hx in range(4) for hy in range(4) for hz in range(4)
        if 0 in (hx, hy, hz) and (hx, hy, hz) != (0, 0, 0)
    ]
    peers.sort(key=lambda peer: -sum(min(hop, 4 - hop) for hop in peer.values()))
    for peer in peers:
        pl.semaphore_signal(barrier, inc=1, device_id=device(**peer), device_id_type=MESH)
    pl.semaphore_signal(barrier, inc=1, device_id=partner, device_id_type=MESH)

    tok_copies = []
    for q in range(4):
        rh, ch = q // 2, q % 2
        tok_copies.append(pltpu.make_async_copy(
            tok.at[pl.ds(rh * 16, 16), pl.ds(ch * 128, 128)],
            G.at[0, q, at["z"], at["y"], at["x"]],
            tok_sem.at[q],
        ))
        tok_copies[-1].start()
    mine = pl.multiple_of(c * 32, 32)
    own_cols = pl.multiple_of(dp * 32, 32)

    def weights_local(layer):
        for kind in range(6):
            pltpu.make_async_copy(
                projections[kind].at[layer],
                WP.at[layer, pl.ds(kind * 64 + mine, 32)],
                w_local.at[layer],
            ).start()
        pltpu.make_async_copy(w_out.at[layer], WO[layer].at[pl.ds(own_cols, 32)], o_sem.at[layer, 0]).start()

    small = [
        pltpu.make_async_copy(src, dst, small_sem.at[i])
        for i, (src, dst) in enumerate(
            ((lens_in, lens), (gain_in, gain), (dbase_in, dbase), (rbase_in, rbase), (ggain_in, ggain)))
    ]
    for copy in small:
        copy.start()
    weights_local(0)
    pl.semaphore_wait(barrier, len(peers) + 1)

    def block(a, q, free, moved=None):
        idx = [moved[ax] if moved and ax in moved else at[ax] for ax in "zyx"]
        idx = [slice(None) if ax in free else i for ax, i in zip("zyx", idx)]
        return G.at[(a, q, *idx)]

    def send(ref, send_sem, recv_sem, **hops):
        pltpu.make_async_remote_copy(
            src_ref=ref, dst_ref=ref, send_sem=send_sem, recv_sem=recv_sem,
            device_id=device(**hops), device_id_type=MESH,
        ).start()

    def landed(ref, sem):
        pltpu.make_async_copy(ref, ref, sem).wait()

    def gather_first(a):
        for q in range(4):
            first, second, third = ORDERS[q]
            if a == 0:
                tok_copies[q].wait()
            for hop in (2, 1, 3):
                send(block(a, q, ()), g_send.at[a, q, 0], g_recv.at[a, q, 0], **{first: hop})
            for over in (2, 1, 3):
                for hop in (2, 1, 3, 0):
                    send(block(a, q, ()), g_send.at[a, q, 1], g_recv.at[a, q, over],
                         **{first: hop, second: over})

    def gather_middle(a):
        for q in range(4):
            first, second, third = ORDERS[q]
            landed(G.at[a, q, 0, 0, pl.ds(0, 3)], g_recv.at[a, q, 0])
            for on in (2, 1, 3):
                send(block(a, q, first), g_send.at[a, q, 2], g_recv.at[a, q, 3 + on], **{third: on})
        if a == 0:
            output_over_x(0)
        for over in (1, 3, 2):
            for q in range(4):
                first, second, third = ORDERS[q]
                landed(G.at[a, q, 0, 0], g_recv.at[a, q, over])
                line = {second: (at[second] + 4 - over) % 4}
                for on in (2, 1, 3):
                    send(block(a, q, first, line), g_send.at[a, q, 2], g_recv.at[a, q, 3 + on], **{third: on})

    def gather_last(a, on):
        for q in range(4):
            landed(G.at[a, q, 0], g_recv.at[a, q, 3 + on])

    def gather_sent(a):
        for q in range(4):
            landed(G.at[a, q, 0, 0, pl.ds(0, 3)], g_send.at[a, q, 0])
            landed(G.at[a, q, pl.ds(0, 3), :, 0], g_send.at[a, q, 1])
            landed(G.at[a, q, pl.ds(0, 3)], g_send.at[a, q, 2])

    def rows_chunk(a, z):
        parts = []
        for y in range(4):
            for ch in range(2):
                halves = [G[a, rh * 2 + ch, z, y].reshape(64, 128) for rh in range(2)]
                parts.append(jnp.concatenate(halves, axis=0))
        return parts

    def exchange_start(n, src, dst):
        for hop in (2, 1, 3):
            to = (at["x"] + hop) % 4
            pltpu.make_async_remote_copy(
                src_ref=src.at[to], dst_ref=dst.at[at["x"]],
                send_sem=a_send.at[n], recv_sem=a_recv.at[n],
                device_id=device(x=hop), device_id_type=MESH,
            ).start()
        dst[at["x"]] = src[at["x"]]

    def exchange_done(n, dst):
        landed(dst.at[pl.ds(0, 3)], a_recv.at[n])

    def exchange_sent(n, src):
        landed(src.at[pl.ds(0, 3)], a_send.at[n])

    def projections_out(layer):
        for kind in range(6):
            pltpu.make_async_remote_copy(
                src_ref=projections[kind].at[layer],
                dst_ref=WP.at[layer, pl.ds(kind * 64 + mine, 32)],
                send_sem=w_send.at[layer], recv_sem=w_recv.at[layer],
                device_id=partner, device_id_type=MESH,
            ).start()

    def output_over_x(layer):
        for part in range(4):
            for hop in (1, 3):
                pltpu.make_async_remote_copy(
                    src_ref=w_out.at[layer, pl.ds(part * 8, 8)],
                    dst_ref=WO[layer].at[pl.ds(pl.multiple_of(own_cols + part * 8, 8), 8)],
                    send_sem=o_sem.at[layer, 1], recv_sem=o_sem.at[layer, 1 + hop],
                    device_id=device(x=hop), device_id_type=MESH,
                ).start()

    def output_far_x(layer):
        for half, hop in enumerate((1, 3)):
            landed(WO[layer].at[pl.ds(0, 32)], o_sem.at[layer, 1 + hop])
            cols = pl.ds(pl.multiple_of((at["x"] + 4 - hop) % 4 * 64 + c * 32 + half * 16, 16), 16)
            pltpu.make_async_remote_copy(
                src_ref=WO[layer].at[cols], dst_ref=WO[layer].at[cols],
                send_sem=o_sem.at[layer, 7], recv_sem=o_sem.at[layer, 8],
                device_id=device(x=hop), device_id_type=MESH,
            ).start()

    def output_to_partner(layer):
        pltpu.make_async_remote_copy(
            src_ref=w_out.at[layer], dst_ref=WO[layer].at[pl.ds(own_cols, 32)],
            send_sem=o_sem.at[layer, 3], recv_sem=o_sem.at[layer, 9],
            device_id=partner, device_id_type=MESH,
        ).start()

    def output_pass_on(layer):
        landed(WO[layer].at[pl.ds(0, 32)], o_sem.at[layer, 8])
        for hop in (1, 2, 3):
            cols = pl.ds(pl.multiple_of(((at["x"] + hop) % 4) * 64 + c * 32, 32), 32)
            pltpu.make_async_remote_copy(
                src_ref=WO[layer].at[cols], dst_ref=WO[layer].at[cols],
                send_sem=o_sem.at[layer, 5], recv_sem=o_sem.at[layer, 6],
                device_id=partner, device_id_type=MESH,
            ).start()

    def output_in(layer):
        landed(WO[layer].at[pl.ds(0, 32)], o_sem.at[layer, 0])
        landed(WO[layer].at[pl.ds(0, 32)], o_sem.at[layer, 9])
        landed(WO[layer].at[pl.ds(0, 96)], o_sem.at[layer, 6])

    def output_sent(layer):
        landed(WO[layer].at[pl.ds(0, 64)], o_sem.at[layer, 1])
        landed(WO[layer].at[pl.ds(0, 32)], o_sem.at[layer, 7])
        landed(WO[layer].at[pl.ds(0, 32)], o_sem.at[layer, 3])
        landed(WO[layer].at[pl.ds(0, 96)], o_sem.at[layer, 5])

    def projections_in(layer):
        landed(WP.at[layer, pl.ds(0, 192)], w_local.at[layer])
        landed(WP.at[layer, pl.ds(0, 192)], w_recv.at[layer])
        scale = gain[layer:layer + 1, :]

        def fold(i, carry):
            rows = pl.ds(pl.multiple_of(i * 16, 16), 16)
            WP[layer, rows, :] = (WP[layer, rows, :].astype(F32) * scale).astype(BF16)
            return carry

        lax.fori_loop(0, 24, fold, 0)

    def weights_sent():
        for layer in range(2):
            landed(WP.at[layer, pl.ds(0, 192)], w_send.at[layer])
            output_sent(layer)

    def put_projected(projected, dst):
        out = projected.astype(BF16)
        for to in range(4):
            dst[to, 0:16, :] = out[to * 16:to * 16 + 16, :]
            dst[to, 16:32, :] = out[64 + to * 16:64 + to * 16 + 16, :]

    def project(layer):
        squares = jnp.zeros((128, 128), F32)
        acc = jnp.zeros((128, 256), F32)
        for on in (0, 1, 3, 2):
            if on:
                gather_last(layer, on)
            for ch in range(2):
                along = ORDERS[ch][2]
                came = (at[along] + 4 - on) % 4
                spots = [(came, other) if along == "z" else (other, came) for other in range(4)]
                parts, weights = [], []
                for z, y in spots:
                    parts.append(jnp.concatenate(
                        [G[layer, rh * 2 + ch, z, y].reshape(64, 128) for rh in range(2)], axis=0))
                    start = pl.multiple_of(z * 1024 + y * 256 + ch * 128, 128)
                    weights.append(WP[layer, 0:256, pl.ds(start, 128)])
                for part in parts:
                    wide = part.astype(F32)
                    squares += wide * wide
                acc += lax.dot_general(
                    jnp.concatenate(parts, axis=1), jnp.concatenate(weights, axis=1), LANES,
                    preferred_element_type=F32,
                )
        factor = lax.rsqrt(jnp.sum(squares, axis=1, keepdims=True) * (1.0 / 4096) + RMS_EPS)
        put_projected(acc * factor, SA4.at[layer])
        exchange_start(2 * layer, SA4.at[layer], RA4.at[layer])
        acc = jnp.zeros((128, 128), F32)
        for z in range(4):
            acc += lax.dot_general(
                jnp.concatenate(rows_chunk(layer, z), axis=1), WP[layer, 256:384, z * 1024:(z + 1) * 1024], LANES,
                preferred_element_type=F32,
            )
        put_projected(acc * factor, SB2.at[layer])
        exchange_start(2 * layer + 1, SB2.at[layer], RB2.at[layer])

    def active_rows():
        row = lax.broadcasted_iota(jnp.int32, (32, 32), 0)
        col = lax.broadcasted_iota(jnp.int32, (32, 32), 1)
        spread = jnp.broadcast_to(lens[0:1, :], (32, 32))
        return jnp.sum(jnp.where(row == col, spread, 0), axis=1, keepdims=True) > STEP

    low = lax.broadcasted_iota(jnp.int32, (32, 128), 1) < 64

    def swap(value):
        return pltpu.roll(value, 64, 1)

    own_lanes = (lax.broadcasted_iota(jnp.int32, (32, 256), 0) // 8
                 == lax.broadcasted_iota(jnp.int32, (32, 256), 1) // 64)

    def pack(layer):
        landed(ST.at[layer], st_sem.at[layer])

        def four(group, carry):
            for half in range(2):
                even, odd = [
                    ST[layer, group * 4 + half * 2 + i].reshape(256, 64) for i in range(2)
                ]
                both = jnp.concatenate([even, odd], axis=1)
                S16[layer, group, :, half * 128:(half + 1) * 128] = both.astype(BF16)
            return carry

        lax.fori_loop(0, 8, four, 0)

    def head_vectors(layer, h):
        cols = slice(h * 64, (h + 1) * 64)
        base = jnp.concatenate([dbase[layer:layer + 1, cols], rbase[layer:layer + 1, cols]], axis=1)
        rec_key = RA4[layer, h, :, 0:128].astype(F32)
        opened = jax.nn.sigmoid(base + RA4[layer, h, :, 128:256].astype(F32))
        dec_rate = jnp.where(low, jnp.exp(-0.6065306597126334 * opened), opened)
        both = rec_key * dec_rate
        key_rec = swap(rec_key)
        square = jnp.sum(jnp.where(low, key_rec * key_rec, 0.0), axis=1, keepdims=True)
        scale = 1.0 / jnp.maximum(jnp.sqrt(square), 1e-12)
        return dec_rate, both, key_rec, scale

    def update_vectors(layer):
        active = active_rows()
        for h in range(4):
            dec_rate, both, key_rec, scale = head_vectors(layer, h)
            key_rate = jnp.where(active, swap(both), 0.0)
            PQ[pl.ds(h, 32, stride=8), :] = key_rate * scale
            PQ[pl.ds(4 + h, 32, stride=8), :] = key_rate
            DEC[pl.ds(h, 32, stride=8), :] = jnp.where(active, dec_rate, 1.0)

    def recur(layer):
        active = active_rows()
        first_sums, second_sums = [], []
        for h in range(4):
            dec_rate, both, key_rec, scale = head_vectors(layer, h)
            total = jnp.sum(jnp.where(low, 0.0, both * key_rec), axis=1, keepdims=True)
            first_sums.append(total * scale)
            second_sums.append(total)
            V8[pl.ds(h, 32, stride=8), :] = key_rec * -scale
            V8[pl.ds(4 + h, 32, stride=8), :] = both
        for group in range(8):
            vectors = V8[group * 32:(group + 1) * 32, :]
            vectors = jnp.where(low, vectors, swap(vectors))
            vectors = jnp.where(own_lanes, jnp.concatenate([vectors, vectors], axis=1), 0.0).astype(BF16)
            got = lax.dot_general(vectors, S16[layer, group], LANES, preferred_element_type=F32)
            for half in range(2):
                M2[half, group * 32:(group + 1) * 32, :] = got[:, half * 128:(half + 1) * 128]
        exchange_done(2 * layer + 1, RB2.at[layer])

        def heads(base):
            return jnp.where(low, M2[base // 2 % 2, pl.ds(base, 32, stride=8), :],
                             M2[base // 2 % 2, pl.ds(base + 1, 32, stride=8), :])

        for half in range(2):
            even, odd = 2 * half, 2 * half + 1
            even_vg, odd_vg = RB2[layer, even].astype(F32), RB2[layer, odd].astype(F32)
            value = jnp.where(low, even_vg, swap(odd_vg))
            gate = jax.nn.sigmoid(jnp.where(low, swap(even_vg), odd_vg))
            sa, direct = heads(even), heads(4 + even)
            half_cols = slice(half * 128, (half + 1) * 128)
            SA[:, half_cols] = sa
            VA[:, half_cols] = value
            readout = (direct + sa * jnp.where(low, first_sums[even], first_sums[odd])
                       + value * jnp.where(low, second_sums[even], second_sums[odd]))

            def head_mean(data):
                return jnp.where(low, jnp.sum(jnp.where(low, data, 0.0), axis=1, keepdims=True),
                                 jnp.sum(jnp.where(low, 0.0, data), axis=1, keepdims=True)) * (1.0 / 64)

            readout = readout - head_mean(readout)
            normal = readout * lax.rsqrt(head_mean(readout * readout) + GROUP_EPS)
            rows = jnp.where(active, normal * ggain[layer:layer + 1, half_cols] * gate, 0.0).astype(BF16)
            for rh in range(2):
                GP[layer][tp, rh * 2 + half] = rows[rh * 16:(rh + 1) * 16, :]

    head_of = lax.broadcasted_iota(jnp.int32, (8, 256), 1) // 64
    row_of = lax.broadcasted_iota(jnp.int32, (8, 256), 0)

    def update(layer, start, count):
        for b in range(start, start + count):
            left = jnp.where(row_of < 4, jnp.broadcast_to(SA[b:b + 1, :], (8, 256)),
                             jnp.broadcast_to(VA[b:b + 1, :], (8, 256)))
            left = jnp.where(row_of % 4 == head_of, left, 0.0)
            delta = lax.dot_general(
                left.astype(BF16), PQ[b * 8:(b + 1) * 8, 0:64].astype(BF16), ROWS,
                preferred_element_type=F32,
            )
            for h in range(4):
                ST[layer, b, h] = (ST[layer, b, h] * DEC[b * 8 + h:b * 8 + h + 1, 0:64]
                                   + delta[h * 64:(h + 1) * 64, :])

    def plane_first(layer):
        here = GP[layer].at[tp]
        for hop_z in (2, 1, 3, 0):
            for hop_y in (2, 1, 3, 0):
                if hop_z or hop_y:
                    send(here, p_send.at[layer], p_recv.at[layer, hop_z], z=hop_z, y=hop_y)

    def plane_last(layer, hop_z):
        landed(GP[layer].at[pl.ds(0, 4 if hop_z else 3)], p_recv.at[layer, hop_z])

    gather_first(0)
    projections_out(0)
    pltpu.make_async_copy(state.at[0], ST.at[0], st_sem.at[0]).start()
    weights_local(1)
    pltpu.make_async_copy(state.at[1], ST.at[1], st_sem.at[1]).start()
    gather_middle(0)
    for copy in small:
        copy.wait()
    projections_in(0)
    pack(0)
    project(0)
    output_far_x(0)
    output_to_partner(0)
    projections_out(1)
    output_to_partner(1)
    exchange_done(0, RA4.at[0])
    recur(0)
    plane_first(0)
    output_pass_on(0)
    update_vectors(0)
    update(0, 0, 32)
    projections_in(1)
    output_in(0)

    def came(hop_z):
        plane_last(0, hop_z)
        return (at["z"] + 4 - hop_z) % 4

    out = output_product(GP0, WO0, [functools.partial(came, hop_z) for hop_z in (0, 1, 3, 2)])
    for q in range(4):
        rh, ch = q // 2, q % 2
        G[1, q, at["z"], at["y"], at["x"]] = out[rh * 16:(rh + 1) * 16, ch * 128:(ch + 1) * 128]
    gather_first(1)
    gather_middle(1)
    output_over_x(1)
    pack(1)
    project(1)
    output_far_x(1)
    exchange_done(2, RA4.at[1])
    recur(1)
    plane_first(1)
    output_pass_on(1)
    update_vectors(1)
    update(1, 0, 32)
    output_in(1)
    for hop_z in range(4):
        plane_last(1, hop_z)
    for a in range(2):
        gather_sent(a)
        exchange_sent(2 * a, SA4.at[a])
        exchange_sent(2 * a + 1, SB2.at[a])
        landed(GP[a].at[pl.ds(0, 15)], p_send.at[a])
    weights_sent()


def finish_kernel(state_in, rows, weight, state_out, mixed_out, mixed, sem):
    copies = [pltpu.make_async_copy(state_in.at[layer], state_out.at[layer], sem.at[layer]) for layer in range(2)]
    for copy in copies:
        copy.start()
    mixed[...] = output_product(rows, weight, [functools.partial(int, z) for z in range(4)])
    copies.append(pltpu.make_async_copy(mixed, mixed_out, sem.at[2]))
    copies[2].start()
    for copy in copies:
        copy.wait()


def local(tokens, lengths, norm_gain, w_recept, w_key, w_value, w_decay, w_rate, w_gate, w_out,
          decay_base, rate_base, group_gain, state):
    weights = [jnp.swapaxes(w, 1, 2) for w in (w_recept, w_key, w_decay, w_rate, w_value, w_gate, w_out)]
    hbm = pl.BlockSpec(memory_space=pltpu.HBM)
    vmem = pl.BlockSpec(memory_space=pltpu.VMEM)
    stepped, rows, columns = pl.pallas_call(
        step_kernel,
        out_shape=(pltpu.VMEM(state.shape, F32), pltpu.VMEM((16, 4, 16, 128), BF16), pltpu.VMEM((256, 4096), BF16)),
        in_specs=[hbm] * 14,
        out_specs=(vmem, vmem, vmem),
        scratch_shapes=[
            pltpu.VMEM((2, 4, 4, 4, 4, 16, 128), BF16),
            pltpu.VMEM((16, 4, 16, 128), BF16),
            pltpu.VMEM((2, 384, 4096), BF16),
            pltpu.VMEM((256, 4096), BF16),
            pltpu.VMEM((2, 4, 32, 256), BF16),
            pltpu.VMEM((2, 4, 32, 256), BF16),
            pltpu.VMEM((2, 4, 32, 128), BF16),
            pltpu.VMEM((2, 4, 32, 128), BF16),
            pltpu.VMEM((256, 128), F32),
            pltpu.VMEM((2, 256, 128), F32),
            pltpu.VMEM((2, 8, 256, 256), BF16),
            pltpu.VMEM((32, 256), F32),
            pltpu.VMEM((32, 256), F32),
            pltpu.VMEM((256, 128), F32),
            pltpu.VMEM((256, 128), F32),
            pltpu.VMEM((1, 32), jnp.int32),
            pltpu.VMEM((2, 4096), F32),
            pltpu.VMEM((2, 256), F32),
            pltpu.VMEM((2, 256), F32),
            pltpu.VMEM((2, 256), F32),
            pltpu.SemaphoreType.DMA((2, 4, 3)),
            pltpu.SemaphoreType.DMA((2, 4, 7)),
            pltpu.SemaphoreType.DMA((2,)),
            pltpu.SemaphoreType.DMA((2, 4)),
            pltpu.SemaphoreType.DMA((4,)),
            pltpu.SemaphoreType.DMA((4,)),
            pltpu.SemaphoreType.DMA((2,)),
            pltpu.SemaphoreType.DMA((2,)),
            pltpu.SemaphoreType.DMA((2,)),
            pltpu.SemaphoreType.DMA((2, 10)),
            pltpu.SemaphoreType.DMA((2,)),
            pltpu.SemaphoreType.DMA((4,)),
            pltpu.SemaphoreType.DMA((5,)),
        ],
        compiler_params=pltpu.CompilerParams(collective_id=0, has_side_effects=True, vmem_limit_bytes=44 << 20),
        name="decode_step",
    )(tokens, lengths.reshape(1, 32), norm_gain, *weights, decay_base, rate_base, group_gain, state)
    new_state, mixed = pl.pallas_call(
        finish_kernel,
        out_shape=(pltpu.HBM(state.shape, F32), pltpu.HBM((32, 256), BF16)),
        in_specs=[vmem] * 3,
        out_specs=(hbm, hbm),
        scratch_shapes=[pltpu.VMEM((32, 256), BF16), pltpu.SemaphoreType.DMA((3,))],
        compiler_params=pltpu.CompilerParams(vmem_limit_bytes=4 << 20),
        name="finish",
    )(stepped, rows, columns)
    return mixed, new_state


def solution(mesh):
    both = P(None, None, ("tp", "dp"))
    in_specs = (
        P("dp", "tp"), P("dp"), P(), both, both, both, both, both, both, both,
        P(None, "tp"), P(None, "tp"), P(None, "tp"), P(None, "dp", "tp", None, None),
    )
    out_specs = (P("dp", "tp"), P(None, "dp", "tp", None, None))
    return jax.shard_map(local, mesh=mesh, in_specs=in_specs, out_specs=out_specs, check_vma=False)
```
